256 devices in a mesh: dp: 4 (over x), kv: 32 (over z, y), tp: 2 (over core).
Axes of the slice: x: 4, y: 4, z: 8, core: 2. Of those that a mesh axis runs over, the one named last changes fastest.
Arguments:
- tokens: bfloat16 [768, 4096], P('dp', ('kv', 'tp')), may hold values from -10 to 10
- gain_mixer: bfloat16 [4096], replicated, may hold values from 0.099609375 to 1.8984375
- weight_query: bfloat16 [4096, 16, 128], P('kv', 'tp'), may hold values from -0.09375 to 0.09375
- weight_key: bfloat16 [4096, 16, 128], P('kv', 'tp'), may hold values from -0.09375 to 0.09375
- weight_value: bfloat16 [4096, 16, 128], P('kv', 'tp'), may hold values from -0.09375 to 0.09375
- weight_outgate: bfloat16 [4096, 16, 128], P('kv', 'tp'), may hold values from -0.09375 to 0.09375
- weight_ingate: bfloat16 [4096, 16], replicated, may hold values from -0.09375 to 0.09375
- weight_forget: bfloat16 [4096, 16], replicated, may hold values from -0.09375 to 0.09375
- bias_input: float32 [16], replicated, may hold values from -3 to 3
- bias_forget: float32 [16], replicated, may hold values from 0 to 5
- memory: float32 [768, 16, 128, 128], P(('dp', 'kv'), 'tp'), may hold values from -2.5 to 2.5
- normalizer: float32 [768, 16, 128], P(('dp', 'kv'), 'tp'), may hold values from -2.5 to 2.5
- stabilizer: float32 [768, 16], P(('dp', 'kv'), 'tp'), may hold values from -1 to 3
- head_gain: bfloat16 [16, 128], replicated, may hold values from 0.099609375 to 1.8984375
- weight_out: bfloat16 [2048, 4096], P('tp', 'kv'), may hold values from -0.125 to 0.125
- gain_channel: bfloat16 [4096], replicated, may hold values from 0.099609375 to 1.8984375
- weight_up: bfloat16 [4096, 16384], P(None, ('kv', 'tp')), may hold values from -0.09375 to 0.09375
- weight_down: bfloat16 [16384, 4096], P(('kv', 'tp')), may hold values from -0.125 to 0.125
Outputs:
- layer_out: bfloat16 [768, 4096], P('dp', ('kv', 'tp'))
- new_memory: float32 [768, 16, 128, 128], P(('dp', 'kv'), 'tp')
- new_normalizer: float32 [768, 16, 128], P(('dp', 'kv'), 'tp')
- new_stabilizer: float32 [768, 16], P(('dp', 'kv'), 'tp')
The draws below stay inside these ranges and needn't reach their ends.
All inputs are finite; a program needn't handle non-finite values.
Results may differ from the reference program's by a relative error of at most 0.017.
Values may be sent and summed in bfloat16 or wider, within the bound.
A program may use at most 64 MiB of HBM per device.

```python
import math
import jax
import jax.numpy as jnp
from jax import lax

D = 4096
HEADS = 16
HD = 128
WIDTH = 2048
FF = 16384
SEQ_DEV = 6
BATCH = 768
N_DP = 4
N_KV = 32
N_TP = 2


def draw_tokens(key, part):
    columns = jnp.arange(D, dtype=jnp.float32) / (D - 1)
    base = jnp.clip(jax.random.normal(key, (BATCH, D), jnp.float32), -4.0, 4.0)
    rising = jnp.exp(columns * math.log(5.0))
    return (base * rising * 0.5).astype(jnp.bfloat16)


def with_spikes(values, rng, source, target, shards_of, factor):
    def block_of(position):
        return (jnp.arange(values.shape[position]) // (values.shape[position] // shards_of)).reshape((-1,) + (1,) * (values.ndim - 1 - position))

    first = jax.random.permutation(rng, shards_of)[block_of(target)]
    far = (block_of(target) + shards_of // 2) % shards_of
    return jnp.where((block_of(source) == first) | (block_of(source) == far), factor * values, values)


def steps_of(own_key, shape, pieces, low, largest):
    def one(position, parts):
        draws = jax.random.uniform(jax.random.fold_in(jax.random.fold_in(own_key, 6), position), (parts,), jnp.float32, low / len(pieces), largest / len(pieces))
        return jnp.repeat(jnp.exp(draws), shape[position] // parts).reshape((-1,) + (1,) * (len(shape) - position - 1))

    factor_of = one(*pieces[0])
    for cut in pieces[1:]:
        factor_of = factor_of * one(*cut)
    return factor_of


def noise(rng, dims, width, limit, split=(), kind=jnp.bfloat16):
    drawn = width * jax.random.normal(rng, dims, jnp.float32)
    if split:
        drawn = drawn * steps_of(rng, dims, split, -0.22, 0.18)
    return jnp.clip(drawn, -limit, limit).astype(kind)


def noise_with(key, dims, width, most, pieces, heavy, held_as=jnp.bfloat16):
    result = width * jax.random.normal(key, dims, jnp.float32)
    if pieces:
        result = result * steps_of(key, dims, pieces, -0.22, 0.18)
    return jnp.clip(with_spikes(result, jax.random.fold_in(key, 3), *heavy), -most, most).astype(held_as)


def setup_inputs(seed: int = 0) -> dict:
    key_list = jax.random.split(jax.random.key(seed), 19)
    return {
        "tokens": draw_tokens(jax.random.fold_in(key_list[18], 71), 0),
        "gain_mixer": jnp.clip(1.0 + 0.18 * jax.random.normal(key_list[1], (D,), jnp.float32), 0.099609375, 1.8984375).astype(jnp.bfloat16),
        "weight_query": noise(key_list[2], (D, HEADS, HD), D ** -0.5, 0.09375, ((0, 32), (1, 2))),
        "weight_key": noise(key_list[3], (D, HEADS, HD), D ** -0.5, 0.09375, ((0, 32), (1, 2))),
        "weight_value": noise(key_list[4], (D, HEADS, HD), D ** -0.5, 0.09375, ((0, 32), (1, 2))),
        "weight_outgate": noise(key_list[5], (D, HEADS, HD), D ** -0.5, 0.09375, ((0, 32), (1, 2))),
        "weight_ingate": noise(key_list[6], (D, HEADS), D ** -0.5, 0.09375),
        "weight_forget": noise(key_list[7], (D, HEADS), D ** -0.5, 0.09375),
        "bias_input": noise(key_list[8], (HEADS,), 1.0, 3.0, (), jnp.float32),
        "bias_forget": jnp.clip(jax.random.uniform(key_list[9], (HEADS,), jnp.float32, 0.0, 5.0), 0.0, 5.0),
        "memory": noise(key_list[10], (BATCH, HEADS, HD, HD), 0.3, 2.5, ((0, 128), (1, 2)), jnp.float32),
        "normalizer": noise(key_list[11], (BATCH, HEADS, HD), 0.3, 2.5, ((0, 128), (1, 2)), jnp.float32),
        "stabilizer": jnp.clip(-1.0 + 4.0 * jax.random.uniform(key_list[12], (BATCH, HEADS), jnp.float32) ** steps_of(key_list[12], (BATCH, HEADS), ((0, 128), (1, 2)), -0.2, 0.2), -1.0, 3.0),
        "head_gain": jnp.clip(1.0 + 0.18 * jax.random.normal(key_list[13], (HEADS, HD), jnp.float32), 0.099609375, 1.8984375).astype(jnp.bfloat16),
        "weight_out": noise(key_list[14], (WIDTH, D), WIDTH ** -0.5, 0.125, ((0, 2), (1, 32))),
        "gain_channel": jnp.clip(1.0 + 0.18 * jax.random.normal(key_list[15], (D,), jnp.float32), 0.099609375, 1.8984375).astype(jnp.bfloat16),
        "weight_up": noise(key_list[16], (D, FF), D ** -0.5, 0.09375, ((1, 64),)),
        "weight_down": noise_with(key_list[17], (FF, D), FF ** -0.5, 0.125, ((0, 64),), (0, 1, 64, 4.0)),
    }


epsilon = 1e-06

def project(scaled, weight):
    return jnp.dot(scaled, weight.reshape(weight.shape[0], -1), preferred_element_type=jnp.float32)

def cell_update(queries, keys_in, values_in, outgates, ingate, forget, memory, normalizer, stabilizer, head_scale):
    head_dim = queries.shape[-1]
    query_wide = queries.astype(jnp.float32)
    key_scaled = keys_in.astype(jnp.float32) * head_dim ** (-0.5)
    value_wide = values_in.astype(jnp.float32)
    new_stabilizer = jnp.maximum(forget + stabilizer, ingate)
    retain = jnp.exp(forget + stabilizer - new_stabilizer)
    inflow = jnp.exp(ingate - new_stabilizer)
    new_memory = retain[..., None, None] * memory + (inflow[..., None] * value_wide)[..., :, None] * key_scaled[..., None, :]
    new_normalizer = retain[..., None] * normalizer + inflow[..., None] * key_scaled
    numerator = jnp.einsum('bhvk,bhk->bhv', new_memory, query_wide, precision=lax.Precision.HIGHEST)
    denominator = lax.optimization_barrier(jnp.sum(new_normalizer * query_wide, axis=-1))
    readout = numerator / jnp.maximum(jnp.abs(denominator), jnp.exp(-new_stabilizer))[..., None]
    centered = readout - lax.optimization_barrier(jnp.mean(readout, axis=-1, keepdims=True))
    normed = centered * lax.rsqrt(lax.optimization_barrier(jnp.mean(centered * centered, axis=-1, keepdims=True)) + epsilon)
    gated_out = normed * head_scale.astype(jnp.float32) * jax.nn.sigmoid(outgates.astype(jnp.float32))
    return (gated_out.astype(jnp.bfloat16), new_memory, new_normalizer, new_stabilizer)

def reference(tokens, gain_mixer, weight_query, weight_key, weight_value, weight_outgate, weight_ingate, weight_forget, bias_input, bias_forget, memory, normalizer, stabilizer, head_gain, weight_out, gain_channel, weight_up, weight_down):
    tokens_wide = tokens.astype(jnp.float32)
    scaled = (tokens_wide * gain_mixer.astype(jnp.float32)).astype(jnp.bfloat16)
    inverse = lax.rsqrt(lax.optimization_barrier(jnp.mean(tokens_wide * tokens_wide, axis=1)) + epsilon)[:, None]
    head_shape = (BATCH, HEADS, HD)
    queries = (inverse * project(scaled, weight_query)).astype(jnp.bfloat16).reshape(head_shape)
    keys_proj = (inverse * project(scaled, weight_key)).astype(jnp.bfloat16).reshape(head_shape)
    values_proj = (inverse * project(scaled, weight_value)).astype(jnp.bfloat16).reshape(head_shape)
    outgates = (inverse * project(scaled, weight_outgate)).astype(jnp.bfloat16).reshape(head_shape)
    ingate = inverse * jnp.dot(scaled, weight_ingate, preferred_element_type=jnp.float32) + bias_input
    forget = jax.nn.log_sigmoid(inverse * jnp.dot(scaled, weight_forget, preferred_element_type=jnp.float32) + bias_forget)
    row_blocks = N_DP * N_KV

    def block_cell(blocked):
        return cell_update(*blocked, head_gain)
    blocked = tuple((array.reshape((row_blocks, SEQ_DEV) + array.shape[1:]) for array in (queries, keys_proj, values_proj, outgates, ingate, forget, memory, normalizer, stabilizer)))
    results = lax.map(block_cell, blocked)
    heads_out, new_memory, new_normalizer, new_stabilizer = tuple((array.reshape((BATCH,) + array.shape[2:]) for array in results))
    heads_flat = heads_out.reshape(BATCH, WIDTH)
    half_width = WIDTH // N_TP
    mixed_rows = tokens_wide
    for member in range(N_TP):
        partial_value = jnp.dot(heads_flat[:, member * half_width:(member + 1) * half_width], weight_out[member * half_width:(member + 1) * half_width], preferred_element_type=jnp.float32).astype(jnp.bfloat16)
        mixed_rows = mixed_rows + partial_value.astype(jnp.float32)
    mixed_rows = mixed_rows.astype(jnp.bfloat16)
    mixed_wide = mixed_rows.astype(jnp.float32)
    scaled_mlp = (mixed_wide * gain_channel.astype(jnp.float32)).astype(jnp.bfloat16)
    inverse_mlp = lax.rsqrt(lax.optimization_barrier(jnp.mean(mixed_wide * mixed_wide, axis=1)) + epsilon)[:, None]
    activation = jax.nn.relu(inverse_mlp * jnp.dot(scaled_mlp, weight_up, preferred_element_type=jnp.float32))
    squared = (activation * activation).astype(jnp.bfloat16)
    layer_out = (mixed_wide + jnp.dot(squared, weight_down, preferred_element_type=jnp.float32)).astype(jnp.bfloat16)
    return (layer_out, new_memory, new_normalizer, new_stabilizer)
```

```python
import functools

import jax
import jax.numpy as jnp
from jax import lax
from jax.experimental import pallas as pl
from jax.experimental.pallas import tpu as pltpu
from jax.sharding import Mesh
from jax.sharding import PartitionSpec as P

EPS = 1e-06
KV_TP = ("z", "y", "tp")
KV = ("z", "y")
DP_KV = ("dp", "z", "y")
MESH = pl.DeviceIdType.MESH
F32 = jnp.float32
BF16 = jnp.bfloat16


def by_distance(n):
    return sorted(range(1, n), key=lambda d: (min(d, n - d), d))


def kernel(
    nz,
    ny,
    width_full,
    tokens,
    gain_mixer,
    w0,
    w1,
    w2,
    w3,
    w_in,
    w_forget,
    bias_in,
    bias_forget,
    memory,
    normalizer,
    stabilizer,
    head_gain,
    w_out,
    gain_channel,
    w_up,
    w_down,
    out,
    inflow_v_out,
    key_out,
    retain_out,
    norm_out,
    stab_out,
    tok_in,
    tok_half,
    tok_all,
    gains,
    wig,
    wfg,
    mem,
    wbuf,
    wide,
    w_flat,
    partial,
    part_send,
    part_recv,
    gate_send,
    gate_recv,
    rows_send,
    rows_recv,
    q_f32,
    mq,
    heads_own,
    heads_all,
    heads_f32,
    wo_all,
    up_all,
    down_all,
    mixed_all,
    acc,
    down_send,
    down_y,
    sum_send,
    sum_recv,
    fin_send,
    fin_recv,
    local_sem,
    pair_send,
    pair_recv,
    wy_send,
    wy_recv,
    ty_send,
    ty_recv,
    pz_send,
    pz_recv,
    gz_send,
    gz_recv,
    ry_send,
    ry_recv,
    hz_send,
    hz_recv,
    hy_send,
    hy_recv,
    mz_send,
    mz_recv,
    my_send,
    my_recv,
    dy_send,
    dy_recv,
    dz_send,
    dz_recv,
):
    z = lax.axis_index("z")
    y = lax.axis_index("y")
    tp = lax.axis_index("tp")
    other = 1 - tp
    half_z = nz // 2
    rows = tokens.shape[0]
    half = rows // 2
    own = 6
    heads = 8
    zrows = ny * own
    block = ny * 128
    near_z = by_distance(nz)
    near_y = by_distance(ny)
    far_z = near_z[::-1]
    pending = []

    def remote(src, dst, send, recv, **to):
        return pltpu.make_async_remote_copy(
            src_ref=src, dst_ref=dst, send_sem=send, recv_sem=recv, device_id=to, device_id_type=MESH
        )

    def push(*args, **to):
        copy = remote(*args, **to)
        copy.start()
        pending.append(copy)
        return copy

    barrier = pltpu.get_barrier_semaphore()
    for d in near_z:
        for t in range(2):
            pl.semaphore_signal(
                barrier, inc=1, device_id={"z": (z + d) % nz, "tp": t}, device_id_type=MESH
            )
    for d in near_y:
        pl.semaphore_signal(barrier, inc=1, device_id={"y": (y + d) % ny}, device_id_type=MESH)
    pl.semaphore_signal(barrier, inc=1, device_id={"tp": other}, device_id_type=MESH)

    rows_of_block = pl.ds(pl.multiple_of(z * block, block), block)
    loads = [
        pltpu.make_async_copy(w_in.at[rows_of_block], wig, local_sem.at[0]),
        pltpu.make_async_copy(w_forget.at[rows_of_block], wfg, local_sem.at[1]),
        pltpu.make_async_copy(memory, mem, local_sem.at[2]),
        pltpu.make_async_copy(w_out, wo_all.at[tp], local_sem.at[3]),
        pltpu.make_async_copy(w_up, up_all.at[tp], local_sem.at[4]),
        pltpu.make_async_copy(w_down, down_all.at[tp], local_sem.at[5]),
    ]
    weights = (w0, w1, w2, w3)
    for m in range(4):

        @pl.when(y == m)
        def _(m=m):
            pltpu.make_async_copy(weights[m], wbuf.at[m], local_sem.at[6]).start()

    for copy in loads:
        copy.start()
    gains[0] = gain_mixer[...].astype(F32)
    gains[1] = gain_channel[...].astype(F32)

    pl.semaphore_wait(barrier, 2 * (nz - 1) + (ny - 1) + 1)

    tok_copy = push(tokens, tok_in, pair_send.at[0], pair_recv.at[0], tp=other)
    for m in range(4):

        @pl.when(y != m)
        def _(m=m):
            remote(weights[m], wbuf.at[y], wy_send.at[m], wy_recv.at[y], y=m).start()

    out_copy = push(w_out, wo_all.at[tp], pair_send.at[1], pair_recv.at[1], tp=other)
    up_copy = push(w_up, up_all.at[tp], pair_send.at[2], pair_recv.at[2], tp=other)
    down_copy = push(w_down, down_all.at[tp], pair_send.at[3], pair_recv.at[3], tp=other)

    tok_copy.wait_recv()
    mine, theirs = tokens[...].astype(F32), tok_in[...].astype(F32)
    first = jnp.where(tp == 0, mine, theirs)
    second = jnp.where(tp == 0, theirs, mine)
    chip = jnp.concatenate([first, second], axis=1).astype(BF16)
    tok_all[y] = chip
    tok_half[0] = chip[:half]
    tok_half[1] = chip[half:]
    for d in near_y:
        push(
            tok_all.at[y], tok_all.at[y], ty_send.at[d], ty_recv.at[y], y=(y + d) % ny
        )
    for d in near_y:
        s = (y + d) % ny
        remote(tok_all.at[s], tok_all.at[s], ty_send.at[d], ty_recv.at[s], y=s).wait_recv()
    squares = jnp.zeros((rows, 1), F32)
    scaled = []
    for s in range(ny):
        wide_rows = tok_all[s].astype(F32)
        squares = squares + jnp.sum(wide_rows * wide_rows, axis=1, keepdims=True)
        scaled.append((wide_rows * gains[0, pl.ds(z * ny + s, 1), :]).astype(BF16))
    x = jnp.concatenate(scaled, axis=1)
    loads[0].wait()
    loads[1].wait()
    gate = jnp.concatenate(
        [
            jnp.dot(x, wig[...], preferred_element_type=F32),
            jnp.dot(x, wfg[...], preferred_element_type=F32),
            jnp.broadcast_to(squares, (rows, 96)),
        ],
        axis=1,
    )
    for k in range(nz):
        gate_send[k] = gate[k * zrows : (k + 1) * zrows]
    for d in far_z:
        to = (z + d) % nz
        push(gate_send.at[to], gate_recv.at[z], gz_send.at[d], gz_recv.at[z], z=to)

    def flatten(s):
        wide[...] = wbuf[s].astype(F32).reshape(128 * heads, 128)
        base = pl.multiple_of(s * 128, 128)
        for h in range(heads):
            w_flat[pl.ds(base, 128), h * 128 : (h + 1) * 128] = wide[
                pl.ds(h, 128, stride=heads), :
            ].astype(BF16)

    pltpu.make_async_copy(weights[0], wbuf.at[y], local_sem.at[6]).wait()
    flatten(y)
    for d in near_y:
        s = (y + d) % ny
        remote(wbuf.at[s], wbuf.at[s], wy_send.at[0], wy_recv.at[s], y=s).wait_recv()
        flatten(s)
    wcols = heads * 64
    for n in range(2):
        partial[n] = jnp.dot(
            x, w_flat[:, n * wcols : (n + 1) * wcols], preferred_element_type=F32
        )
    for k in range(nz):
        part_send[k] = jnp.concatenate(
            [
                partial[0, k * zrows : (k + 1) * zrows, :],
                partial[1, k * zrows : (k + 1) * zrows, :],
            ],
            axis=0,
        ).astype(BF16)
    for d in far_z:
        to = (z + d) % nz
        push(part_send.at[to], part_recv.at[z], pz_send.at[d], pz_recv.at[z], z=to)

    gate_sum = gate_send[z]
    for d in near_z:
        s = (z + d) % nz
        remote(gate_recv.at[s], gate_recv.at[s], gz_send.at[d], gz_recv.at[s], z=s).wait_recv()
        gate_sum = gate_sum + gate_recv[s]
    inverse = lax.rsqrt(gate_sum[:, 32:33] / width_full + EPS)
    gate_pre = inverse * gate_sum
    gate_rows = jnp.zeros((own, 128), F32)
    for k in range(ny):
        gate_rows = gate_rows + jnp.where(y == k, gate_pre[k * own : (k + 1) * own], 0.0)
    in_all = gate_rows[:, 0:16] + bias_in[...]
    forget_all = gate_rows[:, 16:32] + bias_forget[...]
    ingate = jnp.where(tp == 0, in_all[:, :8], in_all[:, 8:])
    forget_pre = jnp.where(tp == 0, forget_all[:, :8], forget_all[:, 8:])
    forget = jnp.minimum(forget_pre, 0.0) - jnp.log(1.0 + jnp.exp(-jnp.abs(forget_pre)))
    carried = forget + stabilizer[...]
    new_stab = jnp.maximum(carried, ingate)
    stab_out[...] = new_stab
    diagonal = lax.broadcasted_iota(jnp.int32, (heads, heads), 0) == lax.broadcasted_iota(
        jnp.int32, (heads, heads), 1
    )

    def column(value):
        return jnp.concatenate(
            [
                jnp.sum(
                    jnp.where(diagonal, jnp.broadcast_to(value[b : b + 1], (heads, heads)), 0.0),
                    axis=1,
                    keepdims=True,
                )
                for b in range(own)
            ],
            axis=0,
        )

    retain = column(jnp.exp(carried - new_stab))
    inflow = column(jnp.exp(ingate - new_stab))
    floor = column(jnp.exp(-new_stab))

    total = part_send[z].astype(F32)
    for d in near_z:
        s = (z + d) % nz
        remote(part_recv.at[s], part_recv.at[s], pz_send.at[d], pz_recv.at[s], z=s).wait_recv()
        total = total + part_recv[s].astype(F32)
    for h in range(heads):
        n, c = h // 4, h % 4
        rows_send[pl.ds(h, zrows, stride=heads), :] = inverse * total[
            n * zrows : (n + 1) * zrows, c * 128 : (c + 1) * 128
        ]
    piece = own * heads
    for d in near_y:
        to = (y + d) % ny
        push(
            rows_send.at[pl.ds(pl.multiple_of(to * piece, piece), piece)],
            rows_recv.at[y],
            ry_send.at[d],
            ry_recv.at[y],
            y=to,
        )
    rows_recv[y] = rows_send[pl.ds(pl.multiple_of(y * piece, piece), piece), :]
    for d in near_y:
        s = (y + d) % ny
        remote(rows_recv.at[s], rows_recv.at[s], ry_send.at[d], ry_recv.at[s], y=s).wait_recv()

    query = rows_recv[0].astype(BF16).astype(F32)
    key = rows_recv[1].astype(BF16).astype(F32) * 128**-0.5
    value = rows_recv[2].astype(BF16).astype(F32)
    gate_o = rows_recv[3].astype(BF16).astype(F32)
    q_f32[...] = query
    new_norm = retain * normalizer[...] + inflow * key
    norm_out[...] = new_norm
    inflow_value = inflow * value
    inflow_v_out[...] = inflow_value
    key_out[...] = key
    retain_out[...] = jnp.broadcast_to(retain, (piece, 128))
    loads[2].wait()
    sub = lax.broadcasted_iota(jnp.int32, (heads, 128), 0)
    contract = (((1,), (1,)), ((), ()))

    def readout_of(b, carry):
        q_b = q_f32[pl.ds(pl.multiple_of(b * heads, heads), heads), :].astype(BF16)
        found = jnp.zeros((heads, 128), F32)
        for h in range(heads):
            m_bh = mem[b * heads + h]
            high = m_bh.astype(BF16)
            low = (m_bh - high.astype(F32)).astype(BF16)
            product = lax.dot_general(
                q_b, high, contract, preferred_element_type=F32
            ) + lax.dot_general(q_b, low, contract, preferred_element_type=F32)
            found = jnp.where(sub == h, product, found)
        mq[pl.ds(pl.multiple_of(b * heads, heads), heads), :] = found
        return carry

    lax.fori_loop(0, own, readout_of, 0)
    numerator = retain * mq[...] + inflow_value * jnp.sum(key * query, axis=1, keepdims=True)
    denominator = jnp.sum(new_norm * query, axis=1, keepdims=True)
    readout = numerator / jnp.maximum(jnp.abs(denominator), floor)
    centered = readout - jnp.mean(readout, axis=1, keepdims=True)
    normed = centered * lax.rsqrt(jnp.mean(centered * centered, axis=1, keepdims=True) + EPS)
    gain_all = head_gain[...].astype(F32)
    gain_own = jnp.where(tp == 0, gain_all[:heads], gain_all[heads:])
    heads_out = (
        normed * jnp.concatenate([gain_own] * own, axis=0) * (1.0 / (1.0 + jnp.exp(-gate_o)))
    ).astype(BF16)
    heads_own[...] = heads_out

    core = z // half_z
    zl = z % half_z

    @pl.when(tp == core)
    def _():
        heads_all[zl, tp, y] = heads_out

    for d in far_z:
        push(
            heads_own,
            heads_all.at[zl, tp, y],
            hz_send.at[d],
            hz_recv.at[zl, tp],
            z=(z + d) % nz,
            tp=core,
        )

    @pl.when(tp != core)
    def _():
        remote(
            heads_own, heads_all.at[zl, tp, y], hz_send.at[0], hz_recv.at[zl, tp], tp=other
        ).start()

    for k in range(half_z):
        for t in range(2):
            here = heads_all.at[k, t, y]
            source = tp * half_z + k

            @pl.when(jnp.logical_or(source != z, tp != t))
            def _():
                remote(here, here, hz_send.at[0], hz_recv.at[k, t], tp=other).wait_recv()

            for d in near_y:
                push(
                    here, here, hy_send.at[d, k, t], hy_recv.at[y, k, t], y=(y + d) % ny
                )
    for k in range(half_z):
        for t in range(2):
            for d in near_y:
                s = (y + d) % ny
                there = heads_all.at[k, t, s]
                remote(there, there, hy_send.at[d, k, t], hy_recv.at[s, k, t], y=s).wait_recv()
            for s in range(ny):
                start = t * half * heads + (k * ny + s) * piece
                heads_f32[start : start + piece, :] = heads_all[k, t, s].astype(F32)
    gathered = jnp.concatenate(
        [
            heads_f32[pl.ds(t * half * heads + h, half, stride=heads), :].astype(BF16)
            for t in range(2)
            for h in range(heads)
        ],
        axis=1,
    )
    loads[3].wait()
    out_copy.wait_recv()
    attended = jnp.dot(
        gathered, wo_all[...].reshape(2 * heads * 128, 128), preferred_element_type=F32
    )
    mixed = (tok_half[tp].astype(F32) + attended).astype(BF16)
    mixed_all[z, y] = mixed

    for d in far_z:
        push(
            mixed_all.at[z, y], mixed_all.at[z, y], mz_send.at[d], mz_recv.at[z], z=(z + d) % nz
        )
    for d in [0] + near_z:
        s = (z + d) % nz
        here = mixed_all.at[s, y]
        if d:
            remote(here, here, mz_send.at[d], mz_recv.at[s], z=s).wait_recv()
        for e in near_y:
            push(here, here, my_send.at[d, e], my_recv.at[y, s], y=(y + e) % ny)
    loads[4].wait()
    up_copy.wait_recv()
    hidden = up_all.shape[2]
    squares = jnp.zeros((half, 1), F32)
    for d in [0] + near_z:
        s = (z + d) % nz
        for e in near_y:
            src = (y + e) % ny
            there = mixed_all.at[s, src]
            remote(there, there, my_send.at[d, e], my_recv.at[src, s], y=src).wait_recv()
        scaled = []
        for k in range(ny):
            wide_rows = mixed_all[s, k].astype(F32)
            squares = squares + jnp.sum(wide_rows * wide_rows, axis=1, keepdims=True)
            scaled.append((wide_rows * gains[1, pl.ds(s * ny + k, 1), :]).astype(BF16))
        lhs = jnp.concatenate(scaled, axis=1)
        here = pl.ds(pl.multiple_of(s * block, block), block)
        for t in range(2):
            product = jnp.dot(lhs, up_all[t, here, :], preferred_element_type=F32)
            if d:
                product = product + acc[t]
            acc[t] = product
    inverse_mlp = lax.rsqrt(squares / width_full + EPS)
    squared = []
    for t in range(2):
        activation = jnp.maximum(inverse_mlp * acc[t], 0.0)
        squared.append((activation * activation).astype(BF16))

    loads[5].wait()
    down_copy.wait_recv()
    order = far_z + [0]
    for d in order:
        to = (z + d) % nz
        here = pl.ds(pl.multiple_of(to * block, block), block)
        product = jnp.dot(
            squared[0], down_all[0, :, here], preferred_element_type=F32
        ) + jnp.dot(squared[1], down_all[1, :, here], preferred_element_type=F32)
        for k in range(ny):
            down_send[to, k] = product[:, k * 128 : (k + 1) * 128].astype(BF16)
        for e in near_y:
            dst = (y + e) % ny
            push(down_send.at[to, dst], down_y.at[y, to], dy_send.at[d, e], dy_recv.at[y, to], y=dst)
    total = None
    for d in order:
        to = (z + d) % nz
        summed = down_send[to, y].astype(F32)
        for e in near_y:
            src = (y + e) % ny
            there = down_y.at[src, to]
            remote(there, there, dy_send.at[d, e], dy_recv.at[src, to], y=src).wait_recv()
            summed = summed + down_y[src, to].astype(F32)
        if d:
            sum_send[to] = summed.astype(BF16)
            push(sum_send.at[to], sum_recv.at[z], dz_send.at[d], dz_recv.at[z], z=to)
        else:
            total = summed
    for d in near_z:
        s = (z + d) % nz
        remote(sum_recv.at[s], sum_recv.at[s], dz_send.at[d], dz_recv.at[s], z=s).wait_recv()
        total = total + sum_recv[s].astype(F32)
    final = (mixed_all[z, y].astype(F32) + total).astype(BF16)
    fin_send[...] = final
    fin_copy = push(fin_send, fin_recv, pair_send.at[4], pair_recv.at[4], tp=other)
    fin_copy.wait_recv()
    mine, theirs = final.astype(F32), fin_recv[...].astype(F32)
    upper = jnp.where(tp == 0, mine, theirs)
    lower = jnp.where(tp == 0, theirs, mine)
    out[:half] = jnp.where(tp == 0, upper[:, :64], upper[:, 64:]).astype(BF16)
    out[half:] = jnp.where(tp == 0, lower[:, :64], lower[:, 64:]).astype(BF16)

    for copy in pending:
        copy.wait_send()
    for m in range(4):

        @pl.when(y != m)
        def _(m=m):
            remote(weights[m], wbuf.at[y], wy_send.at[m], wy_recv.at[y], y=m).wait_send()

    @pl.when(tp != core)
    def _():
        remote(
            heads_own, heads_all.at[zl, tp, y], hz_send.at[0], hz_recv.at[zl, tp], tp=other
        ).wait_send()


def body(
    tokens,
    gain_mixer,
    weight_query,
    weight_key,
    weight_value,
    weight_outgate,
    weight_ingate,
    weight_forget,
    bias_input,
    bias_forget,
    memory,
    normalizer,
    stabilizer,
    head_gain,
    weight_out,
    gain_channel,
    weight_up,
    weight_down,
):
    nz, ny = lax.axis_size("z"), lax.axis_size("y")
    own, heads, hd = memory.shape[:3]
    width_full = gain_mixer.shape[0]
    rows = tokens.shape[0]
    half = rows // 2
    piece = own * heads
    zrows = ny * own
    block = ny * 128
    dma = pltpu.SemaphoreType.DMA
    vmem = pl.BlockSpec(memory_space=pltpu.VMEM)
    hbm = pl.BlockSpec(memory_space=pl.ANY)
    mem48 = memory.reshape(piece, hd, hd)
    layer_out, inflow_v, key, retain, new_norm, new_stab = pl.pallas_call(
        functools.partial(kernel, nz, ny, width_full),
        out_shape=(
            jax.ShapeDtypeStruct(tokens.shape, BF16),
            jax.ShapeDtypeStruct((piece, hd), F32),
            jax.ShapeDtypeStruct((piece, hd), F32),
            jax.ShapeDtypeStruct((piece, hd), F32),
            jax.ShapeDtypeStruct((piece, hd), F32),
            jax.ShapeDtypeStruct((own, heads), F32),
        ),
        in_specs=[vmem, vmem]
        + [hbm] * 6
        + [vmem, vmem, hbm, vmem, vmem, vmem, hbm, vmem, hbm, hbm],
        out_specs=(vmem,) * 6,
        scratch_shapes=[
            pltpu.VMEM(tokens.shape, BF16),
            pltpu.VMEM((2, half, 128), BF16),
            pltpu.VMEM((ny, rows, 128), BF16),
            pltpu.VMEM((2, width_full // 128, 128), F32),
            pltpu.VMEM((block, 16), BF16),
            pltpu.VMEM((block, 16), BF16),
            pltpu.VMEM((piece, hd, hd), F32),
            pltpu.VMEM((ny, 128, heads, hd), BF16),
            pltpu.VMEM((128 * heads, hd), F32),
            pltpu.VMEM((block, heads * hd), BF16),
            pltpu.VMEM((2, rows, heads * hd // 2), F32),
            pltpu.VMEM((nz, 2 * zrows, heads * hd // 2), BF16),
            pltpu.VMEM((nz, 2 * zrows, heads * hd // 2), BF16),
            pltpu.VMEM((nz, zrows, 128), F32),
            pltpu.VMEM((nz, zrows, 128), F32),
            pltpu.VMEM((zrows * heads, hd), F32),
            pltpu.VMEM((ny, piece, hd), F32),
            pltpu.VMEM((piece, hd), F32),
            pltpu.VMEM((piece, hd), F32),
            pltpu.VMEM((piece, hd), BF16),
            pltpu.VMEM((nz // 2, 2, ny, piece, hd), BF16),
            pltpu.VMEM((2 * half * heads, hd), F32),
            pltpu.VMEM((2, heads * hd, 128), BF16),
            pltpu.VMEM((2, *weight_up.shape), BF16),
            pltpu.VMEM((2, *weight_down.shape), BF16),
            pltpu.VMEM((nz, ny, half, 128), BF16),
            pltpu.VMEM((2, half, weight_up.shape[1]), F32),
            pltpu.VMEM((nz, ny, half, 128), BF16),
            pltpu.VMEM((ny, nz, half, 128), BF16),
            pltpu.VMEM((nz, half, 128), BF16),
            pltpu.VMEM((nz, half, 128), BF16),
            pltpu.VMEM((half, 128), BF16),
            pltpu.VMEM((half, 128), BF16),
            dma((7,)),
            dma((5,)),
            dma((5,)),
            dma((4,)),
            dma((4,)),
            dma((ny,)),
            dma((ny,)),
            dma((nz,)),
            dma((nz,)),
            dma((nz,)),
            dma((nz,)),
            dma((ny,)),
            dma((ny,)),
            dma((nz,)),
            dma((nz // 2, 2)),
            dma((ny, nz // 2, 2)),
            dma((ny, nz // 2, 2)),
            dma((nz,)),
            dma((nz,)),
            dma((nz, ny)),
            dma((ny, nz)),
            dma((nz, ny)),
            dma((ny, nz)),
            dma((nz,)),
            dma((nz,)),
        ],
        compiler_params=pltpu.CompilerParams(
            collective_id=0, has_side_effects=True, vmem_limit_bytes=56 * 1024 * 1024
        ),
    )(
        tokens,
        gain_mixer.reshape(-1, 128),
        weight_query,
        weight_key,
        weight_value,
        weight_outgate,
        weight_ingate,
        weight_forget,
        bias_input.reshape(1, -1),
        bias_forget.reshape(1, -1),
        mem48,
        normalizer.reshape(piece, hd),
        stabilizer,
        head_gain,
        weight_out,
        gain_channel.reshape(-1, 128),
        weight_up,
        weight_down,
    )
    new_memory = (
        retain[:, :1, None] * mem48 + inflow_v[:, :, None] * key[:, None, :]
    ).reshape(memory.shape)
    return (layer_out, new_memory, new_norm.reshape(normalizer.shape), new_stab)


def solution(mesh):
    kv = mesh.shape["kv"]
    ny = 4
    torus = Mesh(
        mesh.devices.reshape(mesh.shape["dp"], kv // ny, ny, mesh.shape["tp"]),
        ("dp", "z", "y", "tp"),
    )
    placed = (
        P("dp", KV_TP),
        P(),
        P(KV, "tp", None),
        P(KV, "tp", None),
        P(KV, "tp", None),
        P(KV, "tp", None),
        P(),
        P(),
        P(),
        P(),
        P(DP_KV, "tp", None, None),
        P(DP_KV, "tp", None),
        P(DP_KV, "tp"),
        P(),
        P("tp", KV),
        P(),
        P(None, KV_TP),
        P(KV_TP, None),
    )
    return jax.shard_map(
        body,
        mesh=torus,
        in_specs=placed,
        out_specs=(
            P("dp", KV_TP),
            P(DP_KV, "tp", None, None),
            P(DP_KV, "tp", None),
            P(DP_KV, "tp"),
        ),
        check_vma=False,
    )
```

```python
import functools

import jax
import jax.numpy as jnp
from jax import lax
from jax.experimental import pallas as pl
from jax.experimental.pallas import tpu as pltpu
from jax.sharding import Mesh
from jax.sharding import PartitionSpec as P

EPS = 1e-06
KV_TP = ("z", "y", "tp")
KV = ("z", "y")
DP_KV = ("dp", "z", "y")
MESH = pl.DeviceIdType.MESH
F32 = jnp.float32
BF16 = jnp.bfloat16


def by_distance(n):
    return sorted(range(1, n), key=lambda d: (min(d, n - d), d))


def kernel(
    nz,
    ny,
    width_full,
    tokens_hbm,
    gain_mixer_hbm,
    bias_in_hbm,
    bias_forget_hbm,
    normalizer_hbm,
    stabilizer_hbm,
    head_gain_hbm,
    gain_channel_hbm,
    w0,
    w1,
    w2,
    w3,
    w_in,
    w_forget,
    memory,
    w_out,
    w_up,
    w_down,
    packed,
    tokens,
    gain_mixer,
    bias_in,
    bias_forget,
    normalizer,
    stabilizer,
    head_gain,
    gain_channel,
    tok_in,
    tok_half,
    tok_all,
    gains,
    wig,
    wfg,
    mem,
    mem_split,
    w_raw,
    wide,
    w_own,
    w_flat,
    part_send,
    part_recv,
    gate_send,
    gate_recv,
    rows_wide,
    rows_send,
    rows_recv,
    q_twice,
    mq,
    heads_own,
    heads_all,
    heads_f32,
    wo_all,
    up_all,
    down_all,
    mixed_all,
    acc,
    down_send,
    down_y,
    sum_send,
    sum_recv,
    fin_send,
    fin_recv,
    small_sem,
    local_sem,
    pair_send,
    pair_recv,
    wy_send,
    wy_recv,
    ty_send,
    ty_recv,
    pz_send,
    pz_recv,
    gz_send,
    gz_recv,
    ry_send,
    ry_recv,
    hz_send,
    hz_recv,
    hy_send,
    hy_recv,
    mz_send,
    mz_recv,
    my_send,
    my_recv,
    dy_send,
    dy_recv,
    dz_send,
    dz_recv,
):
    z = lax.axis_index("z")
    y = lax.axis_index("y")
    tp = lax.axis_index("tp")
    other = 1 - tp
    half_z = nz // 2
    rows = tokens.shape[1]
    half = rows // 2
    own = 6
    heads = 8
    zrows = ny * own
    block = ny * 128
    near_z = by_distance(nz)
    near_y = by_distance(ny)
    far_z = near_z[::-1]
    pending = []
    contract = (((1,), (1,)), ((), ()))

    def remote(src, dst, send, recv, **to):
        return pltpu.make_async_remote_copy(
            src_ref=src, dst_ref=dst, send_sem=send, recv_sem=recv, device_id=to, device_id_type=MESH
        )

    def push(*args, **to):
        copy = remote(*args, **to)
        copy.start()
        pending.append(copy)
        return copy

    barrier = pltpu.get_barrier_semaphore()
    for d in near_z:
        for t in range(2):
            pl.semaphore_signal(
                barrier, inc=1, device_id={"z": (z + d) % nz, "tp": t}, device_id_type=MESH
            )
    for d in near_y:
        pl.semaphore_signal(barrier, inc=1, device_id={"y": (y + d) % ny}, device_id_type=MESH)
    pl.semaphore_signal(barrier, inc=1, device_id={"tp": other}, device_id_type=MESH)

    rows_of_block = pl.ds(pl.multiple_of(z * block, block), block)
    loads = [
        pltpu.make_async_copy(w_in.at[:, rows_of_block], wig, local_sem.at[0]),
        pltpu.make_async_copy(w_forget.at[:, rows_of_block], wfg, local_sem.at[1]),
        pltpu.make_async_copy(memory, mem, local_sem.at[2]),
        pltpu.make_async_copy(w_out, wo_all.at[tp], local_sem.at[3]),
        pltpu.make_async_copy(w_up, up_all.at[tp], local_sem.at[4]),
        pltpu.make_async_copy(w_down, down_all.at[tp], local_sem.at[5]),
    ]
    raw_loads = [
        pltpu.make_async_copy(w, w_raw.at[m], local_sem.at[6 + m])
        for m, w in enumerate((w0, w1, w2, w3))
    ]
    small = [
        pltpu.make_async_copy(src, dst, small_sem.at[i])
        for i, (src, dst) in enumerate(
            (
                (tokens_hbm, tokens),
                (gain_mixer_hbm, gain_mixer),
                (bias_in_hbm, bias_in),
                (bias_forget_hbm, bias_forget),
                (normalizer_hbm, normalizer),
                (stabilizer_hbm, stabilizer),
                (head_gain_hbm, head_gain),
                (gain_channel_hbm, gain_channel),
            )
        )
    ]
    for copy in raw_loads + small:
        copy.start()
    chunks = heads // 2
    for m in range(4):
        raw_loads[m].wait()
        wide[...] = w_raw[m].astype(F32).reshape(128 * heads, 128)
        for h in range(heads):
            w_own[m, h // 2, :, (h % 2) * 128 : (h % 2 + 1) * 128] = wide[
                pl.ds(h, 128, stride=heads), :
            ].astype(BF16)
    for copy in small:
        copy.wait()
    gains[0] = gain_mixer[...].astype(F32)
    gains[1] = gain_channel[...].astype(F32)

    pl.semaphore_wait(barrier, 2 * (nz - 1) + (ny - 1) + 1)

    tok_copy = push(tokens, tok_in, pair_send.at[0], pair_recv.at[0], tp=other)
    own_block = pl.ds(pl.multiple_of(y * 128, 128), 128)

    def send_chunk(c):
        for d in near_y:
            to = (y + d) % ny
            push(
                w_own.at[to, c],
                w_flat.at[c, own_block],
                wy_send.at[c, d],
                wy_recv.at[c, y],
                y=to,
            )

    send_chunk(0)
    for copy in loads:
        copy.start()
    tok_copy.wait_recv()
    mine, theirs = tokens[...].astype(F32), tok_in[...].astype(F32)
    first = jnp.where(tp == 0, mine, theirs)
    second = jnp.where(tp == 0, theirs, mine)
    chip = jnp.concatenate([first, second], axis=0).T.astype(BF16)
    tok_all[y] = chip
    tok_half[0] = chip[:half]
    tok_half[1] = chip[half:]
    for d in near_y:
        push(
            tok_all.at[y], tok_all.at[y], ty_send.at[d], ty_recv.at[y], y=(y + d) % ny
        )
    for c in range(1, chunks):
        send_chunk(c)
    out_copy = push(w_out, wo_all.at[tp], pair_send.at[1], pair_recv.at[1], tp=other)
    up_copy = push(w_up, up_all.at[tp], pair_send.at[2], pair_recv.at[2], tp=other)
    down_copy = push(w_down, down_all.at[tp], pair_send.at[3], pair_recv.at[3], tp=other)
    for c in range(chunks):
        w_flat[c, own_block] = w_own[y, c]
    for d in near_y:
        s = (y + d) % ny
        remote(tok_all.at[s], tok_all.at[s], ty_send.at[d], ty_recv.at[s], y=s).wait_recv()
    squares = jnp.zeros((rows, 1), F32)
    scaled = []
    for s in range(ny):
        wide_rows = tok_all[s].astype(F32)
        squares = squares + jnp.sum(wide_rows * wide_rows, axis=1, keepdims=True)
        scaled.append((wide_rows * gains[0, pl.ds(z * ny + s, 1), :]).astype(BF16))
    x = jnp.concatenate(scaled, axis=1)
    loads[0].wait()
    loads[1].wait()
    gate = jnp.concatenate(
        [
            lax.dot_general(x, wig[...], contract, preferred_element_type=F32),
            lax.dot_general(x, wfg[...], contract, preferred_element_type=F32),
            jnp.broadcast_to(squares, (rows, 96)),
        ],
        axis=1,
    )
    for k in range(nz):
        gate_send[k] = gate[k * zrows : (k + 1) * zrows]
    for d in far_z:
        to = (z + d) % nz
        push(gate_send.at[to], gate_recv.at[z], gz_send.at[d], gz_recv.at[z], z=to)

    for c in range(chunks):
        for d in near_y:
            src = (y + d) % ny
            there = w_flat.at[c, pl.ds(pl.multiple_of(src * 128, 128), 128)]
            remote(there, there, wy_send.at[c, d], wy_recv.at[c, src], y=src).wait_recv()
        product = jnp.dot(x, w_flat[c], preferred_element_type=F32)
        for k in range(nz):
            part_send[c, k] = jnp.concatenate(
                [
                    product[k * zrows : (k + 1) * zrows, :128],
                    product[k * zrows : (k + 1) * zrows, 128:],
                ],
                axis=0,
            ).astype(BF16)
        for d in far_z:
            to = (z + d) % nz
            push(
                part_send.at[c, to], part_recv.at[c, z], pz_send.at[c, d], pz_recv.at[c, z], z=to
            )

    loads[2].wait()

    def split(i, carry):
        m_bh = mem[i]
        high = m_bh.astype(BF16)
        mem_split[i, :, :128] = high
        mem_split[i, :, 128:] = (m_bh - high.astype(F32)).astype(BF16)
        return carry

    lax.fori_loop(0, own * heads, split, 0)

    gate_sum = gate_send[z]
    for d in near_z:
        s = (z + d) % nz
        remote(gate_recv.at[s], gate_recv.at[s], gz_send.at[d], gz_recv.at[s], z=s).wait_recv()
        gate_sum = gate_sum + gate_recv[s]
    inverse = lax.rsqrt(gate_sum[:, 32:33] / width_full + EPS)
    gate_pre = inverse * gate_sum
    gate_rows = jnp.zeros((own, 128), F32)
    for k in range(ny):
        gate_rows = gate_rows + jnp.where(y == k, gate_pre[k * own : (k + 1) * own], 0.0)
    in_all = gate_rows[:, 0:16] + bias_in[...]
    forget_all = gate_rows[:, 16:32] + bias_forget[...]
    ingate = jnp.where(tp == 0, in_all[:, :8], in_all[:, 8:])
    forget_pre = jnp.where(tp == 0, forget_all[:, :8], forget_all[:, 8:])
    forget = jnp.minimum(forget_pre, 0.0) - jnp.log(1.0 + jnp.exp(-jnp.abs(forget_pre)))
    carried = forget + stabilizer[...]
    new_stab = jnp.maximum(carried, ingate)
    packed[4 * own * heads : 4 * own * heads + own, :heads] = new_stab
    diagonal = lax.broadcasted_iota(jnp.int32, (heads, heads), 0) == lax.broadcasted_iota(
        jnp.int32, (heads, heads), 1
    )

    def column(value):
        return jnp.concatenate(
            [
                jnp.sum(
                    jnp.where(diagonal, jnp.broadcast_to(value[b : b + 1], (heads, heads)), 0.0),
                    axis=1,
                    keepdims=True,
                )
                for b in range(own)
            ],
            axis=0,
        )

    retain = column(jnp.exp(carried - new_stab))
    inflow = column(jnp.exp(ingate - new_stab))
    floor = column(jnp.exp(-new_stab))

    for c in range(chunks):
        total = part_send[c, z].astype(F32)
        for d in near_z:
            src = (z + d) % nz
            there = part_recv.at[c, src]
            remote(there, there, pz_send.at[c, d], pz_recv.at[c, src], z=src).wait_recv()
            total = total + part_recv[c, src].astype(F32)
        for i in range(2):
            rows_wide[pl.ds(2 * c + i, zrows, stride=heads), :] = (
                inverse * total[i * zrows : (i + 1) * zrows]
            )
    piece = own * heads
    for k in range(ny):
        rows_send[k] = rows_wide[k * piece : (k + 1) * piece, :].astype(BF16)
    for d in near_y:
        to = (y + d) % ny
        push(rows_send.at[to], rows_recv.at[y], ry_send.at[d], ry_recv.at[y], y=to)
    rows_recv[y] = rows_send[y]
    for d in near_y:
        s = (y + d) % ny
        remote(rows_recv.at[s], rows_recv.at[s], ry_send.at[d], ry_recv.at[s], y=s).wait_recv()

    query = rows_recv[0].astype(F32)
    key = rows_recv[1].astype(F32) * 128**-0.5
    value = rows_recv[2].astype(F32)
    gate_o = rows_recv[3].astype(F32)
    q_twice[...] = jnp.concatenate([query, query], axis=1)
    new_norm = retain * normalizer[...] + inflow * key
    packed[3 * piece : 4 * piece] = new_norm
    inflow_value = inflow * value
    packed[:piece] = inflow_value
    packed[piece : 2 * piece] = key
    packed[2 * piece : 3 * piece] = jnp.broadcast_to(retain, (piece, 128))
    sub = lax.broadcasted_iota(jnp.int32, (heads, 128), 0)

    def readout_of(b, carry):
        here = pl.ds(pl.multiple_of(b * heads, heads), heads)
        q_b = q_twice[here, :].astype(BF16)
        found = jnp.zeros((heads, 128), F32)
        for h in range(heads):
            product = lax.dot_general(
                q_b, mem_split[b * heads + h], contract, preferred_element_type=F32
            )
            found = jnp.where(sub == h, product, found)
        mq[here, :] = found
        return carry

    lax.fori_loop(0, own, readout_of, 0)
    numerator = retain * mq[...] + inflow_value * jnp.sum(key * query, axis=1, keepdims=True)
    denominator = jnp.sum(new_norm * query, axis=1, keepdims=True)
    readout = numerator / jnp.maximum(jnp.abs(denominator), floor)
    centered = readout - jnp.mean(readout, axis=1, keepdims=True)
    normed = centered * lax.rsqrt(jnp.mean(centered * centered, axis=1, keepdims=True) + EPS)
    gain_all = head_gain[...].astype(F32)
    gain_own = jnp.where(tp == 0, gain_all[:heads], gain_all[heads:])
    heads_out = (
        normed * jnp.concatenate([gain_own] * own, axis=0) * (1.0 / (1.0 + jnp.exp(-gate_o)))
    ).astype(BF16)
    heads_own[...] = heads_out

    core = z // half_z
    zl = z % half_z

    @pl.when(tp == core)
    def _():
        heads_all[zl, tp, y] = heads_out

    for d in far_z:
        push(
            heads_own,
            heads_all.at[zl, tp, y],
            hz_send.at[d],
            hz_recv.at[zl, tp],
            z=(z + d) % nz,
            tp=core,
        )

    @pl.when(tp != core)
    def _():
        remote(
            heads_own, heads_all.at[zl, tp, y], hz_send.at[0], hz_recv.at[zl, tp], tp=other
        ).start()

    for k in range(half_z):
        for t in range(2):
            here = heads_all.at[k, t, y]
            source = tp * half_z + k

            @pl.when(jnp.logical_or(source != z, tp != t))
            def _():
                remote(here, here, hz_send.at[0], hz_recv.at[k, t], tp=other).wait_recv()

            for d in near_y:
                push(
                    here, here, hy_send.at[d, k, t], hy_recv.at[y, k, t], y=(y + d) % ny
                )
    for k in range(half_z):
        for t in range(2):
            for d in near_y:
                s = (y + d) % ny
                there = heads_all.at[k, t, s]
                remote(there, there, hy_send.at[d, k, t], hy_recv.at[s, k, t], y=s).wait_recv()
            for s in range(ny):
                start = t * half * heads + (k * ny + s) * piece
                heads_f32[start : start + piece, :] = heads_all[k, t, s].astype(F32)
    gathered = jnp.concatenate(
        [
            heads_f32[pl.ds(t * half * heads + h, half, stride=heads), :].astype(BF16)
            for t in range(2)
            for h in range(heads)
        ],
        axis=1,
    )
    loads[3].wait()
    out_copy.wait_recv()
    attended = jnp.dot(
        gathered, wo_all[...].reshape(2 * heads * 128, 128), preferred_element_type=F32
    )
    mixed = (tok_half[tp].astype(F32) + attended).astype(BF16)
    mixed_all[z, y] = mixed

    for d in near_z:
        push(
            mixed_all.at[z, y], mixed_all.at[z, y], mz_send.at[d], mz_recv.at[z], z=(z + d) % nz
        )
    for d in [0] + near_z:
        s = (z + d) % nz
        here = mixed_all.at[s, y]
        if d:
            remote(here, here, mz_send.at[d], mz_recv.at[s], z=s).wait_recv()
        for e in near_y:
            push(here, here, my_send.at[d, e], my_recv.at[y, s], y=(y + e) % ny)
    loads[4].wait()
    up_copy.wait_recv()
    hidden = up_all.shape[2]
    squares = jnp.zeros((half, 1), F32)
    for d in [0] + near_z:
        s = (z + d) % nz
        for e in near_y:
            src = (y + e) % ny
            there = mixed_all.at[s, src]
            remote(there, there, my_send.at[d, e], my_recv.at[src, s], y=src).wait_recv()
        scaled = []
        for k in range(ny):
            wide_rows = mixed_all[s, k].astype(F32)
            squares = squares + jnp.sum(wide_rows * wide_rows, axis=1, keepdims=True)
            scaled.append((wide_rows * gains[1, pl.ds(s * ny + k, 1), :]).astype(BF16))
        lhs = jnp.concatenate(scaled, axis=1)
        here = pl.ds(pl.multiple_of(s * block, block), block)
        for t in range(2):
            product = jnp.dot(lhs, up_all[t, here, :], preferred_element_type=F32)
            if d:
                product = product + acc[t]
            acc[t] = product
    inverse_mlp = lax.rsqrt(squares / width_full + EPS)
    squared = []
    for t in range(2):
        activation = jnp.maximum(inverse_mlp * acc[t], 0.0)
        squared.append((activation * activation).astype(BF16))

    loads[5].wait()
    down_copy.wait_recv()
    order = far_z + [0]
    for d in order:
        to = (z + d) % nz
        here = pl.ds(pl.multiple_of(to * block, block), block)
        product = jnp.dot(
            squared[0], down_all[0, :, here], preferred_element_type=F32
        ) + jnp.dot(squared[1], down_all[1, :, here], preferred_element_type=F32)
        for k in range(ny):
            down_send[to, k] = product[:, k * 128 : (k + 1) * 128].astype(BF16)
        for e in near_y:
            dst = (y + e) % ny
            push(down_send.at[to, dst], down_y.at[y, to], dy_send.at[d, e], dy_recv.at[y, to], y=dst)
    total = None
    for d in order:
        to = (z + d) % nz
        summed = down_send[to, y].astype(F32)
        for e in near_y:
            src = (y + e) % ny
            there = down_y.at[src, to]
            remote(there, there, dy_send.at[d, e], dy_recv.at[src, to], y=src).wait_recv()
            summed = summed + down_y[src, to].astype(F32)
        if d:
            sum_send[to] = summed.astype(BF16)
            push(sum_send.at[to], sum_recv.at[z], dz_send.at[d], dz_recv.at[z], z=to)
        else:
            total = summed
    for d in near_z:
        s = (z + d) % nz
        remote(sum_recv.at[s], sum_recv.at[s], dz_send.at[d], dz_recv.at[s], z=s).wait_recv()
        total = total + sum_recv[s].astype(F32)
    final = (mixed_all[z, y].astype(F32) + total).astype(BF16)
    fin_send[...] = final
    fin_copy = push(fin_send, fin_recv, pair_send.at[4], pair_recv.at[4], tp=other)
    fin_copy.wait_recv()
    mine, theirs = final.astype(F32), fin_recv[...].astype(F32)
    top = 4 * piece + 8
    packed[top : top + half] = jnp.where(tp == 0, mine, theirs)
    packed[top + half : top + rows] = jnp.where(tp == 0, theirs, mine)

    for copy in pending:
        copy.wait_send()
    @pl.when(tp != core)
    def _():
        remote(
            heads_own, heads_all.at[zl, tp, y], hz_send.at[0], hz_recv.at[zl, tp], tp=other
        ).wait_send()


def update(mem, packed, new_mem, out, norm, stab, made, sems):
    count = sems.shape[0]
    piece = mem.shape[0]
    each = piece // count
    inflow_v = packed[:piece].T
    copies = []
    for b in range(count):
        for i in range(b * each, (b + 1) * each):
            key, retain = packed[piece + i], packed[2 * piece + i]
            made[i] = retain[None] * mem[i] + inflow_v[:, i : i + 1] * key[None]
        here = pl.ds(b * each, each)
        copies.append(pltpu.make_async_copy(made.at[here], new_mem.at[here], sems.at[b]))
        copies[-1].start()
    norm[...] = packed[3 * piece : 4 * piece]
    stab[...] = packed[4 * piece : 4 * piece + stab.shape[0], : stab.shape[1]]
    turned = packed[4 * piece + 8 :].T
    first = lax.axis_index("tp") == 0
    out[...] = jnp.where(first, turned[:64], turned[64:]).astype(BF16)
    for copy in copies:
        copy.wait()


def body(
    tokens,
    gain_mixer,
    weight_query,
    weight_key,
    weight_value,
    weight_outgate,
    weight_ingate,
    weight_forget,
    bias_input,
    bias_forget,
    memory,
    normalizer,
    stabilizer,
    head_gain,
    weight_out,
    gain_channel,
    weight_up,
    weight_down,
):
    nz, ny = lax.axis_size("z"), lax.axis_size("y")
    own, heads, hd = memory.shape[:3]
    width_full = gain_mixer.shape[0]
    tokens = tokens.T
    rows = tokens.shape[1]
    half = rows // 2
    piece = own * heads
    zrows = ny * own
    block = ny * 128
    chunks = heads // 2
    dma = pltpu.SemaphoreType.DMA
    vmem = pl.BlockSpec(memory_space=pltpu.VMEM)
    hbm = pl.BlockSpec(memory_space=pl.ANY)
    mem48 = memory.reshape(piece, hd, hd)
    small = (
        tokens,
        gain_mixer.reshape(-1, 128),
        bias_input.reshape(1, -1),
        bias_forget.reshape(1, -1),
        normalizer.reshape(piece, hd),
        stabilizer,
        head_gain,
        gain_channel.reshape(-1, 128),
    )
    packed = pl.pallas_call(
        functools.partial(kernel, nz, ny, width_full),
        out_shape=jax.ShapeDtypeStruct((4 * piece + 8 + rows, hd), F32),
        in_specs=[hbm] * 18,
        out_specs=vmem,
        scratch_shapes=[pltpu.VMEM(value.shape, value.dtype) for value in small]
        + [
            pltpu.VMEM(tokens.shape, BF16),
            pltpu.VMEM((2, half, 128), BF16),
            pltpu.VMEM((ny, rows, 128), BF16),
            pltpu.VMEM((2, width_full // 128, 128), F32),
            pltpu.VMEM((16, block), BF16),
            pltpu.VMEM((16, block), BF16),
            pltpu.VMEM((piece, hd, hd), F32),
            pltpu.VMEM((piece, hd, 2 * hd), BF16),
            pltpu.VMEM((ny, 128, heads, hd), BF16),
            pltpu.VMEM((128 * heads, hd), F32),
            pltpu.VMEM((ny, chunks, 128, 2 * hd), BF16),
            pltpu.VMEM((chunks, block, 2 * hd), BF16),
            pltpu.VMEM((chunks, nz, 2 * zrows, hd), BF16),
            pltpu.VMEM((chunks, nz, 2 * zrows, hd), BF16),
            pltpu.VMEM((nz, zrows, 128), F32),
            pltpu.VMEM((nz, zrows, 128), F32),
            pltpu.VMEM((zrows * heads, hd), F32),
            pltpu.VMEM((ny, piece, hd), BF16),
            pltpu.VMEM((ny, piece, hd), BF16),
            pltpu.VMEM((piece, 2 * hd), F32),
            pltpu.VMEM((piece, hd), F32),
            pltpu.VMEM((piece, hd), BF16),
            pltpu.VMEM((nz // 2, 2, ny, piece, hd), BF16),
            pltpu.VMEM((2 * half * heads, hd), F32),
            pltpu.VMEM((2, heads * hd, 128), BF16),
            pltpu.VMEM((2, *weight_up.shape), BF16),
            pltpu.VMEM((2, *weight_down.shape), BF16),
            pltpu.VMEM((nz, ny, half, 128), BF16),
            pltpu.VMEM((2, half, weight_up.shape[1]), F32),
            pltpu.VMEM((nz, ny, half, 128), BF16),
            pltpu.VMEM((ny, nz, half, 128), BF16),
            pltpu.VMEM((nz, half, 128), BF16),
            pltpu.VMEM((nz, half, 128), BF16),
            pltpu.VMEM((half, 128), BF16),
            pltpu.VMEM((half, 128), BF16),
            dma((8,)),
            dma((10,)),
            dma((5,)),
            dma((5,)),
            dma((chunks, ny)),
            dma((chunks, ny)),
            dma((ny,)),
            dma((ny,)),
            dma((chunks, nz)),
            dma((chunks, nz)),
            dma((nz,)),
            dma((nz,)),
            dma((ny,)),
            dma((ny,)),
            dma((nz,)),
            dma((nz // 2, 2)),
            dma((ny, nz // 2, 2)),
            dma((ny, nz // 2, 2)),
            dma((nz,)),
            dma((nz,)),
            dma((nz, ny)),
            dma((ny, nz)),
            dma((nz, ny)),
            dma((ny, nz)),
            dma((nz,)),
            dma((nz,)),
        ],
        compiler_params=pltpu.CompilerParams(
            collective_id=0, has_side_effects=True, vmem_limit_bytes=56 * 1024 * 1024
        ),
    )(
        *small,
        weight_query,
        weight_key,
        weight_value,
        weight_outgate,
        weight_ingate.T,
        weight_forget.T,
        mem48,
        weight_out,
        weight_up,
        weight_down,
    )
    new_memory, layer_out, new_norm, new_stab = pl.pallas_call(
        update,
        out_shape=(
            jax.ShapeDtypeStruct(mem48.shape, F32),
            jax.ShapeDtypeStruct(tokens.shape, BF16),
            jax.ShapeDtypeStruct((piece, hd), F32),
            jax.ShapeDtypeStruct((own, heads), F32),
        ),
        in_specs=[vmem] * 2,
        out_specs=(hbm, vmem, vmem, vmem),
        scratch_shapes=[pltpu.VMEM(mem48.shape, F32), dma((own,))],
        compiler_params=pltpu.CompilerParams(vmem_limit_bytes=16 * 1024 * 1024),
    )(mem48, packed)
    new_memory = new_memory.reshape(memory.shape)
    return (layer_out.T, new_memory, new_norm.reshape(normalizer.shape), new_stab)


def solution(mesh):
    kv = mesh.shape["kv"]
    ny = 4
    torus = Mesh(
        mesh.devices.reshape(mesh.shape["dp"], kv // ny, ny, mesh.shape["tp"]),
        ("dp", "z", "y", "tp"),
    )
    placed = (
        P("dp", KV_TP),
        P(),
        P(KV, "tp", None),
        P(KV, "tp", None),
        P(KV, "tp", None),
        P(KV, "tp", None),
        P(),
        P(),
        P(),
        P(),
        P(DP_KV, "tp", None, None),
        P(DP_KV, "tp", None),
        P(DP_KV, "tp"),
        P(),
        P("tp", KV),
        P(),
        P(None, KV_TP),
        P(KV_TP, None),
    )
    return jax.shard_map(
        body,
        mesh=torus,
        in_specs=placed,
        out_specs=(
            P("dp", KV_TP),
            P(DP_KV, "tp", None, None),
            P(DP_KV, "tp", None),
            P(DP_KV, "tp"),
        ),
        check_vma=False,
    )
```

```python
import functools

import jax
import jax.numpy as jnp
from jax import lax
from jax.experimental import pallas as pl
from jax.experimental.pallas import tpu as pltpu
from jax.sharding import Mesh
from jax.sharding import PartitionSpec as P

EPS = 1e-06
KV_TP = ("z", "y", "tp")
KV = ("z", "y")
DP_KV = ("dp", "z", "y")
MESH = pl.DeviceIdType.MESH
PHASES = WY, TY, PZ, GZ, RY, HZ, OY, OX, OP, MZ, MY, DY, DZ = range(13)
F32 = jnp.float32
BF16 = jnp.bfloat16


def by_distance(n):
    return sorted(range(1, n), key=lambda d: (min(d, n - d), d))


def kernel(
    nx,
    nz,
    ny,
    width_full,
    tokens_hbm,
    gain_mixer_hbm,
    bias_in_hbm,
    bias_forget_hbm,
    normalizer_hbm,
    stabilizer_hbm,
    head_gain_hbm,
    gain_channel_hbm,
    w0,
    w1,
    w2,
    w3,
    w_in,
    w_forget,
    memory,
    w_out,
    w_up,
    w_down,
    packed,
    tokens,
    gain_mixer,
    bias_in,
    bias_forget,
    normalizer,
    stabilizer,
    head_gain,
    gain_channel,
    tok_in,
    tok_all,
    residual,
    gains,
    wig,
    wfg,
    mem,
    mem_split,
    w_raw,
    wide,
    w_own,
    w_flat,
    part_send,
    part_recv,
    gate_send,
    gate_recv,
    rows_wide,
    rows_send,
    rows_recv,
    q_twice,
    mq,
    heads_own,
    heads_all,
    heads_f32,
    wo_all,
    up_all,
    down_all,
    mixed_all,
    acc,
    down_send,
    down_y,
    sum_send,
    sum_recv,
    fin_send,
    fin_recv,
    small_sem,
    local_sem,
    pair_send,
    pair_recv,
    sent,
    arrived,
    wy_recv,
    pz_recv,
    mz_recv,
    my_recv,
    dy_recv,
):
    x_rank = lax.axis_index("dp")
    z = lax.axis_index("z")
    y = lax.axis_index("y")
    tp = lax.axis_index("tp")
    other = 1 - tp
    half_z = nz // 2
    rows = tokens.shape[1]
    half = rows // 2
    own = 6
    heads = 8
    zrows = ny * own
    block = ny * 128
    near_z = by_distance(nz)
    near_y = by_distance(ny)
    near_x = by_distance(nx)
    far_z = near_z[::-1]
    contract = (((1,), (1,)), ((), ()))

    def remote(src, dst, send, recv, **to):
        return pltpu.make_async_remote_copy(
            src_ref=src, dst_ref=dst, send_sem=send, recv_sem=recv, device_id=to, device_id_type=MESH
        )

    def push(*args, **to):
        copy = remote(*args, **to)
        copy.start()
        return copy

    def await_sent(ref, sem):
        remote(ref, ref, sem, sem, tp=other).wait_send()

    def await_all(ref, sem):
        remote(ref, ref, sem, sem, tp=other).wait_recv()

    barrier = pltpu.get_barrier_semaphore()
    for d in near_z:
        for t in range(2):
            pl.semaphore_signal(
                barrier, inc=1, device_id={"z": (z + d) % nz, "tp": t}, device_id_type=MESH
            )
    for d in near_y:
        pl.semaphore_signal(barrier, inc=1, device_id={"y": (y + d) % ny}, device_id_type=MESH)
    for d in near_x:
        pl.semaphore_signal(barrier, inc=1, device_id={"dp": (x_rank + d) % nx}, device_id_type=MESH)
    pl.semaphore_signal(barrier, inc=1, device_id={"tp": other}, device_id_type=MESH)

    depth = heads * 128

    def out_columns(k):
        return pl.ds(pl.multiple_of(k * 128, 128), 128)

    rows_of_block = pl.ds(pl.multiple_of(z * block, block), block)
    loads = [
        pltpu.make_async_copy(w_in.at[:, rows_of_block], wig, local_sem.at[0]),
        pltpu.make_async_copy(w_forget.at[:, rows_of_block], wfg, local_sem.at[1]),
        pltpu.make_async_copy(memory, mem, local_sem.at[2]),
        pltpu.make_async_copy(w_out, wo_all.at[tp, :, out_columns(y)], local_sem.at[3]),
        pltpu.make_async_copy(w_up, up_all.at[tp], local_sem.at[4]),
        pltpu.make_async_copy(w_down, down_all.at[tp], local_sem.at[5]),
    ]
    raw_loads = [
        pltpu.make_async_copy(w, w_raw.at[m], local_sem.at[6 + m])
        for m, w in enumerate((w0, w1, w2, w3))
    ]
    small = [
        pltpu.make_async_copy(src, dst, small_sem.at[i])
        for i, (src, dst) in enumerate(
            (
                (tokens_hbm, tokens),
                (gain_mixer_hbm, gain_mixer),
                (bias_in_hbm, bias_in),
                (bias_forget_hbm, bias_forget),
                (normalizer_hbm, normalizer),
                (stabilizer_hbm, stabilizer),
                (head_gain_hbm, head_gain),
                (gain_channel_hbm, gain_channel),
            )
        )
    ]
    for copy in raw_loads + small:
        copy.start()
    chunks = heads // 2
    for m in range(4):
        raw_loads[m].wait()
        wide[...] = w_raw[m].astype(F32).reshape(128 * heads, 128)
        for h in range(heads):
            w_own[m, h // 2, :, (h % 2) * 128 : (h % 2 + 1) * 128] = wide[
                pl.ds(h, 128, stride=heads), :
            ].astype(BF16)
    for copy in small:
        copy.wait()
    gains[0] = gain_mixer[...].astype(F32)
    gains[1] = gain_channel[...].astype(F32)

    pl.semaphore_wait(barrier, 2 * (nz - 1) + (ny - 1) + (nx - 1) + 1)

    tok_copy = push(tokens, tok_in, pair_send.at[0], pair_recv.at[0], tp=other)
    own_block = pl.ds(pl.multiple_of(y * 128, 128), 128)

    def send_chunk(c):
        for d in near_y:
            to = (y + d) % ny
            push(
                w_own.at[to, c],
                w_flat.at[c, own_block],
                sent.at[WY],
                wy_recv.at[c],
                y=to,
            )

    send_chunk(0)
    for copy in loads:
        copy.start()
    tok_copy.wait_recv()
    mine, theirs = tokens[...].astype(F32), tok_in[...].astype(F32)
    first = jnp.where(tp == 0, mine, theirs)
    second = jnp.where(tp == 0, theirs, mine)
    chip = jnp.concatenate([first, second], axis=0).T.astype(BF16)
    tok_all[y] = chip
    for d in near_y:
        push(
            tok_all.at[y], tok_all.at[y], sent.at[TY], arrived.at[TY], y=(y + d) % ny
        )
    for c in range(1, chunks):
        send_chunk(c)
    share = pl.ds(pl.multiple_of(x_rank * (depth // nx), depth // nx), depth // nx)
    mine_out = wo_all.at[tp, share, out_columns(y)]
    for d in near_y:
        push(
            w_out.at[share], mine_out, sent.at[OY], arrived.at[OY], y=(y + d) % ny
        )
    own_out = wo_all.at[tp, :, out_columns(y)]
    out_copy = push(w_out, own_out, pair_send.at[1], pair_recv.at[1], tp=other)
    up_copy = push(w_up, up_all.at[tp], pair_send.at[2], pair_recv.at[2], tp=other)
    down_copy = push(w_down, down_all.at[tp], pair_send.at[3], pair_recv.at[3], tp=other)
    for c in range(chunks):
        w_flat[c, own_block] = w_own[y, c]
    await_all(tok_all.at[: ny - 1], arrived.at[TY])
    squares = jnp.zeros((rows, 1), F32)
    scaled = []
    for s in range(ny):
        wide_rows = tok_all[s].astype(F32)
        squares = squares + jnp.sum(wide_rows * wide_rows, axis=1, keepdims=True)
        scaled.append((wide_rows * gains[0, pl.ds(z * ny + s, 1), :]).astype(BF16))
    x = jnp.concatenate(scaled, axis=1)
    loads[0].wait()
    loads[1].wait()
    gate = jnp.concatenate(
        [
            lax.dot_general(x, wig[...], contract, preferred_element_type=F32),
            lax.dot_general(x, wfg[...], contract, preferred_element_type=F32),
            jnp.broadcast_to(squares, (rows, 96)),
        ],
        axis=1,
    )
    for k in range(nz):
        gate_send[k] = gate[k * zrows : (k + 1) * zrows]
    for d in far_z:
        to = (z + d) % nz
        push(gate_send.at[to], gate_recv.at[z], sent.at[GZ], arrived.at[GZ], z=to)

    for c in range(chunks):
        await_all(w_flat.at[c, : (ny - 1) * 128], wy_recv.at[c])
        product = jnp.dot(x, w_flat[c], preferred_element_type=F32)
        for k in range(nz):
            part_send[c, k] = jnp.concatenate(
                [
                    product[k * zrows : (k + 1) * zrows, :128],
                    product[k * zrows : (k + 1) * zrows, 128:],
                ],
                axis=0,
            ).astype(BF16)
        for d in far_z:
            to = (z + d) % nz
            push(
                part_send.at[c, to], part_recv.at[c, z], sent.at[PZ], pz_recv.at[c], z=to
            )

    loads[2].wait()

    def split(i, carry):
        m_bh = mem[i]
        high = m_bh.astype(BF16)
        mem_split[i, :, :128] = high
        mem_split[i, :, 128:] = (m_bh - high.astype(F32)).astype(BF16)
        return carry

    lax.fori_loop(0, own * heads, split, 0)

    at = lax.broadcasted_iota(jnp.int32, (half_z * own, rows), 0)
    row = at + tp * half + y * own
    for k in range(1, half_z):
        row = row + jnp.where(at >= k * own, zrows - own, 0)
    chosen = jnp.where(
        lax.broadcasted_iota(jnp.int32, (half_z * own, rows), 1) == row, 1.0, 0.0
    ).astype(BF16)
    residual[...] = jnp.dot(
        chosen,
        jnp.concatenate([tok_all[k] for k in range(ny)], axis=1),
        preferred_element_type=F32,
    )

    await_all(gate_recv.at[: nz - 1], arrived.at[GZ])
    gate_sum = gate_send[z]
    for d in near_z:
        gate_sum = gate_sum + gate_recv[(z + d) % nz]
    inverse = lax.rsqrt(gate_sum[:, 32:33] / width_full + EPS)
    gate_pre = inverse * gate_sum
    gate_rows = jnp.zeros((own, 128), F32)
    for k in range(ny):
        gate_rows = gate_rows + jnp.where(y == k, gate_pre[k * own : (k + 1) * own], 0.0)
    in_all = gate_rows[:, 0:16] + bias_in[...]
    forget_all = gate_rows[:, 16:32] + bias_forget[...]
    ingate = jnp.where(tp == 0, in_all[:, :8], in_all[:, 8:])
    forget_pre = jnp.where(tp == 0, forget_all[:, :8], forget_all[:, 8:])
    forget = jnp.minimum(forget_pre, 0.0) - jnp.log(1.0 + jnp.exp(-jnp.abs(forget_pre)))
    carried = forget + stabilizer[...]
    new_stab = jnp.maximum(carried, ingate)
    packed[4 * own * heads : 4 * own * heads + own, :heads] = new_stab
    diagonal = lax.broadcasted_iota(jnp.int32, (heads, heads), 0) == lax.broadcasted_iota(
        jnp.int32, (heads, heads), 1
    )

    def column(value):
        return jnp.concatenate(
            [
                jnp.sum(
                    jnp.where(diagonal, jnp.broadcast_to(value[b : b + 1], (heads, heads)), 0.0),
                    axis=1,
                    keepdims=True,
                )
                for b in range(own)
            ],
            axis=0,
        )

    retain = column(jnp.exp(carried - new_stab))
    inflow = column(jnp.exp(ingate - new_stab))
    floor = column(jnp.exp(-new_stab))

    for c in range(chunks):
        if c == chunks - 1:
            await_all(wo_all.at[tp, share, : (ny - 1) * 128], arrived.at[OY])
            for d in near_y:
                there = wo_all.at[tp, share, out_columns((y + d) % ny)]
                for e in near_x:
                    push(there, there, sent.at[OX], arrived.at[OX], dp=(x_rank + e) % nx)
        await_all(part_recv.at[c, : nz - 1], pz_recv.at[c])
        total = part_send[c, z].astype(F32)
        for d in near_z:
            src = (z + d) % nz
            total = total + part_recv[c, src].astype(F32)
        for i in range(2):
            rows_wide[pl.ds(2 * c + i, zrows, stride=heads), :] = (
                inverse * total[i * zrows : (i + 1) * zrows]
            )
    piece = own * heads
    for k in range(ny):
        rows_send[k] = rows_wide[k * piece : (k + 1) * piece, :].astype(BF16)
    for d in near_y:
        to = (y + d) % ny
        push(rows_send.at[to], rows_recv.at[y], sent.at[RY], arrived.at[RY], y=to)
    rows_recv[y] = rows_send[y]
    await_all(rows_recv.at[: ny - 1], arrived.at[RY])

    query = rows_recv[0].astype(F32)
    key = rows_recv[1].astype(F32) * 128**-0.5
    value = rows_recv[2].astype(F32)
    gate_o = rows_recv[3].astype(F32)
    q_twice[...] = jnp.concatenate([query, query], axis=1)
    new_norm = retain * normalizer[...] + inflow * key
    packed[3 * piece : 4 * piece] = new_norm
    inflow_value = inflow * value
    packed[:piece] = inflow_value
    packed[piece : 2 * piece] = key
    packed[2 * piece : 3 * piece] = jnp.broadcast_to(retain, (piece, 128))
    sub = lax.broadcasted_iota(jnp.int32, (heads, 128), 0)

    def readout_of(b, carry):
        here = pl.ds(pl.multiple_of(b * heads, heads), heads)
        q_b = q_twice[here, :].astype(BF16)
        found = jnp.zeros((heads, 128), F32)
        for h in range(heads):
            product = lax.dot_general(
                q_b, mem_split[b * heads + h], contract, preferred_element_type=F32
            )
            found = jnp.where(sub == h, product, found)
        mq[here, :] = found
        return carry

    lax.fori_loop(0, own, readout_of, 0)
    numerator = retain * mq[...] + inflow_value * jnp.sum(key * query, axis=1, keepdims=True)
    denominator = jnp.sum(new_norm * query, axis=1, keepdims=True)
    readout = numerator / jnp.maximum(jnp.abs(denominator), floor)
    centered = readout - jnp.mean(readout, axis=1, keepdims=True)
    normed = centered * lax.rsqrt(jnp.mean(centered * centered, axis=1, keepdims=True) + EPS)
    gain_all = head_gain[...].astype(F32)
    gain_own = jnp.where(tp == 0, gain_all[:heads], gain_all[heads:])
    heads_out = (
        normed * jnp.concatenate([gain_own] * own, axis=0) * (1.0 / (1.0 + jnp.exp(-gate_o)))
    ).astype(BF16)
    heads_own[...] = heads_out

    core = z // half_z
    zl = z % half_z

    @pl.when(tp == core)
    def _():
        heads_all[2 * zl + tp] = heads_out

    for d in far_z:
        push(
            heads_own,
            heads_all.at[2 * zl + tp],
            sent.at[HZ],
            arrived.at[HZ],
            z=(z + d) % nz,
            tp=core,
        )

    @pl.when(tp != core)
    def _():
        push(heads_own, heads_all.at[2 * zl + tp], sent.at[HZ], arrived.at[HZ], tp=other)

    loads[3].wait()
    if nx > 1:
        passed_on = wo_all.at[tp, : depth // nx * (nx - 1), : (ny - 1) * 128]
        await_all(passed_on, arrived.at[OX])
    for d in near_y:
        whole = wo_all.at[tp, :, out_columns((y + d) % ny)]
        push(whole, whole, sent.at[OP], arrived.at[OP], tp=other)

    @pl.when(tp == core)
    def _():
        await_all(heads_all.at[: nz - 1], arrived.at[HZ])

    @pl.when(tp != core)
    def _():
        await_all(heads_all, arrived.at[HZ])

    for k in range(half_z):
        for t in range(2):
            start = (t * half_z + k) * piece
            heads_f32[start : start + piece, :] = heads_all[2 * k + t].astype(F32)
    mrows = half_z * own
    gathered = jnp.concatenate(
        [
            heads_f32[pl.ds(t * half_z * piece + h, mrows, stride=heads), :].astype(BF16)
            for t in range(2)
            for h in range(heads)
        ],
        axis=1,
    )
    out_copy.wait_recv()
    await_all(wo_all.at[other, :, : (ny - 1) * 128], arrived.at[OP])
    attended = jnp.dot(
        gathered, wo_all[...].reshape(2 * depth, block), preferred_element_type=F32
    )
    mixed = residual[...] + attended
    wcols = block // 2
    mixed_all[z, y] = jnp.concatenate([mixed[:, :wcols], mixed[:, wcols:]], axis=0).astype(BF16)

    for d in near_z:
        push(
            mixed_all.at[z, y], mixed_all.at[z, y], sent.at[MZ], mz_recv.at[z], z=(z + d) % nz
        )
    for d in [0] + near_z:
        s = (z + d) % nz
        here = mixed_all.at[s, y]
        if d:
            await_all(here, mz_recv.at[s])
        for e in near_y:
            push(here, here, sent.at[MY], my_recv.at[s], y=(y + e) % ny)
    loads[4].wait()
    up_copy.wait_recv()
    hidden = up_all.shape[2]
    squares = [jnp.zeros((mrows, 1), F32)] * ny
    for d in [0] + near_z:
        s = (z + d) % nz
        await_all(mixed_all.at[s, : ny - 1], my_recv.at[s])
        gain = jnp.concatenate([gains[1, pl.ds(s * ny + k, 1), :] for k in range(ny)], axis=1)
        scaled = []
        for k in range(ny):
            stacked = mixed_all[s, k].astype(F32)
            wide_rows = jnp.concatenate([stacked[:mrows], stacked[mrows:]], axis=1)
            squares[k] = squares[k] + jnp.sum(wide_rows * wide_rows, axis=1, keepdims=True)
            scaled.append(wide_rows * gain)
        lhs = jnp.concatenate(scaled, axis=0).astype(BF16)
        here = pl.ds(pl.multiple_of(s * block, block), block)
        for t in range(2):
            product = jnp.dot(lhs, up_all[t, here, :], preferred_element_type=F32)
            if d:
                product = product + acc[t]
            acc[t] = product
    inverse_mlp = lax.rsqrt(jnp.concatenate(squares, axis=0) / width_full + EPS)
    squared = []
    for t in range(2):
        activation = jnp.maximum(inverse_mlp * acc[t], 0.0)
        squared.append((activation * activation).astype(BF16))

    loads[5].wait()
    down_copy.wait_recv()
    order = far_z + [0]
    for d in order:
        to = (z + d) % nz
        here = pl.ds(pl.multiple_of(to * block, block), block)
        product = jnp.dot(
            squared[0], down_all[0, :, here], preferred_element_type=F32
        ) + jnp.dot(squared[1], down_all[1, :, here], preferred_element_type=F32)
        for k in range(ny):
            down_send[to, k] = product[:, k * 128 : (k + 1) * 128].astype(BF16)
        for e in near_y:
            dst = (y + e) % ny
            push(down_send.at[to, dst], down_y.at[y, to], sent.at[DY], dy_recv.at[to], y=dst)
    quarter = half // 2

    def columns_of(value, t):
        cols = value[:, 64 * t : 64 * (t + 1)]
        return jnp.concatenate([cols[:quarter], cols[quarter:]], axis=1)

    for d in order:
        to = (z + d) % nz
        await_all(down_y.at[: ny - 1, to], dy_recv.at[to])
        summed = down_send[to, y].astype(F32)
        for e in near_y:
            summed = summed + down_y[(y + e) % ny, to].astype(F32)
        if d:
            for t in range(2):
                sum_send[t, to] = columns_of(summed, t).astype(BF16)
                push(sum_send.at[t, to], sum_recv.at[tp, z], sent.at[DZ], arrived.at[DZ], z=to, tp=t)
        else:
            carried = []
            for k in range(ny):
                stacked = mixed_all[z, k].astype(F32)
                mine = jnp.zeros((mrows, 128), F32)
                for c in range(ny):
                    down, across = c // (ny // 2) * mrows, c % (ny // 2) * 128
                    mine = jnp.where(
                        y == c, stacked[down : down + mrows, across : across + 128], mine
                    )
                carried.append(mine)
            whole = summed + jnp.concatenate(carried, axis=0)
            fin_send[0] = columns_of(whole, 0)
            fin_send[1] = columns_of(whole, 1)
            fin_copy = push(
                fin_send.at[other], fin_recv, pair_send.at[4], pair_recv.at[4], tp=other
            )
    await_all(sum_recv.at[:, : nz - 1], arrived.at[DZ])
    total = [fin_send[tp], jnp.zeros((quarter, 128), F32)]
    for d in near_z:
        src = (z + d) % nz
        total[0] = total[0] + sum_recv[tp, src].astype(F32)
        total[1] = total[1] + sum_recv[other, src].astype(F32)
    fin_copy.wait_recv()
    total[1] = total[1] + fin_recv[...]
    top = 4 * piece + 8
    packed[top : top + quarter] = jnp.where(tp == 0, total[0], total[1])
    packed[top + quarter : top + half] = jnp.where(tp == 0, total[1], total[0])

    for copy in (tok_copy, out_copy, up_copy, down_copy, fin_copy):
        copy.wait_send()
    await_sent(w_own.at[: ny - 1], sent.at[WY])
    await_sent(tok_all.at[: ny - 1], sent.at[TY])
    await_sent(part_send.at[:, : nz - 1], sent.at[PZ])
    await_sent(gate_send.at[: nz - 1], sent.at[GZ])
    await_sent(rows_send.at[: ny - 1], sent.at[RY])
    await_sent(wo_all.at[tp, share, : (ny - 1) * 128], sent.at[OY])
    if nx > 1:
        await_sent(passed_on, sent.at[OX])
    await_sent(wo_all.at[tp, :, : (ny - 1) * 128], sent.at[OP])
    await_sent(mixed_all.at[: nz - 1, 0], sent.at[MZ])
    await_sent(mixed_all.at[:, : ny - 1], sent.at[MY])
    await_sent(down_send.at[:, : ny - 1], sent.at[DY])
    await_sent(sum_send.at[:, : nz - 1], sent.at[DZ])

    @pl.when(tp == core)
    def _():
        await_sent(heads_all.at[: nz - 1], sent.at[HZ])

    @pl.when(tp != core)
    def _():
        await_sent(heads_all, sent.at[HZ])


def update(ny, mem, packed, new_mem, out, norm, stab, made, sems):
    count = sems.shape[0]
    piece = mem.shape[0]
    each = piece // count
    inflow_v = packed[:piece].T
    copies = []
    for b in range(count):
        for i in range(b * each, (b + 1) * each):
            key, retain = packed[piece + i], packed[2 * piece + i]
            made[i] = retain[None] * mem[i] + inflow_v[:, i : i + 1] * key[None]
        here = pl.ds(b * each, each)
        copies.append(pltpu.make_async_copy(made.at[here], new_mem.at[here], sems.at[b]))
        copies[-1].start()
    norm[...] = packed[3 * piece : 4 * piece]
    stab[...] = packed[4 * piece : 4 * piece + stab.shape[0], : stab.shape[1]]
    rows = out.shape[1]
    own, blocks = stab.shape[0], rows // stab.shape[0] // 2
    per = blocks // ny
    quarter = rows // 4
    line = lax.broadcasted_iota(jnp.int32, (rows // 2, rows), 0).astype(F32)
    column = lax.broadcasted_iota(jnp.int32, (rows // 2, rows), 1).astype(F32)
    side = jnp.where(line >= quarter, 1.0, 0.0)
    result = packed[4 * piece + 8 :].T.astype(BF16)
    turned = jnp.zeros((64, rows), F32)
    for upper in range(2):
        at = line + side * quarter + upper * quarter
        group = jnp.floor((at + 0.5) / own)
        inner = group - side * blocks
        in_y = jnp.floor((inner + 0.5) / per)
        in_z = inner - in_y * per
        target = (side * blocks + in_z * ny + in_y) * own + (at - group * own)
        order = jnp.where(column == target, 1.0, 0.0).astype(BF16)
        turned = turned + jnp.dot(
            result[64 * upper : 64 * (upper + 1)], order, preferred_element_type=F32
        )
    out[...] = turned.astype(BF16)
    for copy in copies:
        copy.wait()


def body(
    tokens,
    gain_mixer,
    weight_query,
    weight_key,
    weight_value,
    weight_outgate,
    weight_ingate,
    weight_forget,
    bias_input,
    bias_forget,
    memory,
    normalizer,
    stabilizer,
    head_gain,
    weight_out,
    gain_channel,
    weight_up,
    weight_down,
):
    nx, nz, ny = lax.axis_size("dp"), lax.axis_size("z"), lax.axis_size("y")
    own, heads, hd = memory.shape[:3]
    width_full = gain_mixer.shape[0]
    tokens = tokens.T
    rows = tokens.shape[1]
    half = rows // 2
    piece = own * heads
    zrows = ny * own
    block = ny * 128
    chunks = heads // 2
    mrows = nz // 2 * own
    dma = pltpu.SemaphoreType.DMA
    vmem = pl.BlockSpec(memory_space=pltpu.VMEM)
    hbm = pl.BlockSpec(memory_space=pl.ANY)
    mem48 = memory.reshape(piece, hd, hd)
    small = (
        tokens,
        gain_mixer.reshape(-1, 128),
        bias_input.reshape(1, -1),
        bias_forget.reshape(1, -1),
        normalizer.reshape(piece, hd),
        stabilizer,
        head_gain,
        gain_channel.reshape(-1, 128),
    )
    packed = pl.pallas_call(
        functools.partial(kernel, nx, nz, ny, width_full),
        out_shape=jax.ShapeDtypeStruct((4 * piece + 8 + half, hd), F32),
        in_specs=[hbm] * 18,
        out_specs=vmem,
        scratch_shapes=[pltpu.VMEM(value.shape, value.dtype) for value in small]
        + [
            pltpu.VMEM(tokens.shape, BF16),
            pltpu.VMEM((ny, rows, 128), BF16),
            pltpu.VMEM((mrows, block), F32),
            pltpu.VMEM((2, width_full // 128, 128), F32),
            pltpu.VMEM((16, block), BF16),
            pltpu.VMEM((16, block), BF16),
            pltpu.VMEM((piece, hd, hd), F32),
            pltpu.VMEM((piece, hd, 2 * hd), BF16),
            pltpu.VMEM((ny, 128, heads, hd), BF16),
            pltpu.VMEM((128 * heads, hd), F32),
            pltpu.VMEM((ny, chunks, 128, 2 * hd), BF16),
            pltpu.VMEM((chunks, block, 2 * hd), BF16),
            pltpu.VMEM((chunks, nz, 2 * zrows, hd), BF16),
            pltpu.VMEM((chunks, nz, 2 * zrows, hd), BF16),
            pltpu.VMEM((nz, zrows, 128), F32),
            pltpu.VMEM((nz, zrows, 128), F32),
            pltpu.VMEM((zrows * heads, hd), F32),
            pltpu.VMEM((ny, piece, hd), BF16),
            pltpu.VMEM((ny, piece, hd), BF16),
            pltpu.VMEM((piece, 2 * hd), F32),
            pltpu.VMEM((piece, hd), F32),
            pltpu.VMEM((piece, hd), BF16),
            pltpu.VMEM((nz, piece, hd), BF16),
            pltpu.VMEM((nz * piece, hd), F32),
            pltpu.VMEM((2, heads * hd, block), BF16),
            pltpu.VMEM((2, *weight_up.shape), BF16),
            pltpu.VMEM((2, *weight_down.shape), BF16),
            pltpu.VMEM((nz, ny, 2 * mrows, block // 2), BF16),
            pltpu.VMEM((2, half, weight_up.shape[1]), F32),
            pltpu.VMEM((nz, ny, half, 128), BF16),
            pltpu.VMEM((ny, nz, half, 128), BF16),
            pltpu.VMEM((2, nz, half // 2, 128), BF16),
            pltpu.VMEM((2, nz, half // 2, 128), BF16),
            pltpu.VMEM((2, half // 2, 128), F32),
            pltpu.VMEM((half // 2, 128), F32),
            dma((8,)),
            dma((10,)),
            dma((5,)),
            dma((5,)),
            dma((len(PHASES),)),
            dma((len(PHASES),)),
            dma((chunks,)),
            dma((chunks,)),
            dma((nz,)),
            dma((nz,)),
            dma((nz,)),
        ],
        compiler_params=pltpu.CompilerParams(
            collective_id=0, has_side_effects=True, vmem_limit_bytes=56 * 1024 * 1024
        ),
    )(
        *small,
        weight_query,
        weight_key,
        weight_value,
        weight_outgate,
        weight_ingate.T,
        weight_forget.T,
        mem48,
        weight_out,
        weight_up,
        weight_down,
    )
    new_memory, layer_out, new_norm, new_stab = pl.pallas_call(
        functools.partial(update, ny),
        out_shape=(
            jax.ShapeDtypeStruct(mem48.shape, F32),
            jax.ShapeDtypeStruct(tokens.shape, BF16),
            jax.ShapeDtypeStruct((piece, hd), F32),
            jax.ShapeDtypeStruct((own, heads), F32),
        ),
        in_specs=[vmem] * 2,
        out_specs=(hbm, vmem, vmem, vmem),
        scratch_shapes=[pltpu.VMEM(mem48.shape, F32), dma((own,))],
        compiler_params=pltpu.CompilerParams(vmem_limit_bytes=16 * 1024 * 1024),
    )(mem48, packed)
    new_memory = new_memory.reshape(memory.shape)
    return (layer_out.T, new_memory, new_norm.reshape(normalizer.shape), new_stab)


def solution(mesh):
    kv = mesh.shape["kv"]
    ny = 4
    torus = Mesh(
        mesh.devices.reshape(mesh.shape["dp"], kv // ny, ny, mesh.shape["tp"]),
        ("dp", "z", "y", "tp"),
    )
    placed = (
        P("dp", KV_TP),
        P(),
        P(KV, "tp", None),
        P(KV, "tp", None),
        P(KV, "tp", None),
        P(KV, "tp", None),
        P(),
        P(),
        P(),
        P(),
        P(DP_KV, "tp", None, None),
        P(DP_KV, "tp", None),
        P(DP_KV, "tp"),
        P(),
        P("tp", KV),
        P(),
        P(None, KV_TP),
        P(KV_TP, None),
    )
    return jax.shard_map(
        body,
        mesh=torus,
        in_specs=placed,
        out_specs=(
            P("dp", KV_TP),
            P(DP_KV, "tp", None, None),
            P(DP_KV, "tp", None),
            P(DP_KV, "tp"),
        ),
        check_vma=False,
    )
```

```python
import functools

import jax
import jax.numpy as jnp
from jax import lax
from jax.experimental import pallas as pl
from jax.experimental.pallas import tpu as pltpu
from jax.sharding import Mesh
from jax.sharding import PartitionSpec as P

EPS = 1e-06
KV_TP = ("z", "y", "tp")
KV = ("z", "y")
DP_KV = ("dp", "z", "y")
MESH = pl.DeviceIdType.MESH
PHASES = WY, WQ, WX, TY, PZ, GZ, RY, HZ, OY, OX, OD, OP, MZ, MN, MY, DN, DY, DZ = range(18)
F32 = jnp.float32
BF16 = jnp.bfloat16


def by_distance(n):
    return sorted(range(1, n), key=lambda d: (min(d, n - d), d))


def kernel(
    nx,
    nz,
    ny,
    width_full,
    tokens_hbm,
    gain_mixer_hbm,
    bias_in_hbm,
    bias_forget_hbm,
    normalizer_hbm,
    stabilizer_hbm,
    head_gain_hbm,
    gain_channel_hbm,
    w0,
    w1,
    w2,
    w3,
    w_in,
    w_forget,
    memory,
    w_out,
    w_up,
    w_down,
    packed,
    tokens,
    gain_mixer,
    bias_in,
    bias_forget,
    normalizer,
    stabilizer,
    head_gain,
    gain_channel,
    tok_in,
    tok_all,
    residual,
    gains,
    wig,
    wfg,
    mem,
    mem_split,
    w_raw,
    wide,
    w_own,
    w_flat,
    part_send,
    part_recv,
    gate_send,
    gate_recv,
    rows_wide,
    rows_send,
    rows_recv,
    q_twice,
    mq,
    heads_own,
    heads_all,
    heads_f32,
    wo_all,
    up_all,
    down_all,
    mixed_all,
    acc,
    down_send,
    down_own,
    down_next,
    down_y,
    sum_send,
    sum_recv,
    fin_send,
    fin_recv,
    small_sem,
    local_sem,
    pair_send,
    pair_recv,
    sent,
    arrived,
    wy_recv,
    pz_recv,
    mz_recv,
    my_recv,
    dy_recv,
):
    x_rank = lax.axis_index("dp")
    z = lax.axis_index("z")
    y = lax.axis_index("y")
    tp = lax.axis_index("tp")
    other = 1 - tp
    half_z = nz // 2
    rows = tokens.shape[1]
    half = rows // 2
    own = 6
    heads = 8
    zrows = ny * own
    block = ny * 128
    near_z = by_distance(nz)
    near_y = by_distance(ny)
    near_x = by_distance(nx)
    far_z = near_z[::-1]
    next_z = [d for d in near_z if min(d, nz - d) == 1]
    rest_z = [d for d in near_z if d not in next_z]
    contract = (((1,), (1,)), ((), ()))

    def remote(src, dst, send, recv, **to):
        return pltpu.make_async_remote_copy(
            src_ref=src, dst_ref=dst, send_sem=send, recv_sem=recv, device_id=to, device_id_type=MESH
        )

    def push(*args, **to):
        copy = remote(*args, **to)
        copy.start()
        return copy

    def await_sent(ref, sem):
        remote(ref, ref, sem, sem, tp=other).wait_send()

    def await_all(ref, sem):
        remote(ref, ref, sem, sem, tp=other).wait_recv()

    barrier = pltpu.get_barrier_semaphore()
    for d in near_z:
        for t in range(2):
            pl.semaphore_signal(
                barrier, inc=1, device_id={"z": (z + d) % nz, "tp": t}, device_id_type=MESH
            )
    for d in near_y:
        pl.semaphore_signal(barrier, inc=1, device_id={"y": (y + d) % ny}, device_id_type=MESH)
    for d in near_x:
        pl.semaphore_signal(barrier, inc=1, device_id={"dp": (x_rank + d) % nx}, device_id_type=MESH)
    pl.semaphore_signal(barrier, inc=1, device_id={"tp": other}, device_id_type=MESH)

    depth = heads * 128

    def out_columns(k):
        return pl.ds(pl.multiple_of(k * 128, 128), 128)

    rows_of_block = pl.ds(pl.multiple_of(z * block, block), block)
    loads = [
        pltpu.make_async_copy(w_in.at[:, rows_of_block], wig, local_sem.at[0]),
        pltpu.make_async_copy(w_forget.at[:, rows_of_block], wfg, local_sem.at[1]),
        pltpu.make_async_copy(memory, mem, local_sem.at[2]),
        pltpu.make_async_copy(w_out, wo_all.at[tp, :, out_columns(y)], local_sem.at[3]),
        pltpu.make_async_copy(w_up, up_all.at[tp], local_sem.at[4]),
        pltpu.make_async_copy(w_down, down_all.at[tp], local_sem.at[5]),
    ]
    raw_loads = [
        pltpu.make_async_copy(w, w_raw.at[m], local_sem.at[6 + m])
        for m, w in enumerate((w0, w1, w2, w3))
    ]
    small = [
        pltpu.make_async_copy(src, dst, small_sem.at[i])
        for i, (src, dst) in enumerate(
            (
                (tokens_hbm, tokens),
                (gain_mixer_hbm, gain_mixer),
                (bias_in_hbm, bias_in),
                (bias_forget_hbm, bias_forget),
                (normalizer_hbm, normalizer),
                (stabilizer_hbm, stabilizer),
                (head_gain_hbm, head_gain),
                (gain_channel_hbm, gain_channel),
            )
        )
    ]
    for copy in raw_loads + small:
        copy.start()
    chunks = heads // 2
    for m in range(4):
        raw_loads[m].wait()
        wide[...] = w_raw[m].astype(F32).reshape(128 * heads, 128)
        for h in range(heads):
            w_own[m, h // 2, :, (h % 2) * 128 : (h % 2 + 1) * 128] = wide[
                pl.ds(h, 128, stride=heads), :
            ].astype(BF16)
    for copy in small:
        copy.wait()
    gains[0] = gain_mixer[...].astype(F32)
    gains[1] = gain_channel[...].astype(F32)

    pl.semaphore_wait(barrier, 2 * (nz - 1) + (ny - 1) + (nx - 1) + 1)

    tok_copy = push(tokens, tok_in, pair_send.at[0], pair_recv.at[0], tp=other)
    own_block = pl.ds(pl.multiple_of(y * 128, 128), 128)

    def send_chunk(c):
        for d in near_y:
            to = (y + d) % ny
            push(
                w_own.at[to, c],
                w_flat.at[c, own_block],
                sent.at[WY],
                wy_recv.at[c],
                y=to,
            )

    last = chunks - 1
    some = 128 // nx

    def share_of(k):
        return pl.ds(pl.multiple_of(k * 128 + x_rank * some, some), some)

    send_chunk(0)
    for d in near_y:
        to = (y + d) % ny
        push(
            w_own.at[to, last, share_of(0)],
            w_flat.at[last, share_of(y)],
            sent.at[WQ],
            arrived.at[WQ],
            y=to,
        )
    for copy in loads:
        copy.start()
    tok_copy.wait_recv()
    mine, theirs = tokens[...].astype(F32), tok_in[...].astype(F32)
    first = jnp.where(tp == 0, mine, theirs)
    second = jnp.where(tp == 0, theirs, mine)
    chip = jnp.concatenate([first, second], axis=0).T.astype(BF16)
    tok_all[y] = chip
    for d in near_y:
        push(
            tok_all.at[y], tok_all.at[y], sent.at[TY], arrived.at[TY], y=(y + d) % ny
        )
    for c in range(1, last):
        send_chunk(c)
    direct = depth // 2
    part = (depth - direct) // nx
    share = pl.ds(pl.multiple_of(direct + x_rank * part, part), part)
    for d in near_y:
        to = (y + d) % ny
        push(w_out.at[share], wo_all.at[tp, share, out_columns(y)], sent.at[OY], arrived.at[OY], y=to)
    head = pl.ds(0, direct)
    for d in near_y:
        to = (y + d) % ny
        push(w_out.at[head], wo_all.at[tp, head, out_columns(y)], sent.at[OD], arrived.at[OD], y=to)
    own_out = wo_all.at[tp, :, out_columns(y)]
    out_copy = push(w_out, own_out, pair_send.at[1], pair_recv.at[1], tp=other)
    for c in range(chunks):
        w_flat[c, own_block] = w_own[y, c]
    await_all(w_flat.at[last, : (ny - 1) * some], arrived.at[WQ])
    for d in near_y:
        there = w_flat.at[last, share_of((y + d) % ny)]
        for e in near_x:
            push(there, there, sent.at[WX], arrived.at[WX], dp=(x_rank + e) % nx)
    await_all(tok_all.at[: ny - 1], arrived.at[TY])
    x = jnp.concatenate(
        [
            (tok_all[s].astype(F32) * gains[0, pl.ds(z * ny + s, 1), :]).astype(BF16)
            for s in range(ny)
        ],
        axis=1,
    )

    def project(c):
        product = jnp.dot(x, w_flat[c], preferred_element_type=F32)
        for k in range(nz):
            part_send[c, k] = jnp.concatenate(
                [
                    product[k * zrows : (k + 1) * zrows, :128],
                    product[k * zrows : (k + 1) * zrows, 128:],
                ],
                axis=0,
            ).astype(BF16)
        for d in far_z:
            to = (z + d) % nz
            push(
                part_send.at[c, to], part_recv.at[c, z], sent.at[PZ], pz_recv.at[c], z=to
            )

    await_all(w_flat.at[0, : (ny - 1) * 128], wy_recv.at[0])
    project(0)
    squares = jnp.zeros((rows, 1), F32)
    for s in range(ny):
        wide_rows = tok_all[s].astype(F32)
        squares = squares + jnp.sum(wide_rows * wide_rows, axis=1, keepdims=True)
    loads[0].wait()
    loads[1].wait()
    gate = jnp.concatenate(
        [
            lax.dot_general(x, wig[...], contract, preferred_element_type=F32),
            lax.dot_general(x, wfg[...], contract, preferred_element_type=F32),
            jnp.broadcast_to(squares, (rows, 96)),
        ],
        axis=1,
    )
    for k in range(nz):
        gate_send[k] = gate[k * zrows : (k + 1) * zrows]
    for d in far_z:
        to = (z + d) % nz
        push(gate_send.at[to], gate_recv.at[z], sent.at[GZ], arrived.at[GZ], z=to)

    if nx > 1:
        shared = w_flat.at[last, : (ny - 1) * (nx - 1) * some]
        await_all(shared, arrived.at[WX])
    project(last)
    for c in range(1, last):
        await_all(w_flat.at[c, : (ny - 1) * 128], wy_recv.at[c])
        project(c)

    await_all(wo_all.at[tp, share, : (ny - 1) * 128], arrived.at[OY])
    for d in near_y:
        there = wo_all.at[tp, share, out_columns((y + d) % ny)]
        for e in near_x:
            push(there, there, sent.at[OX], arrived.at[OX], dp=(x_rank + e) % nx)
    up_copy = push(w_up, up_all.at[tp], pair_send.at[2], pair_recv.at[2], tp=other)
    down_copy = push(w_down, down_all.at[tp], pair_send.at[3], pair_recv.at[3], tp=other)

    loads[2].wait()

    def split(i, carry):
        m_bh = mem[i]
        high = m_bh.astype(BF16)
        mem_split[i, :, :128] = high
        mem_split[i, :, 128:] = (m_bh - high.astype(F32)).astype(BF16)
        return carry

    lax.fori_loop(0, own * heads, split, 0)

    at = lax.broadcasted_iota(jnp.int32, (half_z * own, rows), 0)
    row = at + tp * half + y * own
    for k in range(1, half_z):
        row = row + jnp.where(at >= k * own, zrows - own, 0)
    chosen = jnp.where(
        lax.broadcasted_iota(jnp.int32, (half_z * own, rows), 1) == row, 1.0, 0.0
    ).astype(BF16)
    residual[...] = jnp.dot(
        chosen,
        jnp.concatenate([tok_all[k] for k in range(ny)], axis=1),
        preferred_element_type=F32,
    )

    await_all(gate_recv.at[: nz - 1], arrived.at[GZ])
    gate_sum = gate_send[z]
    for d in near_z:
        gate_sum = gate_sum + gate_recv[(z + d) % nz]
    inverse = lax.rsqrt(gate_sum[:, 32:33] / width_full + EPS)
    gate_pre = inverse * gate_sum
    gate_rows = jnp.zeros((own, 128), F32)
    for k in range(ny):
        gate_rows = gate_rows + jnp.where(y == k, gate_pre[k * own : (k + 1) * own], 0.0)
    in_all = gate_rows[:, 0:16] + bias_in[...]
    forget_all = gate_rows[:, 16:32] + bias_forget[...]
    ingate = jnp.where(tp == 0, in_all[:, :8], in_all[:, 8:])
    forget_pre = jnp.where(tp == 0, forget_all[:, :8], forget_all[:, 8:])
    forget = jnp.minimum(forget_pre, 0.0) - jnp.log(1.0 + jnp.exp(-jnp.abs(forget_pre)))
    carried = forget + stabilizer[...]
    new_stab = jnp.maximum(carried, ingate)
    packed[4 * own * heads : 4 * own * heads + own, :heads] = new_stab
    diagonal = lax.broadcasted_iota(jnp.int32, (heads, heads), 0) == lax.broadcasted_iota(
        jnp.int32, (heads, heads), 1
    )

    def column(value):
        return jnp.concatenate(
            [
                jnp.sum(
                    jnp.where(diagonal, jnp.broadcast_to(value[b : b + 1], (heads, heads)), 0.0),
                    axis=1,
                    keepdims=True,
                )
                for b in range(own)
            ],
            axis=0,
        )

    retain = column(jnp.exp(carried - new_stab))
    inflow = column(jnp.exp(ingate - new_stab))
    floor = column(jnp.exp(-new_stab))

    for c in [0, last] + list(range(1, last)):
        await_all(part_recv.at[c, : nz - 1], pz_recv.at[c])
        total = part_send[c, z].astype(F32)
        for d in near_z:
            src = (z + d) % nz
            total = total + part_recv[c, src].astype(F32)
        for i in range(2):
            rows_wide[pl.ds(2 * c + i, zrows, stride=heads), :] = (
                inverse * total[i * zrows : (i + 1) * zrows]
            )
    piece = own * heads
    for k in range(ny):
        rows_send[k] = rows_wide[k * piece : (k + 1) * piece, :].astype(BF16)
    for d in near_y:
        to = (y + d) % ny
        push(rows_send.at[to], rows_recv.at[y], sent.at[RY], arrived.at[RY], y=to)
    rows_recv[y] = rows_send[y]
    await_all(rows_recv.at[: ny - 1], arrived.at[RY])

    query = rows_recv[0].astype(F32)
    key = rows_recv[1].astype(F32) * 128**-0.5
    value = rows_recv[2].astype(F32)
    gate_o = rows_recv[3].astype(F32)
    q_twice[...] = jnp.concatenate([query, query], axis=1)
    new_norm = retain * normalizer[...] + inflow * key
    packed[3 * piece : 4 * piece] = new_norm
    inflow_value = inflow * value
    packed[:piece] = inflow_value
    packed[piece : 2 * piece] = key
    packed[2 * piece : 3 * piece] = jnp.broadcast_to(retain, (piece, 128))
    sub = lax.broadcasted_iota(jnp.int32, (heads, 128), 0)

    for b in range(own):
        these = slice(b * heads, (b + 1) * heads)
        product = lax.dot_general(
            q_twice[these, :].astype(BF16),
            mem_split[these].reshape(heads * 128, 256),
            contract,
            preferred_element_type=F32,
        )
        found = product[:, :128]
        for h in range(1, heads):
            found = jnp.where(sub == h, product[:, h * 128 : (h + 1) * 128], found)
        mq[these, :] = found
    numerator = retain * mq[...] + inflow_value * jnp.sum(key * query, axis=1, keepdims=True)
    denominator = jnp.sum(new_norm * query, axis=1, keepdims=True)
    readout = numerator / jnp.maximum(jnp.abs(denominator), floor)
    centered = readout - jnp.mean(readout, axis=1, keepdims=True)
    normed = centered * lax.rsqrt(jnp.mean(centered * centered, axis=1, keepdims=True) + EPS)
    gain_all = head_gain[...].astype(F32)
    gain_own = jnp.where(tp == 0, gain_all[:heads], gain_all[heads:])
    heads_out = (
        normed * jnp.concatenate([gain_own] * own, axis=0) * (1.0 / (1.0 + jnp.exp(-gate_o)))
    ).astype(BF16)
    heads_own[...] = heads_out

    core = z // half_z
    zl = z % half_z

    @pl.when(tp == core)
    def _():
        heads_all[2 * zl + tp] = heads_out

    for d in far_z:
        push(
            heads_own,
            heads_all.at[2 * zl + tp],
            sent.at[HZ],
            arrived.at[HZ],
            z=(z + d) % nz,
            tp=core,
        )

    @pl.when(tp != core)
    def _():
        push(heads_own, heads_all.at[2 * zl + tp], sent.at[HZ], arrived.at[HZ], tp=other)

    loads[3].wait()
    if nx > 1:
        passed_on = wo_all.at[tp, : part * (nx - 1), : (ny - 1) * 128]
        await_all(passed_on, arrived.at[OX])
    await_all(wo_all.at[tp, head, : (ny - 1) * 128], arrived.at[OD])
    for d in near_y:
        whole = wo_all.at[tp, :, out_columns((y + d) % ny)]
        push(whole, whole, sent.at[OP], arrived.at[OP], tp=other)

    @pl.when(tp == core)
    def _():
        await_all(heads_all.at[: nz - 1], arrived.at[HZ])

    @pl.when(tp != core)
    def _():
        await_all(heads_all, arrived.at[HZ])

    for k in range(half_z):
        for t in range(2):
            start = (t * half_z + k) * piece
            heads_f32[start : start + piece, :] = heads_all[2 * k + t].astype(F32)
    mrows = half_z * own
    gathered = jnp.concatenate(
        [
            heads_f32[pl.ds(t * half_z * piece + h, mrows, stride=heads), :].astype(BF16)
            for t in range(2)
            for h in range(heads)
        ],
        axis=1,
    )
    out_copy.wait_recv()
    await_all(wo_all.at[other, :, : (ny - 1) * 128], arrived.at[OP])
    attended = jnp.dot(
        gathered, wo_all[...].reshape(2 * depth, block), preferred_element_type=F32
    )
    mixed = residual[...] + attended
    wcols = block // 2
    mixed_all[z, y] = jnp.concatenate([mixed[:, :wcols], mixed[:, wcols:]], axis=0).astype(BF16)

    mine_here = mixed_all.at[z, y]
    for e in near_y:
        push(mine_here, mine_here, sent.at[MY], my_recv.at[z], y=(y + e) % ny)
    for d in near_z:
        push(mine_here, mine_here, sent.at[MZ], mz_recv.at[z], z=(z + d) % nz)
    await_all(mixed_all.at[z, : ny - 1], my_recv.at[z])
    for e in near_y:
        there = mixed_all.at[z, (y + e) % ny]
        for d in next_z:
            push(there, there, sent.at[MN], mz_recv.at[z], z=(z + d) % nz)
    for d in rest_z:
        s = (z + d) % nz
        here = mixed_all.at[s, y]
        await_all(here, mz_recv.at[s])
        for e in near_y:
            push(here, here, sent.at[MY], my_recv.at[s], y=(y + e) % ny)
    loads[4].wait()
    up_copy.wait_recv()
    hidden = up_all.shape[2]
    squares = [jnp.zeros((mrows, 1), F32)] * ny
    for d in [0] + near_z:
        s = (z + d) % nz
        if d in next_z:
            await_all(mixed_all.at[s], mz_recv.at[s])
        elif d:
            await_all(mixed_all.at[s, : ny - 1], my_recv.at[s])
        gain = jnp.concatenate([gains[1, pl.ds(s * ny + k, 1), :] for k in range(ny)], axis=1)
        scaled = []
        for k in range(ny):
            stacked = mixed_all[s, k].astype(F32)
            wide_rows = jnp.concatenate([stacked[:mrows], stacked[mrows:]], axis=1)
            squares[k] = squares[k] + jnp.sum(wide_rows * wide_rows, axis=1, keepdims=True)
            scaled.append(wide_rows * gain)
        lhs = jnp.concatenate(scaled, axis=0).astype(BF16)
        here = pl.ds(pl.multiple_of(s * block, block), block)
        for t in range(2):
            product = jnp.dot(lhs, up_all[t, here, :], preferred_element_type=F32)
            if d:
                product = product + acc[t]
            acc[t] = product
    inverse_mlp = lax.rsqrt(jnp.concatenate(squares, axis=0) / width_full + EPS)
    squared = []
    for t in range(2):
        activation = jnp.maximum(inverse_mlp * acc[t], 0.0)
        squared.append((activation * activation).astype(BF16))

    loads[5].wait()
    down_copy.wait_recv()
    rest = rest_z[::-1]
    for d in next_z + rest + [0]:
        to = (z + d) % nz
        here = pl.ds(pl.multiple_of(to * block, block), block)
        product = jnp.dot(
            squared[0], down_all[0, :, here], preferred_element_type=F32
        ) + jnp.dot(squared[1], down_all[1, :, here], preferred_element_type=F32)
        for k in range(ny):
            piece_k = product[:, k * 128 : (k + 1) * 128]
            if d:
                down_send[to, k] = piece_k.astype(BF16)
            else:
                down_own[k] = piece_k
        if d in next_z:
            push(
                down_send.at[to],
                down_next.at[next_z.index(d)],
                sent.at[DN],
                arrived.at[DN],
                z=to,
            )
        elif d:
            for e in near_y:
                dst = (y + e) % ny
                push(
                    down_send.at[to, dst], down_y.at[y, to], sent.at[DY], dy_recv.at[to], y=dst
                )
    carried = []
    for k in range(ny):
        stacked = mixed_all[z, k].astype(F32)
        mine = jnp.zeros((mrows, 128), F32)
        for c in range(ny):
            down, across = c // (ny // 2) * mrows, c % (ny // 2) * 128
            mine = jnp.where(y == c, stacked[down : down + mrows, across : across + 128], mine)
        carried.append(mine)
    carried = jnp.concatenate(carried, axis=0)
    quarter = half // 2

    def columns_of(value, t):
        cols = value[:, 64 * t : 64 * (t + 1)]
        return jnp.concatenate([cols[:quarter], cols[quarter:]], axis=1)

    def add_next():
        await_all(down_next, arrived.at[DN])
        for k in range(ny):
            added = down_own[k]
            for i in range(len(next_z)):
                added = added + down_next[i, k].astype(F32)
            down_own[k] = added
            down_send[z, k] = added.astype(BF16)
        for e in near_y:
            dst = (y + e) % ny
            push(down_send.at[z, dst], down_y.at[y, z], sent.at[DY], dy_recv.at[z], y=dst)

    if not rest:
        add_next()
    for d in rest + [0]:
        to = (z + d) % nz
        await_all(down_y.at[: ny - 1, to], dy_recv.at[to])
        summed = down_send[to, y].astype(F32) if d else down_own[y]
        for e in near_y:
            summed = summed + down_y[(y + e) % ny, to].astype(F32)
        if d:
            for t in range(2):
                sum_send[t, to] = columns_of(summed, t).astype(BF16)
                push(sum_send.at[t, to], sum_recv.at[tp, z], sent.at[DZ], arrived.at[DZ], z=to, tp=t)
            if d == rest[0]:
                add_next()
        else:
            whole = summed + carried
            fin_send[0] = columns_of(whole, 0)
            fin_send[1] = columns_of(whole, 1)
            fin_copy = push(
                fin_send.at[other], fin_recv, pair_send.at[4], pair_recv.at[4], tp=other
            )
    if rest:
        await_all(sum_recv.at[:, : len(rest)], arrived.at[DZ])
    total = [fin_send[tp], jnp.zeros((quarter, 128), F32)]
    for d in rest:
        src = (z + d) % nz
        total[0] = total[0] + sum_recv[tp, src].astype(F32)
        total[1] = total[1] + sum_recv[other, src].astype(F32)
    fin_copy.wait_recv()
    total[1] = total[1] + fin_recv[...]
    top = 4 * piece + 8
    packed[top : top + quarter] = jnp.where(tp == 0, total[0], total[1])
    packed[top + quarter : top + half] = jnp.where(tp == 0, total[1], total[0])

    for copy in (tok_copy, out_copy, up_copy, down_copy, fin_copy):
        copy.wait_send()
    await_sent(w_own.at[: ny - 1, :last], sent.at[WY])
    await_sent(w_flat.at[last, : (ny - 1) * some], sent.at[WQ])
    await_sent(wo_all.at[tp, head, : (ny - 1) * 128], sent.at[OD])
    await_sent(tok_all.at[: ny - 1], sent.at[TY])
    await_sent(part_send.at[:, : nz - 1], sent.at[PZ])
    await_sent(gate_send.at[: nz - 1], sent.at[GZ])
    await_sent(rows_send.at[: ny - 1], sent.at[RY])
    await_sent(wo_all.at[tp, share, : (ny - 1) * 128], sent.at[OY])
    if nx > 1:
        await_sent(shared, sent.at[WX])
        await_sent(passed_on, sent.at[OX])
    await_sent(wo_all.at[tp, :, : (ny - 1) * 128], sent.at[OP])
    await_sent(mixed_all.at[: nz - 1, 0], sent.at[MZ])
    await_sent(mixed_all.at[: len(next_z), : ny - 1], sent.at[MN])
    await_sent(mixed_all.at[: nz - len(next_z), : ny - 1], sent.at[MY])
    await_sent(down_next, sent.at[DN])
    await_sent(down_send.at[: nz - len(next_z), : ny - 1], sent.at[DY])
    if rest:
        await_sent(sum_send.at[:, : len(rest)], sent.at[DZ])

    @pl.when(tp == core)
    def _():
        await_sent(heads_all.at[: nz - 1], sent.at[HZ])

    @pl.when(tp != core)
    def _():
        await_sent(heads_all, sent.at[HZ])


def update(ny, mem, packed_hbm, new_mem, out_hbm, norm_hbm, stab_hbm, packed, made, out, stab, sems):
    load = pltpu.make_async_copy(packed_hbm, packed, sems.at[0])
    load.start()
    piece = mem.shape[0]
    own = stab.shape[0]
    count = sems.shape[0] - 4
    each = piece // count
    copies = []

    def send(src, dst):
        copies.append(pltpu.make_async_copy(src, dst, sems.at[1 + len(copies)]))
        copies[-1].start()

    rows = out.shape[1]
    blocks = rows // own // 2
    per = blocks // ny
    quarter = rows // 4
    line = lax.broadcasted_iota(jnp.int32, (rows // 2, rows), 0).astype(F32)
    column = lax.broadcasted_iota(jnp.int32, (rows // 2, rows), 1).astype(F32)
    side = jnp.where(line >= quarter, 1.0, 0.0)
    orders = []
    for upper in range(2):
        at = line + side * quarter + upper * quarter
        group = jnp.floor((at + 0.5) / own)
        inner = group - side * blocks
        in_y = jnp.floor((inner + 0.5) / per)
        in_z = inner - in_y * per
        target = (side * blocks + in_z * ny + in_y) * own + (at - group * own)
        orders.append(jnp.where(column == target, 1.0, 0.0).astype(BF16))
    load.wait()
    inflow_v = packed[:piece].T
    for b in range(count):
        for i in range(b * each, (b + 1) * each):
            key, retain = packed[piece + i], packed[2 * piece + i]
            made[i] = retain[None] * mem[i] + inflow_v[:, i : i + 1] * key[None]
        here = pl.ds(b * each, each)
        send(made.at[here], new_mem.at[here])
        if b == 0:
            send(packed.at[pl.ds(3 * piece, piece)], norm_hbm)
            stab[...] = packed[4 * piece : 4 * piece + own, : stab.shape[1]]
            send(stab, stab_hbm)
            result = packed[4 * piece + 8 :].T.astype(BF16)
            turned = jnp.dot(result[:64], orders[0], preferred_element_type=F32) + jnp.dot(
                result[64:], orders[1], preferred_element_type=F32
            )
            out[...] = turned.astype(BF16)
            send(out, out_hbm)
    for copy in copies:
        copy.wait()


def body(
    tokens,
    gain_mixer,
    weight_query,
    weight_key,
    weight_value,
    weight_outgate,
    weight_ingate,
    weight_forget,
    bias_input,
    bias_forget,
    memory,
    normalizer,
    stabilizer,
    head_gain,
    weight_out,
    gain_channel,
    weight_up,
    weight_down,
):
    nx, nz, ny = lax.axis_size("dp"), lax.axis_size("z"), lax.axis_size("y")
    own, heads, hd = memory.shape[:3]
    width_full = gain_mixer.shape[0]
    tokens = tokens.T
    rows = tokens.shape[1]
    half = rows // 2
    piece = own * heads
    zrows = ny * own
    block = ny * 128
    chunks = heads // 2
    mrows = nz // 2 * own
    dma = pltpu.SemaphoreType.DMA
    vmem = pl.BlockSpec(memory_space=pltpu.VMEM)
    hbm = pl.BlockSpec(memory_space=pl.ANY)
    mem48 = memory.reshape(piece, hd, hd)
    small = (
        tokens,
        gain_mixer.reshape(-1, 128),
        bias_input.reshape(1, -1),
        bias_forget.reshape(1, -1),
        normalizer.reshape(piece, hd),
        stabilizer,
        head_gain,
        gain_channel.reshape(-1, 128),
    )
    packed = pl.pallas_call(
        functools.partial(kernel, nx, nz, ny, width_full),
        out_shape=jax.ShapeDtypeStruct((4 * piece + 8 + half, hd), F32),
        in_specs=[hbm] * 18,
        out_specs=vmem,
        scratch_shapes=[pltpu.VMEM(value.shape, value.dtype) for value in small]
        + [
            pltpu.VMEM(tokens.shape, BF16),
            pltpu.VMEM((ny, rows, 128), BF16),
            pltpu.VMEM((mrows, block), F32),
            pltpu.VMEM((2, width_full // 128, 128), F32),
            pltpu.VMEM((16, block), BF16),
            pltpu.VMEM((16, block), BF16),
            pltpu.VMEM((piece, hd, hd), F32),
            pltpu.VMEM((piece, hd, 2 * hd), BF16),
            pltpu.VMEM((ny, 128, heads, hd), BF16),
            pltpu.VMEM((128 * heads, hd), F32),
            pltpu.VMEM((ny, chunks, 128, 2 * hd), BF16),
            pltpu.VMEM((chunks, block, 2 * hd), BF16),
            pltpu.VMEM((chunks, nz, 2 * zrows, hd), BF16),
            pltpu.VMEM((chunks, nz, 2 * zrows, hd), BF16),
            pltpu.VMEM((nz, zrows, 128), F32),
            pltpu.VMEM((nz, zrows, 128), F32),
            pltpu.VMEM((zrows * heads, hd), F32),
            pltpu.VMEM((ny, piece, hd), BF16),
            pltpu.VMEM((ny, piece, hd), BF16),
            pltpu.VMEM((piece, 2 * hd), F32),
            pltpu.VMEM((piece, hd), F32),
            pltpu.VMEM((piece, hd), BF16),
            pltpu.VMEM((nz, piece, hd), BF16),
            pltpu.VMEM((nz * piece, hd), F32),
            pltpu.VMEM((2, heads * hd, block), BF16),
            pltpu.VMEM((2, *weight_up.shape), BF16),
            pltpu.VMEM((2, *weight_down.shape), BF16),
            pltpu.VMEM((nz, ny, 2 * mrows, block // 2), BF16),
            pltpu.VMEM((2, half, weight_up.shape[1]), F32),
            pltpu.VMEM((nz, ny, half, 128), BF16),
            pltpu.VMEM((ny, half, 128), F32),
            pltpu.VMEM((min(2, nz - 1), ny, half, 128), BF16),
            pltpu.VMEM((ny, nz, half, 128), BF16),
            pltpu.VMEM((2, nz, half // 2, 128), BF16),
            pltpu.VMEM((2, nz, half // 2, 128), BF16),
            pltpu.VMEM((2, half // 2, 128), F32),
            pltpu.VMEM((half // 2, 128), F32),
            dma((8,)),
            dma((10,)),
            dma((5,)),
            dma((5,)),
            dma((len(PHASES),)),
            dma((len(PHASES),)),
            dma((chunks,)),
            dma((chunks,)),
            dma((nz,)),
            dma((nz,)),
            dma((nz,)),
        ],
        compiler_params=pltpu.CompilerParams(
            collective_id=0, has_side_effects=True, vmem_limit_bytes=56 * 1024 * 1024
        ),
    )(
        *small,
        weight_query,
        weight_key,
        weight_value,
        weight_outgate,
        weight_ingate.T,
        weight_forget.T,
        mem48,
        weight_out,
        weight_up,
        weight_down,
    )
    new_memory, layer_out, new_norm, new_stab = pl.pallas_call(
        functools.partial(update, ny),
        out_shape=(
            jax.ShapeDtypeStruct(mem48.shape, F32),
            jax.ShapeDtypeStruct(tokens.shape, BF16),
            jax.ShapeDtypeStruct((piece, hd), F32),
            jax.ShapeDtypeStruct((own, heads), F32),
        ),
        in_specs=[vmem, pl.BlockSpec(memory_space=pltpu.HBM)],
        out_specs=(hbm,) * 4,
        scratch_shapes=[
            pltpu.VMEM(packed.shape, F32),
            pltpu.VMEM(mem48.shape, F32),
            pltpu.VMEM(tokens.shape, BF16),
            pltpu.VMEM((own, heads), F32),
            dma((piece // 4 + 4,)),
        ],
        compiler_params=pltpu.CompilerParams(vmem_limit_bytes=16 * 1024 * 1024),
    )(mem48, packed)
    new_memory = new_memory.reshape(memory.shape)
    return (layer_out.T, new_memory, new_norm.reshape(normalizer.shape), new_stab)


def solution(mesh):
    kv = mesh.shape["kv"]
    ny = 4
    torus = Mesh(
        mesh.devices.reshape(mesh.shape["dp"], kv // ny, ny, mesh.shape["tp"]),
        ("dp", "z", "y", "tp"),
    )
    placed = (
        P("dp", KV_TP),
        P(),
        P(KV, "tp", None),
        P(KV, "tp", None),
        P(KV, "tp", None),
        P(KV, "tp", None),
        P(),
        P(),
        P(),
        P(),
        P(DP_KV, "tp", None, None),
        P(DP_KV, "tp", None),
        P(DP_KV, "tp"),
        P(),
        P("tp", KV),
        P(),
        P(None, KV_TP),
        P(KV_TP, None),
    )
    return jax.shard_map(
        body,
        mesh=torus,
        in_specs=placed,
        out_specs=(
            P("dp", KV_TP),
            P(DP_KV, "tp", None, None),
            P(DP_KV, "tp", None),
            P(DP_KV, "tp"),
        ),
        check_vma=False,
    )
```

```python
import functools

import jax
import jax.numpy as jnp
from jax import lax
from jax.experimental import pallas as pl
from jax.experimental.pallas import tpu as pltpu
from jax.sharding import Mesh
from jax.sharding import PartitionSpec as P

EPS = 1e-06
KV_TP = ("z", "y", "tp")
KV = ("z", "y")
DP_KV = ("dp", "z", "y")
MESH = pl.DeviceIdType.MESH
PHASES = WY, WQ, WX, TY, PZ, GZ, RY, HZ, OY, OX, OD, OP, MZ, MN, MY, DN, DY, DZ = range(18)
F32 = jnp.float32
BF16 = jnp.bfloat16


def by_distance(n):
    return sorted(range(1, n), key=lambda d: (min(d, n - d), d))


def kernel(
    nx,
    nz,
    ny,
    width_full,
    tokens_hbm,
    gain_mixer_hbm,
    bias_in_hbm,
    bias_forget_hbm,
    normalizer_hbm,
    stabilizer_hbm,
    head_gain_hbm,
    gain_channel_hbm,
    w0,
    w1,
    w2,
    w3,
    w_in,
    w_forget,
    memory,
    w_out,
    w_up,
    w_down,
    packed,
    tokens,
    gain_mixer,
    bias_in,
    bias_forget,
    normalizer,
    stabilizer,
    head_gain,
    gain_channel,
    tok_in,
    tok_all,
    residual,
    gains,
    wig,
    wfg,
    mem,
    mem_split,
    w_raw,
    wide,
    w_own,
    w_flat,
    part_send,
    part_recv,
    gate_send,
    gate_recv,
    rows_wide,
    rows_send,
    rows_recv,
    q_twice,
    mq,
    heads_own,
    heads_all,
    heads_f32,
    wo_all,
    up_all,
    down_all,
    mixed_all,
    acc,
    down_send,
    down_own,
    down_next,
    down_y,
    sum_send,
    sum_recv,
    fin_send,
    fin_recv,
    small_sem,
    local_sem,
    pair_send,
    pair_recv,
    sent,
    arrived,
    wy_recv,
    pz_recv,
    mz_recv,
    my_recv,
    dy_recv,
):
    x_rank = lax.axis_index("dp")
    z = lax.axis_index("z")
    y = lax.axis_index("y")
    tp = lax.axis_index("tp")
    other = 1 - tp
    half_z = nz // 2
    rows = tokens.shape[1]
    half = rows // 2
    own = 6
    heads = 8
    zrows = ny * own
    block = ny * 128
    near_z = by_distance(nz)
    near_y = by_distance(ny)
    near_x = by_distance(nx)
    far_z = near_z[::-1]
    next_z = [d for d in near_z if min(d, nz - d) == 1]
    rest_z = [d for d in near_z if d not in next_z]
    contract = (((1,), (1,)), ((), ()))

    def remote(src, dst, send, recv, **to):
        return pltpu.make_async_remote_copy(
            src_ref=src, dst_ref=dst, send_sem=send, recv_sem=recv, device_id=to, device_id_type=MESH
        )

    def push(*args, **to):
        copy = remote(*args, **to)
        copy.start()
        return copy

    def await_sent(ref, sem):
        remote(ref, ref, sem, sem, tp=other).wait_send()

    def await_all(ref, sem):
        remote(ref, ref, sem, sem, tp=other).wait_recv()

    barrier = pltpu.get_barrier_semaphore()
    for d in near_z:
        for t in range(2):
            pl.semaphore_signal(
                barrier, inc=1, device_id={"z": (z + d) % nz, "tp": t}, device_id_type=MESH
            )
    for d in near_y:
        pl.semaphore_signal(barrier, inc=1, device_id={"y": (y + d) % ny}, device_id_type=MESH)
    for d in near_x:
        pl.semaphore_signal(barrier, inc=1, device_id={"dp": (x_rank + d) % nx}, device_id_type=MESH)
    pl.semaphore_signal(barrier, inc=1, device_id={"tp": other}, device_id_type=MESH)

    depth = heads * 128

    def out_columns(k):
        return pl.ds(pl.multiple_of(k * 128, 128), 128)

    rows_of_block = pl.ds(pl.multiple_of(z * block, block), block)
    loads = [
        pltpu.make_async_copy(w_in.at[:, rows_of_block], wig, local_sem.at[0]),
        pltpu.make_async_copy(w_forget.at[:, rows_of_block], wfg, local_sem.at[1]),
        pltpu.make_async_copy(memory, mem, local_sem.at[2]),
        pltpu.make_async_copy(w_out, wo_all.at[tp, :, out_columns(y)], local_sem.at[3]),
        pltpu.make_async_copy(w_up, up_all.at[tp], local_sem.at[4]),
        pltpu.make_async_copy(w_down, down_all.at[tp], local_sem.at[5]),
    ]
    raw_loads = [
        pltpu.make_async_copy(w, w_raw.at[m], local_sem.at[6 + m])
        for m, w in enumerate((w0, w1, w2, w3))
    ]
    small = [
        pltpu.make_async_copy(src, dst, small_sem.at[i])
        for i, (src, dst) in enumerate(
            (
                (tokens_hbm, tokens),
                (gain_mixer_hbm, gain_mixer),
                (bias_in_hbm, bias_in),
                (bias_forget_hbm, bias_forget),
                (normalizer_hbm, normalizer),
                (stabilizer_hbm, stabilizer),
                (head_gain_hbm, head_gain),
                (gain_channel_hbm, gain_channel),
            )
        )
    ]
    for copy in raw_loads + small:
        copy.start()
    chunks = heads // 2
    for m in range(4):
        raw_loads[m].wait()
        wide[...] = w_raw[m].astype(F32).reshape(128 * heads, 128)
        for h in range(heads):
            w_own[m, h // 2, :, (h % 2) * 128 : (h % 2 + 1) * 128] = wide[
                pl.ds(h, 128, stride=heads), :
            ].astype(BF16)
    for copy in small:
        copy.wait()
    gains[0] = gain_mixer[...].astype(F32)
    gains[1] = gain_channel[...].astype(F32)

    pl.semaphore_wait(barrier, 2 * (nz - 1) + (ny - 1) + (nx - 1) + 1)

    tok_copy = push(tokens, tok_in, pair_send.at[0], pair_recv.at[0], tp=other)
    own_block = pl.ds(pl.multiple_of(y * 128, 128), 128)

    def send_chunk(c):
        for d in near_y:
            to = (y + d) % ny
            push(
                w_own.at[to, c],
                w_flat.at[c, own_block],
                sent.at[WY],
                wy_recv.at[c],
                y=to,
            )

    direct_chunks = chunks // 2
    some = 128 // nx

    def share_of(k):
        return pl.ds(pl.multiple_of(k * 128 + x_rank * some, some), some)

    for d in near_y:
        to = (y + d) % ny
        push(
            w_own.at[to, direct_chunks:, share_of(0)],
            w_flat.at[direct_chunks:, share_of(y)],
            sent.at[WQ],
            arrived.at[WQ],
            y=to,
        )
    for copy in loads:
        copy.start()
    tok_copy.wait_recv()
    mine, theirs = tokens[...].astype(F32), tok_in[...].astype(F32)
    first = jnp.where(tp == 0, mine, theirs)
    second = jnp.where(tp == 0, theirs, mine)
    chip = jnp.concatenate([first, second], axis=0).T.astype(BF16)
    tok_all[y] = chip
    for d in near_y:
        push(
            tok_all.at[y], tok_all.at[y], sent.at[TY], arrived.at[TY], y=(y + d) % ny
        )
    for c in range(direct_chunks):
        send_chunk(c)
    direct = depth // 2
    part = (depth - direct) // nx
    share = pl.ds(pl.multiple_of(direct + x_rank * part, part), part)
    for d in near_y:
        to = (y + d) % ny
        push(w_out.at[share], wo_all.at[tp, share, out_columns(y)], sent.at[OY], arrived.at[OY], y=to)
    head = pl.ds(0, direct)
    for d in near_y:
        to = (y + d) % ny
        push(w_out.at[head], wo_all.at[tp, head, out_columns(y)], sent.at[OD], arrived.at[OD], y=to)
    own_out = wo_all.at[tp, :, out_columns(y)]
    out_copy = push(w_out, own_out, pair_send.at[1], pair_recv.at[1], tp=other)
    for c in range(chunks):
        w_flat[c, own_block] = w_own[y, c]
    await_all(w_flat.at[direct_chunks:, : (ny - 1) * some], arrived.at[WQ])
    shared_chunks = range(direct_chunks, chunks)
    for c in shared_chunks:
        for d in near_y:
            there = w_flat.at[c, share_of((y + d) % ny)]
            for e in near_x:
                push(there, there, sent.at[WX], wy_recv.at[c], dp=(x_rank + e) % nx)
    await_all(tok_all.at[: ny - 1], arrived.at[TY])
    x = jnp.concatenate(
        [
            (tok_all[s].astype(F32) * gains[0, pl.ds(z * ny + s, 1), :]).astype(BF16)
            for s in range(ny)
        ],
        axis=1,
    )

    def project(c):
        product = jnp.dot(x, w_flat[c], preferred_element_type=F32)
        for k in range(nz):
            part_send[c, k] = jnp.concatenate(
                [
                    product[k * zrows : (k + 1) * zrows, :128],
                    product[k * zrows : (k + 1) * zrows, 128:],
                ],
                axis=0,
            ).astype(BF16)
        for d in far_z:
            to = (z + d) % nz
            push(
                part_send.at[c, to], part_recv.at[c, z], sent.at[PZ], pz_recv.at[c], z=to
            )

    squares = jnp.zeros((rows, 1), F32)
    for s in range(ny):
        wide_rows = tok_all[s].astype(F32)
        squares = squares + jnp.sum(wide_rows * wide_rows, axis=1, keepdims=True)
    loads[0].wait()
    loads[1].wait()
    gate = jnp.concatenate(
        [
            lax.dot_general(x, wig[...], contract, preferred_element_type=F32),
            lax.dot_general(x, wfg[...], contract, preferred_element_type=F32),
            jnp.broadcast_to(squares, (rows, 8)),
        ],
        axis=1,
    )
    for k in range(nz):
        groups = [gate[k * zrows + g * 8 : k * zrows + (g + 1) * 8] for g in range(zrows // 8)]
        gate_send[k] = jnp.concatenate(groups + [jnp.zeros((8, 128 - 5 * zrows), F32)], axis=1)
    for d in far_z:
        to = (z + d) % nz
        push(gate_send.at[to], gate_recv.at[z], sent.at[GZ], arrived.at[GZ], z=to)

    sequence = [direct_chunks, 0] + list(range(direct_chunks + 1, chunks)) + list(range(1, direct_chunks))
    for c in sequence:
        if c < direct_chunks:
            await_all(w_flat.at[c, : (ny - 1) * 128], wy_recv.at[c])
        elif nx > 1:
            await_all(w_flat.at[c, : (ny - 1) * (nx - 1) * some], wy_recv.at[c])
        project(c)

    await_all(wo_all.at[tp, share, : (ny - 1) * 128], arrived.at[OY])
    for d in near_y:
        there = wo_all.at[tp, share, out_columns((y + d) % ny)]
        for e in near_x:
            push(there, there, sent.at[OX], arrived.at[OX], dp=(x_rank + e) % nx)
    up_copy = push(w_up, up_all.at[tp], pair_send.at[2], pair_recv.at[2], tp=other)
    down_copy = push(w_down, down_all.at[tp], pair_send.at[3], pair_recv.at[3], tp=other)

    loads[2].wait()

    def split(i, carry):
        m_bh = mem[i]
        high = m_bh.astype(BF16)
        mem_split[i, :, :128] = high
        mem_split[i, :, 128:] = (m_bh - high.astype(F32)).astype(BF16)
        return carry

    lax.fori_loop(0, own * heads, split, 0)

    at = lax.broadcasted_iota(jnp.int32, (half_z * own, rows), 0)
    row = at + tp * half + y * own
    for k in range(1, half_z):
        row = row + jnp.where(at >= k * own, zrows - own, 0)
    chosen = jnp.where(
        lax.broadcasted_iota(jnp.int32, (half_z * own, rows), 1) == row, 1.0, 0.0
    ).astype(BF16)
    residual[...] = jnp.dot(
        chosen,
        jnp.concatenate([tok_all[k] for k in range(ny)], axis=1),
        preferred_element_type=F32,
    )

    await_all(gate_recv.at[: nz - 1], arrived.at[GZ])
    gate_sum = gate_send[z]
    for d in near_z:
        gate_sum = gate_sum + gate_recv[(z + d) % nz]
    gate_sum = jnp.concatenate(
        [gate_sum[:, g * 40 : (g + 1) * 40] for g in range(zrows // 8)], axis=0
    )
    inverse = lax.rsqrt(gate_sum[:, 32:33] / width_full + EPS)
    gate_pre = inverse * gate_sum
    gate_rows = jnp.zeros((own, 40), F32)
    for k in range(ny):
        gate_rows = gate_rows + jnp.where(y == k, gate_pre[k * own : (k + 1) * own], 0.0)
    in_all = gate_rows[:, 0:16] + bias_in[...]
    forget_all = gate_rows[:, 16:32] + bias_forget[...]
    ingate = jnp.where(tp == 0, in_all[:, :8], in_all[:, 8:])
    forget_pre = jnp.where(tp == 0, forget_all[:, :8], forget_all[:, 8:])
    forget = jnp.minimum(forget_pre, 0.0) - jnp.log(1.0 + jnp.exp(-jnp.abs(forget_pre)))
    carried = forget + stabilizer[...]
    new_stab = jnp.maximum(carried, ingate)
    packed[4 * own * heads : 4 * own * heads + own, :heads] = new_stab
    diagonal = lax.broadcasted_iota(jnp.int32, (heads, heads), 0) == lax.broadcasted_iota(
        jnp.int32, (heads, heads), 1
    )

    def column(value):
        return jnp.concatenate(
            [
                jnp.sum(
                    jnp.where(diagonal, jnp.broadcast_to(value[b : b + 1], (heads, heads)), 0.0),
                    axis=1,
                    keepdims=True,
                )
                for b in range(own)
            ],
            axis=0,
        )

    retain = column(jnp.exp(carried - new_stab))
    inflow = column(jnp.exp(ingate - new_stab))
    floor = column(jnp.exp(-new_stab))

    for c in sequence:
        await_all(part_recv.at[c, : nz - 1], pz_recv.at[c])
        total = part_send[c, z].astype(F32)
        for d in near_z:
            src = (z + d) % nz
            total = total + part_recv[c, src].astype(F32)
        for i in range(2):
            rows_wide[pl.ds(2 * c + i, zrows, stride=heads), :] = (
                inverse * total[i * zrows : (i + 1) * zrows]
            )
    piece = own * heads
    for k in range(ny):
        rows_send[k] = rows_wide[k * piece : (k + 1) * piece, :].astype(BF16)
    for d in near_y:
        to = (y + d) % ny
        push(rows_send.at[to], rows_recv.at[y], sent.at[RY], arrived.at[RY], y=to)
    rows_recv[y] = rows_send[y]
    await_all(rows_recv.at[: ny - 1], arrived.at[RY])

    query = rows_recv[0].astype(F32)
    key = rows_recv[1].astype(F32) * 128**-0.5
    value = rows_recv[2].astype(F32)
    gate_o = rows_recv[3].astype(F32)
    q_twice[...] = jnp.concatenate([query, query], axis=1)
    new_norm = retain * normalizer[...] + inflow * key
    packed[3 * piece : 4 * piece] = new_norm
    inflow_value = inflow * value
    packed[:piece] = inflow_value
    packed[piece : 2 * piece] = key
    packed[2 * piece : 3 * piece] = jnp.broadcast_to(retain, (piece, 128))
    sub = lax.broadcasted_iota(jnp.int32, (heads, 128), 0)

    for b in range(own):
        these = slice(b * heads, (b + 1) * heads)
        product = lax.dot_general(
            q_twice[these, :].astype(BF16),
            mem_split[these].reshape(heads * 128, 256),
            contract,
            preferred_element_type=F32,
        )
        found = product[:, :128]
        for h in range(1, heads):
            found = jnp.where(sub == h, product[:, h * 128 : (h + 1) * 128], found)
        mq[these, :] = found
    numerator = retain * mq[...] + inflow_value * jnp.sum(key * query, axis=1, keepdims=True)
    denominator = jnp.sum(new_norm * query, axis=1, keepdims=True)
    readout = numerator / jnp.maximum(jnp.abs(denominator), floor)
    centered = readout - jnp.mean(readout, axis=1, keepdims=True)
    normed = centered * lax.rsqrt(jnp.mean(centered * centered, axis=1, keepdims=True) + EPS)
    gain_all = head_gain[...].astype(F32)
    gain_own = jnp.where(tp == 0, gain_all[:heads], gain_all[heads:])
    heads_out = (
        normed * jnp.concatenate([gain_own] * own, axis=0) * (1.0 / (1.0 + jnp.exp(-gate_o)))
    ).astype(BF16)
    heads_own[...] = heads_out

    core = z // half_z
    zl = z % half_z

    @pl.when(tp == core)
    def _():
        heads_all[2 * zl + tp] = heads_out

    for d in far_z:
        push(
            heads_own,
            heads_all.at[2 * zl + tp],
            sent.at[HZ],
            arrived.at[HZ],
            z=(z + d) % nz,
            tp=core,
        )

    @pl.when(tp != core)
    def _():
        push(heads_own, heads_all.at[2 * zl + tp], sent.at[HZ], arrived.at[HZ], tp=other)

    loads[3].wait()
    if nx > 1:
        passed_on = wo_all.at[tp, : part * (nx - 1), : (ny - 1) * 128]
        await_all(passed_on, arrived.at[OX])
    await_all(wo_all.at[tp, head, : (ny - 1) * 128], arrived.at[OD])
    for d in near_y:
        whole = wo_all.at[tp, :, out_columns((y + d) % ny)]
        push(whole, whole, sent.at[OP], arrived.at[OP], tp=other)

    @pl.when(tp == core)
    def _():
        await_all(heads_all.at[: nz - 1], arrived.at[HZ])

    @pl.when(tp != core)
    def _():
        await_all(heads_all, arrived.at[HZ])

    for k in range(half_z):
        for t in range(2):
            start = (t * half_z + k) * piece
            heads_f32[start : start + piece, :] = heads_all[2 * k + t].astype(F32)
    mrows = half_z * own
    gathered = jnp.concatenate(
        [
            heads_f32[pl.ds(t * half_z * piece + h, mrows, stride=heads), :].astype(BF16)
            for t in range(2)
            for h in range(heads)
        ],
        axis=1,
    )
    out_copy.wait_recv()
    await_all(wo_all.at[other, :, : (ny - 1) * 128], arrived.at[OP])
    attended = jnp.dot(
        gathered, wo_all[...].reshape(2 * depth, block), preferred_element_type=F32
    )
    mixed = residual[...] + attended
    wcols = block // 2
    mixed_all[z, y] = jnp.concatenate([mixed[:, :wcols], mixed[:, wcols:]], axis=0).astype(BF16)

    mine_here = mixed_all.at[z, y]
    for e in near_y:
        push(mine_here, mine_here, sent.at[MY], my_recv.at[z], y=(y + e) % ny)
    for d in rest_z + next_z:
        push(mine_here, mine_here, sent.at[MZ], mz_recv.at[z], z=(z + d) % nz)
    await_all(mixed_all.at[z, : ny - 1], my_recv.at[z])
    for e in near_y:
        there = mixed_all.at[z, (y + e) % ny]
        for d in next_z:
            push(there, there, sent.at[MN], mz_recv.at[z], z=(z + d) % nz)
    for d in rest_z:
        s = (z + d) % nz
        here = mixed_all.at[s, y]
        await_all(here, mz_recv.at[s])
        for e in near_y:
            push(here, here, sent.at[MY], my_recv.at[s], y=(y + e) % ny)
    loads[4].wait()
    up_copy.wait_recv()
    hidden = up_all.shape[2]
    squares = [jnp.zeros((mrows, 1), F32)] * ny
    for d in [0] + near_z:
        s = (z + d) % nz
        if d in next_z:
            await_all(mixed_all.at[s], mz_recv.at[s])
        elif d:
            await_all(mixed_all.at[s, : ny - 1], my_recv.at[s])
        gain = jnp.concatenate([gains[1, pl.ds(s * ny + k, 1), :] for k in range(ny)], axis=1)
        scaled = []
        for k in range(ny):
            stacked = mixed_all[s, k].astype(F32)
            wide_rows = jnp.concatenate([stacked[:mrows], stacked[mrows:]], axis=1)
            squares[k] = squares[k] + jnp.sum(wide_rows * wide_rows, axis=1, keepdims=True)
            scaled.append(wide_rows * gain)
        lhs = jnp.concatenate(scaled, axis=0).astype(BF16)
        here = pl.ds(pl.multiple_of(s * block, block), block)
        for t in range(2):
            product = jnp.dot(lhs, up_all[t, here, :], preferred_element_type=F32)
            if d:
                product = product + acc[t]
            acc[t] = product
    inverse_mlp = lax.rsqrt(jnp.concatenate(squares, axis=0) / width_full + EPS)
    squared = []
    for t in range(2):
        activation = jnp.maximum(inverse_mlp * acc[t], 0.0)
        squared.append((activation * activation).astype(BF16))

    loads[5].wait()
    down_copy.wait_recv()
    rest = rest_z[::-1]
    for d in rest[:1] + next_z + rest[1:] + [0]:
        to = (z + d) % nz
        here = pl.ds(pl.multiple_of(to * block, block), block)
        product = jnp.dot(
            squared[0], down_all[0, :, here], preferred_element_type=F32
        ) + jnp.dot(squared[1], down_all[1, :, here], preferred_element_type=F32)
        for k in range(ny):
            piece_k = product[:, k * 128 : (k + 1) * 128]
            if d:
                down_send[to, k] = piece_k.astype(BF16)
            else:
                down_own[k] = piece_k
        if d in next_z:
            push(
                down_send.at[to],
                down_next.at[next_z.index(d)],
                sent.at[DN],
                arrived.at[DN],
                z=to,
            )
        elif d:
            for e in near_y:
                dst = (y + e) % ny
                push(
                    down_send.at[to, dst], down_y.at[y, to], sent.at[DY], dy_recv.at[to], y=dst
                )
    carried = []
    for k in range(ny):
        stacked = mixed_all[z, k].astype(F32)
        mine = jnp.zeros((mrows, 128), F32)
        for c in range(ny):
            down, across = c // (ny // 2) * mrows, c % (ny // 2) * 128
            mine = jnp.where(y == c, stacked[down : down + mrows, across : across + 128], mine)
        carried.append(mine)
    carried = jnp.concatenate(carried, axis=0)
    quarter = half // 2

    def columns_of(value, t):
        cols = value[:, 64 * t : 64 * (t + 1)]
        return jnp.concatenate([cols[:quarter], cols[quarter:]], axis=1)

    def add_next():
        await_all(down_next, arrived.at[DN])
        for k in range(ny):
            added = down_own[k]
            for i in range(len(next_z)):
                added = added + down_next[i, k].astype(F32)
            down_own[k] = added
            down_send[z, k] = added.astype(BF16)
        for e in near_y:
            dst = (y + e) % ny
            push(down_send.at[z, dst], down_y.at[y, z], sent.at[DY], dy_recv.at[z], y=dst)

    if not rest:
        add_next()
    for d in rest + [0]:
        to = (z + d) % nz
        await_all(down_y.at[: ny - 1, to], dy_recv.at[to])
        summed = down_send[to, y].astype(F32) if d else down_own[y]
        for e in near_y:
            summed = summed + down_y[(y + e) % ny, to].astype(F32)
        if d:
            for t in range(2):
                sum_send[t, to] = columns_of(summed, t).astype(BF16)
                push(sum_send.at[t, to], sum_recv.at[tp, z], sent.at[DZ], arrived.at[DZ], z=to, tp=t)
            if d == rest[0]:
                add_next()
        else:
            whole = summed + carried
            fin_send[0] = columns_of(whole, 0)
            fin_send[1] = columns_of(whole, 1)
            fin_copy = push(
                fin_send.at[other], fin_recv, pair_send.at[4], pair_recv.at[4], tp=other
            )
    if rest:
        await_all(sum_recv.at[:, : len(rest)], arrived.at[DZ])
    total = [fin_send[tp], jnp.zeros((quarter, 128), F32)]
    for d in rest:
        src = (z + d) % nz
        total[0] = total[0] + sum_recv[tp, src].astype(F32)
        total[1] = total[1] + sum_recv[other, src].astype(F32)
    fin_copy.wait_recv()
    total[1] = total[1] + fin_recv[...]
    top = 4 * piece + 8
    packed[top : top + quarter] = jnp.where(tp == 0, total[0], total[1])
    packed[top + quarter : top + half] = jnp.where(tp == 0, total[1], total[0])

    for copy in (tok_copy, out_copy, up_copy, down_copy, fin_copy):
        copy.wait_send()
    await_sent(w_own.at[: ny - 1, :direct_chunks], sent.at[WY])
    await_sent(w_flat.at[direct_chunks:, : (ny - 1) * some], sent.at[WQ])
    await_sent(wo_all.at[tp, head, : (ny - 1) * 128], sent.at[OD])
    await_sent(tok_all.at[: ny - 1], sent.at[TY])
    await_sent(part_send.at[:, : nz - 1], sent.at[PZ])
    await_sent(gate_send.at[: nz - 1], sent.at[GZ])
    await_sent(rows_send.at[: ny - 1], sent.at[RY])
    await_sent(wo_all.at[tp, share, : (ny - 1) * 128], sent.at[OY])
    if nx > 1:
        await_sent(w_flat.at[direct_chunks:, : (ny - 1) * (nx - 1) * some], sent.at[WX])
        await_sent(passed_on, sent.at[OX])
    await_sent(wo_all.at[tp, :, : (ny - 1) * 128], sent.at[OP])
    await_sent(mixed_all.at[: nz - 1, 0], sent.at[MZ])
    await_sent(mixed_all.at[: len(next_z), : ny - 1], sent.at[MN])
    await_sent(mixed_all.at[: nz - len(next_z), : ny - 1], sent.at[MY])
    await_sent(down_next, sent.at[DN])
    await_sent(down_send.at[: nz - len(next_z), : ny - 1], sent.at[DY])
    if rest:
        await_sent(sum_send.at[:, : len(rest)], sent.at[DZ])

    @pl.when(tp == core)
    def _():
        await_sent(heads_all.at[: nz - 1], sent.at[HZ])

    @pl.when(tp != core)
    def _():
        await_sent(heads_all, sent.at[HZ])


def update(ny, mem, packed_hbm, new_mem, out_hbm, norm_hbm, stab_hbm, packed, made, out, stab, sems):
    load = pltpu.make_async_copy(packed_hbm, packed, sems.at[0])
    load.start()
    piece = mem.shape[0]
    own = stab.shape[0]
    count = sems.shape[0] - 4
    each = piece // count
    copies = []

    def send(src, dst):
        copies.append(pltpu.make_async_copy(src, dst, sems.at[1 + len(copies)]))
        copies[-1].start()

    rows = out.shape[1]
    blocks = rows // own // 2
    per = blocks // ny
    quarter = rows // 4
    line = lax.broadcasted_iota(jnp.int32, (rows // 2, rows), 0).astype(F32)
    column = lax.broadcasted_iota(jnp.int32, (rows // 2, rows), 1).astype(F32)
    side = jnp.where(line >= quarter, 1.0, 0.0)
    orders = []
    for upper in range(2):
        at = line + side * quarter + upper * quarter
        group = jnp.floor((at + 0.5) / own)
        inner = group - side * blocks
        in_y = jnp.floor((inner + 0.5) / per)
        in_z = inner - in_y * per
        target = (side * blocks + in_z * ny + in_y) * own + (at - group * own)
        orders.append(jnp.where(column == target, 1.0, 0.0).astype(BF16))
    load.wait()
    inflow_v = packed[:piece].T
    for b in range(count):
        for i in range(b * each, (b + 1) * each):
            key, retain = packed[piece + i], packed[2 * piece + i]
            made[i] = retain[None] * mem[i] + inflow_v[:, i : i + 1] * key[None]
        here = pl.ds(b * each, each)
        send(made.at[here], new_mem.at[here])
        if b == 0:
            send(packed.at[pl.ds(3 * piece, piece)], norm_hbm)
            stab[...] = packed[4 * piece : 4 * piece + own, : stab.shape[1]]
            send(stab, stab_hbm)
            result = packed[4 * piece + 8 :].T.astype(BF16)
            turned = jnp.dot(result[:64], orders[0], preferred_element_type=F32) + jnp.dot(
                result[64:], orders[1], preferred_element_type=F32
            )
            out[...] = turned.astype(BF16)
            send(out, out_hbm)
    for copy in copies:
        copy.wait()


def body(
    tokens,
    gain_mixer,
    weight_query,
    weight_key,
    weight_value,
    weight_outgate,
    weight_ingate,
    weight_forget,
    bias_input,
    bias_forget,
    memory,
    normalizer,
    stabilizer,
    head_gain,
    weight_out,
    gain_channel,
    weight_up,
    weight_down,
):
    nx, nz, ny = lax.axis_size("dp"), lax.axis_size("z"), lax.axis_size("y")
    own, heads, hd = memory.shape[:3]
    width_full = gain_mixer.shape[0]
    tokens = tokens.T
    rows = tokens.shape[1]
    half = rows // 2
    piece = own * heads
    zrows = ny * own
    block = ny * 128
    chunks = heads // 2
    mrows = nz // 2 * own
    dma = pltpu.SemaphoreType.DMA
    vmem = pl.BlockSpec(memory_space=pltpu.VMEM)
    hbm = pl.BlockSpec(memory_space=pl.ANY)
    mem48 = memory.reshape(piece, hd, hd)
    small = (
        tokens,
        gain_mixer.reshape(-1, 128),
        bias_input.reshape(1, -1),
        bias_forget.reshape(1, -1),
        normalizer.reshape(piece, hd),
        stabilizer,
        head_gain,
        gain_channel.reshape(-1, 128),
    )
    packed = pl.pallas_call(
        functools.partial(kernel, nx, nz, ny, width_full),
        out_shape=jax.ShapeDtypeStruct((4 * piece + 8 + half, hd), F32),
        in_specs=[hbm] * 18,
        out_specs=vmem,
        scratch_shapes=[pltpu.VMEM(value.shape, value.dtype) for value in small]
        + [
            pltpu.VMEM(tokens.shape, BF16),
            pltpu.VMEM((ny, rows, 128), BF16),
            pltpu.VMEM((mrows, block), F32),
            pltpu.VMEM((2, width_full // 128, 128), F32),
            pltpu.VMEM((16, block), BF16),
            pltpu.VMEM((16, block), BF16),
            pltpu.VMEM((piece, hd, hd), F32),
            pltpu.VMEM((piece, hd, 2 * hd), BF16),
            pltpu.VMEM((ny, 128, heads, hd), BF16),
            pltpu.VMEM((128 * heads, hd), F32),
            pltpu.VMEM((ny, chunks, 128, 2 * hd), BF16),
            pltpu.VMEM((chunks, block, 2 * hd), BF16),
            pltpu.VMEM((chunks, nz, 2 * zrows, hd), BF16),
            pltpu.VMEM((chunks, nz, 2 * zrows, hd), BF16),
            pltpu.VMEM((nz, 8, 128), F32),
            pltpu.VMEM((nz, 8, 128), F32),
            pltpu.VMEM((zrows * heads, hd), F32),
            pltpu.VMEM((ny, piece, hd), BF16),
            pltpu.VMEM((ny, piece, hd), BF16),
            pltpu.VMEM((piece, 2 * hd), F32),
            pltpu.VMEM((piece, hd), F32),
            pltpu.VMEM((piece, hd), BF16),
            pltpu.VMEM((nz, piece, hd), BF16),
            pltpu.VMEM((nz * piece, hd), F32),
            pltpu.VMEM((2, heads * hd, block), BF16),
            pltpu.VMEM((2, *weight_up.shape), BF16),
            pltpu.VMEM((2, *weight_down.shape), BF16),
            pltpu.VMEM((nz, ny, 2 * mrows, block // 2), BF16),
            pltpu.VMEM((2, half, weight_up.shape[1]), F32),
            pltpu.VMEM((nz, ny, half, 128), BF16),
            pltpu.VMEM((ny, half, 128), F32),
            pltpu.VMEM((min(2, nz - 1), ny, half, 128), BF16),
            pltpu.VMEM((ny, nz, half, 128), BF16),
            pltpu.VMEM((2, nz, half // 2, 128), BF16),
            pltpu.VMEM((2, nz, half // 2, 128), BF16),
            pltpu.VMEM((2, half // 2, 128), F32),
            pltpu.VMEM((half // 2, 128), F32),
            dma((8,)),
            dma((10,)),
            dma((5,)),
            dma((5,)),
            dma((len(PHASES),)),
            dma((len(PHASES),)),
            dma((chunks,)),
            dma((chunks,)),
            dma((nz,)),
            dma((nz,)),
            dma((nz,)),
        ],
        compiler_params=pltpu.CompilerParams(
            collective_id=0, has_side_effects=True, vmem_limit_bytes=56 * 1024 * 1024
        ),
    )(
        *small,
        weight_query,
        weight_key,
        weight_value,
        weight_outgate,
        weight_ingate.T,
        weight_forget.T,
        mem48,
        weight_out,
        weight_up,
        weight_down,
    )
    new_memory, layer_out, new_norm, new_stab = pl.pallas_call(
        functools.partial(update, ny),
        out_shape=(
            jax.ShapeDtypeStruct(mem48.shape, F32),
            jax.ShapeDtypeStruct(tokens.shape, BF16),
            jax.ShapeDtypeStruct((piece, hd), F32),
            jax.ShapeDtypeStruct((own, heads), F32),
        ),
        in_specs=[vmem, pl.BlockSpec(memory_space=pltpu.HBM)],
        out_specs=(hbm,) * 4,
        scratch_shapes=[
            pltpu.VMEM(packed.shape, F32),
            pltpu.VMEM(mem48.shape, F32),
            pltpu.VMEM(tokens.shape, BF16),
            pltpu.VMEM((own, heads), F32),
            dma((piece // 4 + 4,)),
        ],
        compiler_params=pltpu.CompilerParams(vmem_limit_bytes=16 * 1024 * 1024),
    )(mem48, packed)
    new_memory = new_memory.reshape(memory.shape)
    return (layer_out.T, new_memory, new_norm.reshape(normalizer.shape), new_stab)


def solution(mesh):
    kv = mesh.shape["kv"]
    ny = 4
    torus = Mesh(
        mesh.devices.reshape(mesh.shape["dp"], kv // ny, ny, mesh.shape["tp"]),
        ("dp", "z", "y", "tp"),
    )
    placed = (
        P("dp", KV_TP),
        P(),
        P(KV, "tp", None),
        P(KV, "tp", None),
        P(KV, "tp", None),
        P(KV, "tp", None),
        P(),
        P(),
        P(),
        P(),
        P(DP_KV, "tp", None, None),
        P(DP_KV, "tp", None),
        P(DP_KV, "tp"),
        P(),
        P("tp", KV),
        P(),
        P(None, KV_TP),
        P(KV_TP, None),
    )
    return jax.shard_map(
        body,
        mesh=torus,
        in_specs=placed,
        out_specs=(
            P("dp", KV_TP),
            P(DP_KV, "tp", None, None),
            P(DP_KV, "tp", None),
            P(DP_KV, "tp"),
        ),
        check_vma=False,
    )
```

```python
import functools

import jax
import jax.numpy as jnp
from jax import lax
from jax.experimental import pallas as pl
from jax.experimental.pallas import tpu as pltpu
from jax.sharding import Mesh
from jax.sharding import PartitionSpec as P

EPS = 1e-06
KV_TP = ("z", "y", "tp")
KV = ("z", "y")
DP_KV = ("dp", "z", "y")
MESH = pl.DeviceIdType.MESH
PHASES = WY, WQ, WX, TY, PZ, GZ, RY, HZ, OY, OX, OD, OP, MZ, MN, MY, DN, DY, DZ = range(18)
F32 = jnp.float32
BF16 = jnp.bfloat16


def by_distance(n):
    return sorted(range(1, n), key=lambda d: (min(d, n - d), d))


def kernel(
    nx,
    nz,
    ny,
    width_full,
    tokens_hbm,
    gain_mixer_hbm,
    bias_in_hbm,
    bias_forget_hbm,
    normalizer_hbm,
    stabilizer_hbm,
    head_gain_hbm,
    gain_channel_hbm,
    w0,
    w1,
    w2,
    w3,
    w_in,
    w_forget,
    memory,
    w_out,
    w_up,
    w_down,
    packed,
    tokens,
    gain_mixer,
    bias_in,
    bias_forget,
    normalizer,
    stabilizer,
    head_gain,
    gain_channel,
    tok_in,
    tok_all,
    residual,
    gains,
    wig,
    wfg,
    mem,
    mem_split,
    w_raw,
    wide,
    w_own,
    w_flat,
    part_send,
    part_recv,
    gate_send,
    gate_recv,
    rows_wide,
    rows_send,
    rows_recv,
    q_twice,
    mq,
    heads_own,
    heads_all,
    heads_f32,
    wo_all,
    up_all,
    down_all,
    mixed_all,
    acc,
    down_send,
    down_own,
    down_next,
    down_y,
    sum_send,
    sum_recv,
    fin_send,
    fin_recv,
    small_sem,
    local_sem,
    pair_send,
    pair_recv,
    sent,
    arrived,
    wy_recv,
    wq_recv,
    pz_recv,
    mz_recv,
    my_recv,
    dy_recv,
):
    x_rank = lax.axis_index("dp")
    z = lax.axis_index("z")
    y = lax.axis_index("y")
    tp = lax.axis_index("tp")
    other = 1 - tp
    half_z = nz // 2
    rows = tokens.shape[1]
    half = rows // 2
    own = 6
    heads = 8
    zrows = ny * own
    block = ny * 128
    near_z = by_distance(nz)
    near_y = by_distance(ny)
    near_x = by_distance(nx)
    far_z = near_z[::-1]
    next_z = [d for d in near_z if min(d, nz - d) == 1]
    rest_z = [d for d in near_z if d not in next_z]
    contract = (((1,), (1,)), ((), ()))

    def remote(src, dst, send, recv, **to):
        return pltpu.make_async_remote_copy(
            src_ref=src, dst_ref=dst, send_sem=send, recv_sem=recv, device_id=to, device_id_type=MESH
        )

    def push(*args, **to):
        copy = remote(*args, **to)
        copy.start()
        return copy

    def await_sent(ref, sem):
        remote(ref, ref, sem, sem, tp=other).wait_send()

    def await_all(ref, sem):
        remote(ref, ref, sem, sem, tp=other).wait_recv()

    barrier = pltpu.get_barrier_semaphore()
    for d in near_z:
        for t in range(2):
            pl.semaphore_signal(
                barrier, inc=1, device_id={"z": (z + d) % nz, "tp": t}, device_id_type=MESH
            )
    for d in near_y:
        pl.semaphore_signal(barrier, inc=1, device_id={"y": (y + d) % ny}, device_id_type=MESH)
    for d in near_x:
        pl.semaphore_signal(barrier, inc=1, device_id={"dp": (x_rank + d) % nx}, device_id_type=MESH)
    pl.semaphore_signal(barrier, inc=1, device_id={"tp": other}, device_id_type=MESH)

    depth = heads * 128

    def out_columns(k):
        return pl.ds(pl.multiple_of(k * 128, 128), 128)

    rows_of_block = pl.ds(pl.multiple_of(z * block, block), block)
    loads = [
        pltpu.make_async_copy(w_in.at[:, rows_of_block], wig, local_sem.at[0]),
        pltpu.make_async_copy(w_forget.at[:, rows_of_block], wfg, local_sem.at[1]),
        pltpu.make_async_copy(memory, mem, local_sem.at[2]),
        pltpu.make_async_copy(w_out, wo_all.at[tp, :, out_columns(y)], local_sem.at[3]),
        pltpu.make_async_copy(w_up, up_all.at[tp], local_sem.at[4]),
        pltpu.make_async_copy(w_down, down_all.at[tp], local_sem.at[5]),
    ]
    raw_loads = [
        pltpu.make_async_copy(w, w_raw.at[m], local_sem.at[6 + m])
        for m, w in enumerate((w0, w1, w2, w3))
    ]
    small = [
        pltpu.make_async_copy(src, dst, small_sem.at[i])
        for i, (src, dst) in enumerate(
            (
                (tokens_hbm, tokens),
                (gain_mixer_hbm, gain_mixer),
                (bias_in_hbm, bias_in),
                (bias_forget_hbm, bias_forget),
                (normalizer_hbm, normalizer),
                (stabilizer_hbm, stabilizer),
                (head_gain_hbm, head_gain),
                (gain_channel_hbm, gain_channel),
            )
        )
    ]
    for copy in raw_loads + small:
        copy.start()
    chunks = heads // 2
    direct_chunks = chunks // 2
    shared_chunks = range(direct_chunks, chunks)

    def flatten(m, which):
        for c in which:
            for i in range(2):
                w_own[m, c, :, i * 128 : (i + 1) * 128] = wide[
                    m, pl.ds(2 * c + i, 128, stride=heads), :
                ].astype(BF16)

    for m in range(4):
        raw_loads[m].wait()
        wide[m] = w_raw[m].astype(F32).reshape(128 * heads, 128)
        flatten(m, shared_chunks)
    small[0].wait()
    pl.semaphore_wait(barrier, 2 * (nz - 1) + (ny - 1) + (nx - 1) + 1)

    tok_copy = push(tokens, tok_in, pair_send.at[0], pair_recv.at[0], tp=other)
    own_block = pl.ds(pl.multiple_of(y * 128, 128), 128)

    def send_chunk(c):
        for d in near_y:
            to = (y + d) % ny
            push(
                w_own.at[to, c],
                w_flat.at[c, own_block],
                sent.at[WY],
                wy_recv.at[c],
                y=to,
            )

    some = 128 // nx

    def share_of(k):
        return pl.ds(pl.multiple_of(k * 128 + x_rank * some, some), some)

    for c in shared_chunks:
        for d in near_y:
            to = (y + d) % ny
            push(
                w_own.at[to, c, share_of(0)], w_flat.at[c, share_of(y)], sent.at[WQ], wq_recv.at[c], y=to
            )
    for copy in loads:
        copy.start()
    for m in range(4):
        flatten(m, range(direct_chunks))
    for copy in small[1:]:
        copy.wait()
    gains[0] = gain_mixer[...].astype(F32)
    gains[1] = gain_channel[...].astype(F32)
    tok_copy.wait_recv()
    mine, theirs = tokens[...].astype(F32), tok_in[...].astype(F32)
    first = jnp.where(tp == 0, mine, theirs)
    second = jnp.where(tp == 0, theirs, mine)
    chip = jnp.concatenate([first, second], axis=0).T.astype(BF16)
    tok_all[y] = chip
    for d in near_y:
        push(
            tok_all.at[y], tok_all.at[y], sent.at[TY], arrived.at[TY], y=(y + d) % ny
        )
    for c in range(direct_chunks):
        send_chunk(c)
    direct = depth // 2
    part = (depth - direct) // nx
    share = pl.ds(pl.multiple_of(direct + x_rank * part, part), part)
    for d in near_y:
        to = (y + d) % ny
        push(w_out.at[share], wo_all.at[tp, share, out_columns(y)], sent.at[OY], arrived.at[OY], y=to)
    head = pl.ds(0, direct)
    for d in near_y:
        to = (y + d) % ny
        push(w_out.at[head], wo_all.at[tp, head, out_columns(y)], sent.at[OD], arrived.at[OD], y=to)
    own_out = wo_all.at[tp, :, out_columns(y)]
    out_copy = push(w_out, own_out, pair_send.at[1], pair_recv.at[1], tp=other)
    for c in range(chunks):
        w_flat[c, own_block] = w_own[y, c]
    for c in shared_chunks:
        await_all(w_flat.at[c, : (ny - 1) * some], wq_recv.at[c])
        for d in near_y:
            there = w_flat.at[c, share_of((y + d) % ny)]
            for e in near_x:
                push(there, there, sent.at[WX], wy_recv.at[c], dp=(x_rank + e) % nx)
    await_all(tok_all.at[: ny - 1], arrived.at[TY])
    x = jnp.concatenate(
        [
            (tok_all[s].astype(F32) * gains[0, pl.ds(z * ny + s, 1), :]).astype(BF16)
            for s in range(ny)
        ],
        axis=1,
    )

    def project(c):
        product = jnp.dot(x, w_flat[c], preferred_element_type=F32)
        for k in range(nz):
            part_send[c, k] = jnp.concatenate(
                [
                    product[k * zrows : (k + 1) * zrows, :128],
                    product[k * zrows : (k + 1) * zrows, 128:],
                ],
                axis=0,
            ).astype(BF16)
        for d in far_z:
            to = (z + d) % nz
            push(
                part_send.at[c, to], part_recv.at[c, z], sent.at[PZ], pz_recv.at[c], z=to
            )

    squares = jnp.zeros((rows, 1), F32)
    for s in range(ny):
        wide_rows = tok_all[s].astype(F32)
        squares = squares + jnp.sum(wide_rows * wide_rows, axis=1, keepdims=True)
    loads[0].wait()
    loads[1].wait()
    gate = jnp.concatenate(
        [
            lax.dot_general(x, wig[...], contract, preferred_element_type=F32),
            lax.dot_general(x, wfg[...], contract, preferred_element_type=F32),
            jnp.broadcast_to(squares, (rows, 8)),
        ],
        axis=1,
    )
    for k in range(nz):
        groups = [gate[k * zrows + g * 8 : k * zrows + (g + 1) * 8] for g in range(zrows // 8)]
        gate_send[k] = jnp.concatenate(groups + [jnp.zeros((8, 128 - 5 * zrows), F32)], axis=1)
    for d in far_z:
        to = (z + d) % nz
        push(gate_send.at[to], gate_recv.at[z], sent.at[GZ], arrived.at[GZ], z=to)

    sequence = [direct_chunks, 0] + list(range(direct_chunks + 1, chunks)) + list(range(1, direct_chunks))
    for c in sequence:
        if c < direct_chunks:
            await_all(w_flat.at[c, : (ny - 1) * 128], wy_recv.at[c])
        elif nx > 1:
            await_all(w_flat.at[c, : (ny - 1) * (nx - 1) * some], wy_recv.at[c])
        project(c)

    await_all(wo_all.at[tp, share, : (ny - 1) * 128], arrived.at[OY])
    for d in near_y:
        there = wo_all.at[tp, share, out_columns((y + d) % ny)]
        for e in near_x:
            push(there, there, sent.at[OX], arrived.at[OX], dp=(x_rank + e) % nx)
    up_copy = push(w_up, up_all.at[tp], pair_send.at[2], pair_recv.at[2], tp=other)
    down_copy = push(w_down, down_all.at[tp], pair_send.at[3], pair_recv.at[3], tp=other)

    loads[2].wait()

    def split(i, carry):
        m_bh = mem[i]
        high = m_bh.astype(BF16)
        mem_split[i, :, :128] = high
        mem_split[i, :, 128:] = (m_bh - high.astype(F32)).astype(BF16)
        return carry

    lax.fori_loop(0, own * heads, split, 0)

    at = lax.broadcasted_iota(jnp.int32, (half_z * own, rows), 0)
    row = at + tp * half + y * own
    for k in range(1, half_z):
        row = row + jnp.where(at >= k * own, zrows - own, 0)
    chosen = jnp.where(
        lax.broadcasted_iota(jnp.int32, (half_z * own, rows), 1) == row, 1.0, 0.0
    ).astype(BF16)
    residual[...] = jnp.dot(
        chosen,
        jnp.concatenate([tok_all[k] for k in range(ny)], axis=1),
        preferred_element_type=F32,
    )

    await_all(gate_recv.at[: nz - 1], arrived.at[GZ])
    gate_sum = gate_send[z]
    for d in near_z:
        gate_sum = gate_sum + gate_recv[(z + d) % nz]
    gate_sum = jnp.concatenate(
        [gate_sum[:, g * 40 : (g + 1) * 40] for g in range(zrows // 8)], axis=0
    )
    inverse = lax.rsqrt(gate_sum[:, 32:33] / width_full + EPS)
    gate_pre = inverse * gate_sum
    gate_rows = jnp.zeros((own, 40), F32)
    for k in range(ny):
        gate_rows = gate_rows + jnp.where(y == k, gate_pre[k * own : (k + 1) * own], 0.0)
    in_all = gate_rows[:, 0:16] + bias_in[...]
    forget_all = gate_rows[:, 16:32] + bias_forget[...]
    ingate = jnp.where(tp == 0, in_all[:, :8], in_all[:, 8:])
    forget_pre = jnp.where(tp == 0, forget_all[:, :8], forget_all[:, 8:])
    forget = jnp.minimum(forget_pre, 0.0) - jnp.log(1.0 + jnp.exp(-jnp.abs(forget_pre)))
    carried = forget + stabilizer[...]
    new_stab = jnp.maximum(carried, ingate)
    packed[4 * own * heads : 4 * own * heads + own, :heads] = new_stab
    diagonal = lax.broadcasted_iota(jnp.int32, (heads, heads), 0) == lax.broadcasted_iota(
        jnp.int32, (heads, heads), 1
    )

    def column(value):
        return jnp.concatenate(
            [
                jnp.sum(
                    jnp.where(diagonal, jnp.broadcast_to(value[b : b + 1], (heads, heads)), 0.0),
                    axis=1,
                    keepdims=True,
                )
                for b in range(own)
            ],
            axis=0,
        )

    retain = column(jnp.exp(carried - new_stab))
    inflow = column(jnp.exp(ingate - new_stab))
    floor = column(jnp.exp(-new_stab))

    for c in sequence:
        await_all(part_recv.at[c, : nz - 1], pz_recv.at[c])
        total = part_send[c, z].astype(F32)
        for d in near_z:
            src = (z + d) % nz
            total = total + part_recv[c, src].astype(F32)
        for i in range(2):
            rows_wide[pl.ds(2 * c + i, zrows, stride=heads), :] = (
                inverse * total[i * zrows : (i + 1) * zrows]
            )
    piece = own * heads
    for k in range(ny):
        rows_send[k] = rows_wide[k * piece : (k + 1) * piece, :].astype(BF16)
    for d in near_y:
        to = (y + d) % ny
        push(rows_send.at[to], rows_recv.at[y], sent.at[RY], arrived.at[RY], y=to)
    rows_recv[y] = rows_send[y]
    await_all(rows_recv.at[: ny - 1], arrived.at[RY])

    query = rows_recv[0].astype(F32)
    key = rows_recv[1].astype(F32) * 128**-0.5
    value = rows_recv[2].astype(F32)
    gate_o = rows_recv[3].astype(F32)
    q_twice[...] = jnp.concatenate([query, query], axis=1)
    new_norm = retain * normalizer[...] + inflow * key
    packed[3 * piece : 4 * piece] = new_norm
    inflow_value = inflow * value
    packed[:piece] = inflow_value
    packed[piece : 2 * piece] = key
    packed[2 * piece : 3 * piece] = jnp.broadcast_to(retain, (piece, 128))
    sub = lax.broadcasted_iota(jnp.int32, (heads, 128), 0)

    for b in range(own):
        these = slice(b * heads, (b + 1) * heads)
        product = lax.dot_general(
            q_twice[these, :].astype(BF16),
            mem_split[these].reshape(heads * 128, 256),
            contract,
            preferred_element_type=F32,
        )
        found = product[:, :128]
        for h in range(1, heads):
            found = jnp.where(sub == h, product[:, h * 128 : (h + 1) * 128], found)
        mq[these, :] = found
    numerator = retain * mq[...] + inflow_value * jnp.sum(key * query, axis=1, keepdims=True)
    denominator = jnp.sum(new_norm * query, axis=1, keepdims=True)
    readout = numerator / jnp.maximum(jnp.abs(denominator), floor)
    centered = readout - jnp.mean(readout, axis=1, keepdims=True)
    normed = centered * lax.rsqrt(jnp.mean(centered * centered, axis=1, keepdims=True) + EPS)
    gain_all = head_gain[...].astype(F32)
    gain_own = jnp.where(tp == 0, gain_all[:heads], gain_all[heads:])
    heads_out = (
        normed * jnp.concatenate([gain_own] * own, axis=0) * (1.0 / (1.0 + jnp.exp(-gate_o)))
    ).astype(BF16)
    heads_own[...] = heads_out

    core = z // half_z
    zl = z % half_z

    @pl.when(tp == core)
    def _():
        heads_all[2 * zl + tp] = heads_out

    for d in far_z:
        push(
            heads_own,
            heads_all.at[2 * zl + tp],
            sent.at[HZ],
            arrived.at[HZ],
            z=(z + d) % nz,
            tp=core,
        )

    @pl.when(tp != core)
    def _():
        push(heads_own, heads_all.at[2 * zl + tp], sent.at[HZ], arrived.at[HZ], tp=other)

    loads[3].wait()
    if nx > 1:
        passed_on = wo_all.at[tp, : part * (nx - 1), : (ny - 1) * 128]
        await_all(passed_on, arrived.at[OX])
    await_all(wo_all.at[tp, head, : (ny - 1) * 128], arrived.at[OD])
    for d in near_y:
        whole = wo_all.at[tp, :, out_columns((y + d) % ny)]
        push(whole, whole, sent.at[OP], arrived.at[OP], tp=other)

    @pl.when(tp == core)
    def _():
        await_all(heads_all.at[: nz - 1], arrived.at[HZ])

    @pl.when(tp != core)
    def _():
        await_all(heads_all, arrived.at[HZ])

    for k in range(half_z):
        for t in range(2):
            start = (t * half_z + k) * piece
            heads_f32[start : start + piece, :] = heads_all[2 * k + t].astype(F32)
    mrows = half_z * own
    gathered = jnp.concatenate(
        [
            heads_f32[pl.ds(t * half_z * piece + h, mrows, stride=heads), :].astype(BF16)
            for t in range(2)
            for h in range(heads)
        ],
        axis=1,
    )
    out_copy.wait_recv()
    await_all(wo_all.at[other, :, : (ny - 1) * 128], arrived.at[OP])
    attended = jnp.dot(
        gathered, wo_all[...].reshape(2 * depth, block), preferred_element_type=F32
    )
    mixed = residual[...] + attended
    wcols = block // 2
    mixed_all[z, y] = jnp.concatenate([mixed[:, :wcols], mixed[:, wcols:]], axis=0).astype(BF16)

    mine_here = mixed_all.at[z, y]
    for e in near_y:
        push(mine_here, mine_here, sent.at[MY], my_recv.at[z], y=(y + e) % ny)
    for d in rest_z + next_z:
        push(mine_here, mine_here, sent.at[MZ], mz_recv.at[z], z=(z + d) % nz)
    await_all(mixed_all.at[z, : ny - 1], my_recv.at[z])
    for e in near_y:
        there = mixed_all.at[z, (y + e) % ny]
        for d in next_z:
            push(there, there, sent.at[MN], mz_recv.at[z], z=(z + d) % nz)
    for d in rest_z:
        s = (z + d) % nz
        here = mixed_all.at[s, y]
        await_all(here, mz_recv.at[s])
        for e in near_y:
            push(here, here, sent.at[MY], my_recv.at[s], y=(y + e) % ny)
    loads[4].wait()
    up_copy.wait_recv()
    hidden = up_all.shape[2]
    squares = [jnp.zeros((mrows, 1), F32)] * ny
    for d in [0] + near_z:
        s = (z + d) % nz
        if d in next_z:
            await_all(mixed_all.at[s], mz_recv.at[s])
        elif d:
            await_all(mixed_all.at[s, : ny - 1], my_recv.at[s])
        gain = jnp.concatenate([gains[1, pl.ds(s * ny + k, 1), :] for k in range(ny)], axis=1)
        scaled = []
        for k in range(ny):
            stacked = mixed_all[s, k].astype(F32)
            wide_rows = jnp.concatenate([stacked[:mrows], stacked[mrows:]], axis=1)
            squares[k] = squares[k] + jnp.sum(wide_rows * wide_rows, axis=1, keepdims=True)
            scaled.append(wide_rows * gain)
        lhs = jnp.concatenate(scaled, axis=0).astype(BF16)
        here = pl.ds(pl.multiple_of(s * block, block), block)
        for t in range(2):
            product = jnp.dot(lhs, up_all[t, here, :], preferred_element_type=F32)
            if d:
                product = product + acc[t]
            acc[t] = product
    inverse_mlp = lax.rsqrt(jnp.concatenate(squares, axis=0) / width_full + EPS)
    squared = []
    for t in range(2):
        activation = jnp.maximum(inverse_mlp * acc[t], 0.0)
        squared.append((activation * activation).astype(BF16))

    loads[5].wait()
    down_copy.wait_recv()
    rest = rest_z[::-1]
    for d in rest[:1] + next_z + rest[1:] + [0]:
        to = (z + d) % nz
        here = pl.ds(pl.multiple_of(to * block, block), block)
        product = jnp.dot(
            squared[0], down_all[0, :, here], preferred_element_type=F32
        ) + jnp.dot(squared[1], down_all[1, :, here], preferred_element_type=F32)
        for k in range(ny):
            piece_k = product[:, k * 128 : (k + 1) * 128]
            if d:
                down_send[to, k] = piece_k.astype(BF16)
            else:
                down_own[k] = piece_k
        if d in next_z:
            push(
                down_send.at[to],
                down_next.at[next_z.index(d)],
                sent.at[DN],
                arrived.at[DN],
                z=to,
            )
        elif d:
            for e in near_y:
                dst = (y + e) % ny
                push(
                    down_send.at[to, dst], down_y.at[y, to], sent.at[DY], dy_recv.at[to], y=dst
                )
    carried = []
    for k in range(ny):
        stacked = mixed_all[z, k].astype(F32)
        mine = jnp.zeros((mrows, 128), F32)
        for c in range(ny):
            down, across = c // (ny // 2) * mrows, c % (ny // 2) * 128
            mine = jnp.where(y == c, stacked[down : down + mrows, across : across + 128], mine)
        carried.append(mine)
    carried = jnp.concatenate(carried, axis=0)
    quarter = half // 2

    def columns_of(value, t):
        cols = value[:, 64 * t : 64 * (t + 1)]
        return jnp.concatenate([cols[:quarter], cols[quarter:]], axis=1)

    def add_next():
        await_all(down_next, arrived.at[DN])
        for k in range(ny):
            added = down_own[k]
            for i in range(len(next_z)):
                added = added + down_next[i, k].astype(F32)
            down_own[k] = added
            down_send[z, k] = added.astype(BF16)
        for e in near_y:
            dst = (y + e) % ny
            push(down_send.at[z, dst], down_y.at[y, z], sent.at[DY], dy_recv.at[z], y=dst)

    if not rest:
        add_next()
    for d in rest + [0]:
        to = (z + d) % nz
        await_all(down_y.at[: ny - 1, to], dy_recv.at[to])
        summed = down_send[to, y].astype(F32) if d else down_own[y]
        for e in near_y:
            summed = summed + down_y[(y + e) % ny, to].astype(F32)
        if d:
            for t in range(2):
                sum_send[t, to] = columns_of(summed, t).astype(BF16)
                push(sum_send.at[t, to], sum_recv.at[tp, z], sent.at[DZ], arrived.at[DZ], z=to, tp=t)
            if d == rest[0]:
                add_next()
        else:
            whole = summed + carried
            fin_send[0] = columns_of(whole, 0)
            fin_send[1] = columns_of(whole, 1)
            fin_copy = push(
                fin_send.at[other], fin_recv, pair_send.at[4], pair_recv.at[4], tp=other
            )
    if rest:
        await_all(sum_recv.at[:, : len(rest)], arrived.at[DZ])
    total = [fin_send[tp], jnp.zeros((quarter, 128), F32)]
    for d in rest:
        src = (z + d) % nz
        total[0] = total[0] + sum_recv[tp, src].astype(F32)
        total[1] = total[1] + sum_recv[other, src].astype(F32)
    fin_copy.wait_recv()
    total[1] = total[1] + fin_recv[...]
    top = 4 * piece + 8
    packed[top : top + quarter] = jnp.where(tp == 0, total[0], total[1])
    packed[top + quarter : top + half] = jnp.where(tp == 0, total[1], total[0])

    for copy in (tok_copy, out_copy, up_copy, down_copy, fin_copy):
        copy.wait_send()
    await_sent(w_own.at[: ny - 1, :direct_chunks], sent.at[WY])
    await_sent(w_flat.at[direct_chunks:, : (ny - 1) * some], sent.at[WQ])
    await_sent(wo_all.at[tp, head, : (ny - 1) * 128], sent.at[OD])
    await_sent(tok_all.at[: ny - 1], sent.at[TY])
    await_sent(part_send.at[:, : nz - 1], sent.at[PZ])
    await_sent(gate_send.at[: nz - 1], sent.at[GZ])
    await_sent(rows_send.at[: ny - 1], sent.at[RY])
    await_sent(wo_all.at[tp, share, : (ny - 1) * 128], sent.at[OY])
    if nx > 1:
        await_sent(w_flat.at[direct_chunks:, : (ny - 1) * (nx - 1) * some], sent.at[WX])
        await_sent(passed_on, sent.at[OX])
    await_sent(wo_all.at[tp, :, : (ny - 1) * 128], sent.at[OP])
    await_sent(mixed_all.at[: nz - 1, 0], sent.at[MZ])
    await_sent(mixed_all.at[: len(next_z), : ny - 1], sent.at[MN])
    await_sent(mixed_all.at[: nz - len(next_z), : ny - 1], sent.at[MY])
    await_sent(down_next, sent.at[DN])
    await_sent(down_send.at[: nz - len(next_z), : ny - 1], sent.at[DY])
    if rest:
        await_sent(sum_send.at[:, : len(rest)], sent.at[DZ])

    @pl.when(tp == core)
    def _():
        await_sent(heads_all.at[: nz - 1], sent.at[HZ])

    @pl.when(tp != core)
    def _():
        await_sent(heads_all, sent.at[HZ])


def update(ny, mem, packed, new_mem, out_hbm, norm_hbm, stab_hbm, made, out, stab, sems):
    piece = mem.shape[0]
    own = stab.shape[0]
    count = sems.shape[0] - 3
    each = piece // count
    copies = []

    def send(src, dst):
        copies.append(pltpu.make_async_copy(src, dst, sems.at[len(copies)]))
        copies[-1].start()

    inflow_v = packed[:piece].T
    for b in range(count):
        for i in range(b * each, (b + 1) * each):
            key, retain = packed[piece + i], packed[2 * piece + i]
            made[i] = retain[None] * mem[i] + inflow_v[:, i : i + 1] * key[None]
        here = pl.ds(b * each, each)
        send(made.at[here], new_mem.at[here])
        if b == 0:
            send(packed.at[pl.ds(3 * piece, piece)], norm_hbm)
            stab[...] = packed[4 * piece : 4 * piece + own, : stab.shape[1]]
            send(stab, stab_hbm)
            rows = out.shape[1]
            blocks = rows // own // 2
            per = blocks // ny
            quarter = rows // 4
            line = lax.broadcasted_iota(jnp.int32, (rows // 2, rows), 0).astype(F32)
            column = lax.broadcasted_iota(jnp.int32, (rows // 2, rows), 1).astype(F32)
            side = jnp.where(line >= quarter, 1.0, 0.0)
            orders = []
            for upper in range(2):
                at = line + side * quarter + upper * quarter
                group = jnp.floor((at + 0.5) / own)
                inner = group - side * blocks
                in_y = jnp.floor((inner + 0.5) / per)
                in_z = inner - in_y * per
                target = (side * blocks + in_z * ny + in_y) * own + (at - group * own)
                orders.append(jnp.where(column == target, 1.0, 0.0).astype(BF16))
            result = packed[4 * piece + 8 :].T.astype(BF16)
            turned = jnp.dot(result[:64], orders[0], preferred_element_type=F32) + jnp.dot(
                result[64:], orders[1], preferred_element_type=F32
            )
            out[...] = turned.astype(BF16)
            send(out, out_hbm)
    for copy in copies:
        copy.wait()


def body(
    tokens,
    gain_mixer,
    weight_query,
    weight_key,
    weight_value,
    weight_outgate,
    weight_ingate,
    weight_forget,
    bias_input,
    bias_forget,
    memory,
    normalizer,
    stabilizer,
    head_gain,
    weight_out,
    gain_channel,
    weight_up,
    weight_down,
):
    nx, nz, ny = lax.axis_size("dp"), lax.axis_size("z"), lax.axis_size("y")
    own, heads, hd = memory.shape[:3]
    width_full = gain_mixer.shape[0]
    tokens = tokens.T
    rows = tokens.shape[1]
    half = rows // 2
    piece = own * heads
    zrows = ny * own
    block = ny * 128
    chunks = heads // 2
    mrows = nz // 2 * own
    dma = pltpu.SemaphoreType.DMA
    vmem = pl.BlockSpec(memory_space=pltpu.VMEM)
    hbm = pl.BlockSpec(memory_space=pl.ANY)
    mem48 = memory.reshape(piece, hd, hd)
    small = (
        tokens,
        gain_mixer.reshape(-1, 128),
        bias_input.reshape(1, -1),
        bias_forget.reshape(1, -1),
        normalizer.reshape(piece, hd),
        stabilizer,
        head_gain,
        gain_channel.reshape(-1, 128),
    )
    packed = pl.pallas_call(
        functools.partial(kernel, nx, nz, ny, width_full),
        out_shape=jax.ShapeDtypeStruct((4 * piece + 8 + half, hd), F32),
        in_specs=[hbm] * 18,
        out_specs=vmem,
        scratch_shapes=[pltpu.VMEM(value.shape, value.dtype) for value in small]
        + [
            pltpu.VMEM(tokens.shape, BF16),
            pltpu.VMEM((ny, rows, 128), BF16),
            pltpu.VMEM((mrows, block), F32),
            pltpu.VMEM((2, width_full // 128, 128), F32),
            pltpu.VMEM((16, block), BF16),
            pltpu.VMEM((16, block), BF16),
            pltpu.VMEM((piece, hd, hd), F32),
            pltpu.VMEM((piece, hd, 2 * hd), BF16),
            pltpu.VMEM((ny, 128, heads, hd), BF16),
            pltpu.VMEM((4, 128 * heads, hd), F32),
            pltpu.VMEM((ny, chunks, 128, 2 * hd), BF16),
            pltpu.VMEM((chunks, block, 2 * hd), BF16),
            pltpu.VMEM((chunks, nz, 2 * zrows, hd), BF16),
            pltpu.VMEM((chunks, nz, 2 * zrows, hd), BF16),
            pltpu.VMEM((nz, 8, 128), F32),
            pltpu.VMEM((nz, 8, 128), F32),
            pltpu.VMEM((zrows * heads, hd), F32),
            pltpu.VMEM((ny, piece, hd), BF16),
            pltpu.VMEM((ny, piece, hd), BF16),
            pltpu.VMEM((piece, 2 * hd), F32),
            pltpu.VMEM((piece, hd), F32),
            pltpu.VMEM((piece, hd), BF16),
            pltpu.VMEM((nz, piece, hd), BF16),
            pltpu.VMEM((nz * piece, hd), F32),
            pltpu.VMEM((2, heads * hd, block), BF16),
            pltpu.VMEM((2, *weight_up.shape), BF16),
            pltpu.VMEM((2, *weight_down.shape), BF16),
            pltpu.VMEM((nz, ny, 2 * mrows, block // 2), BF16),
            pltpu.VMEM((2, half, weight_up.shape[1]), F32),
            pltpu.VMEM((nz, ny, half, 128), BF16),
            pltpu.VMEM((ny, half, 128), F32),
            pltpu.VMEM((min(2, nz - 1), ny, half, 128), BF16),
            pltpu.VMEM((ny, nz, half, 128), BF16),
            pltpu.VMEM((2, nz, half // 2, 128), BF16),
            pltpu.VMEM((2, nz, half // 2, 128), BF16),
            pltpu.VMEM((2, half // 2, 128), F32),
            pltpu.VMEM((half // 2, 128), F32),
            dma((8,)),
            dma((10,)),
            dma((5,)),
            dma((5,)),
            dma((len(PHASES),)),
            dma((len(PHASES),)),
            dma((chunks,)),
            dma((chunks,)),
            dma((chunks,)),
            dma((nz,)),
            dma((nz,)),
            dma((nz,)),
        ],
        compiler_params=pltpu.CompilerParams(
            collective_id=0, has_side_effects=True, vmem_limit_bytes=56 * 1024 * 1024
        ),
    )(
        *small,
        weight_query,
        weight_key,
        weight_value,
        weight_outgate,
        weight_ingate.T,
        weight_forget.T,
        mem48,
        weight_out,
        weight_up,
        weight_down,
    )
    new_memory, layer_out, new_norm, new_stab = pl.pallas_call(
        functools.partial(update, ny),
        out_shape=(
            jax.ShapeDtypeStruct(mem48.shape, F32),
            jax.ShapeDtypeStruct(tokens.shape, BF16),
            jax.ShapeDtypeStruct((piece, hd), F32),
            jax.ShapeDtypeStruct((own, heads), F32),
        ),
        in_specs=[vmem, vmem],
        out_specs=(hbm,) * 4,
        scratch_shapes=[
            pltpu.VMEM(mem48.shape, F32),
            pltpu.VMEM(tokens.shape, BF16),
            pltpu.VMEM((own, heads), F32),
            dma((piece // 4 + 3,)),
        ],
        compiler_params=pltpu.CompilerParams(vmem_limit_bytes=16 * 1024 * 1024),
    )(mem48, packed)
    new_memory = new_memory.reshape(memory.shape)
    return (layer_out.T, new_memory, new_norm.reshape(normalizer.shape), new_stab)


def solution(mesh):
    kv = mesh.shape["kv"]
    ny = 4
    torus = Mesh(
        mesh.devices.reshape(mesh.shape["dp"], kv // ny, ny, mesh.shape["tp"]),
        ("dp", "z", "y", "tp"),
    )
    placed = (
        P("dp", KV_TP),
        P(),
        P(KV, "tp", None),
        P(KV, "tp", None),
        P(KV, "tp", None),
        P(KV, "tp", None),
        P(),
        P(),
        P(),
        P(),
        P(DP_KV, "tp", None, None),
        P(DP_KV, "tp", None),
        P(DP_KV, "tp"),
        P(),
        P("tp", KV),
        P(),
        P(None, KV_TP),
        P(KV_TP, None),
    )
    return jax.shard_map(
        body,
        mesh=torus,
        in_specs=placed,
        out_specs=(
            P("dp", KV_TP),
            P(DP_KV, "tp", None, None),
            P(DP_KV, "tp", None),
            P(DP_KV, "tp"),
        ),
        check_vma=False,
    )
```

```python
import functools

import jax
import jax.numpy as jnp
from jax import lax
from jax.experimental import pallas as pl
from jax.experimental.pallas import tpu as pltpu
from jax.sharding import Mesh
from jax.sharding import PartitionSpec as P

EPS = 1e-06
KV_TP = ("z", "y", "tp")
KV = ("z", "y")
DP_KV = ("dp", "z", "y")
MESH = pl.DeviceIdType.MESH
PHASES = WY, WQ, WX, TY, PZ, GZ, RY, HZ, OY, OX, OD, OP, MZ, MN, MY, DN, DY, DZ = range(18)
F32 = jnp.float32
BF16 = jnp.bfloat16


def by_distance(n):
    return sorted(range(1, n), key=lambda d: (min(d, n - d), d))


def kernel(
    nx,
    nz,
    ny,
    width_full,
    tokens_hbm,
    gain_mixer_hbm,
    bias_in_hbm,
    bias_forget_hbm,
    normalizer_hbm,
    stabilizer_hbm,
    head_gain_hbm,
    gain_channel_hbm,
    w0,
    w1,
    w2,
    w3,
    w_in,
    w_forget,
    memory,
    w_out,
    w_up,
    w_down,
    packed,
    tokens,
    gain_mixer,
    bias_in,
    bias_forget,
    normalizer,
    stabilizer,
    head_gain,
    gain_channel,
    tok_in,
    tok_all,
    residual,
    gains,
    wig,
    wfg,
    mem,
    mem_split,
    w_raw,
    wide,
    w_own,
    w_flat,
    part_send,
    part_recv,
    gate_send,
    gate_recv,
    rows_wide,
    rows_send,
    rows_recv,
    q_twice,
    mq,
    heads_own,
    heads_all,
    heads_f32,
    wo_all,
    up_all,
    down_all,
    mixed_all,
    acc,
    down_send,
    down_own,
    down_next,
    down_y,
    sum_send,
    sum_recv,
    fin_send,
    fin_recv,
    small_sem,
    local_sem,
    pair_send,
    pair_recv,
    sent,
    arrived,
    wy_recv,
    wq_recv,
    pz_recv,
    mz_recv,
    my_recv,
    dy_recv,
):
    x_rank = lax.axis_index("dp")
    z = lax.axis_index("z")
    y = lax.axis_index("y")
    tp = lax.axis_index("tp")
    other = 1 - tp
    half_z = nz // 2
    rows = tokens.shape[1]
    half = rows // 2
    own = 6
    heads = 8
    zrows = ny * own
    block = ny * 128
    near_z = by_distance(nz)
    near_y = by_distance(ny)[::-1]
    near_x = by_distance(nx)[::-1]
    far_z = near_z[::-1]
    next_z = [d for d in near_z if min(d, nz - d) == 1]
    rest_z = [d for d in near_z if d not in next_z]
    contract = (((1,), (1,)), ((), ()))

    def remote(src, dst, send, recv, **to):
        return pltpu.make_async_remote_copy(
            src_ref=src, dst_ref=dst, send_sem=send, recv_sem=recv, device_id=to, device_id_type=MESH
        )

    def push(*args, **to):
        copy = remote(*args, **to)
        copy.start()
        return copy

    def await_sent(ref, sem):
        remote(ref, ref, sem, sem, tp=other).wait_send()

    def await_all(ref, sem):
        remote(ref, ref, sem, sem, tp=other).wait_recv()

    barrier = pltpu.get_barrier_semaphore()
    for d in near_z:
        for t in range(2):
            pl.semaphore_signal(
                barrier, inc=1, device_id={"z": (z + d) % nz, "tp": t}, device_id_type=MESH
            )
    for d in near_y:
        pl.semaphore_signal(barrier, inc=1, device_id={"y": (y + d) % ny}, device_id_type=MESH)
    for d in near_x:
        pl.semaphore_signal(barrier, inc=1, device_id={"dp": (x_rank + d) % nx}, device_id_type=MESH)
    pl.semaphore_signal(barrier, inc=1, device_id={"tp": other}, device_id_type=MESH)

    depth = heads * 128

    def out_columns(k):
        return pl.ds(pl.multiple_of(k * 128, 128), 128)

    rows_of_block = pl.ds(pl.multiple_of(z * block, block), block)
    loads = [
        pltpu.make_async_copy(w_in.at[:, rows_of_block], wig, local_sem.at[0]),
        pltpu.make_async_copy(w_forget.at[:, rows_of_block], wfg, local_sem.at[1]),
        pltpu.make_async_copy(memory, mem, local_sem.at[2]),
        pltpu.make_async_copy(w_out, wo_all.at[tp, :, out_columns(y)], local_sem.at[3]),
        pltpu.make_async_copy(w_up, up_all.at[tp], local_sem.at[4]),
        pltpu.make_async_copy(w_down, down_all.at[tp], local_sem.at[5]),
    ]
    raw_loads = [
        pltpu.make_async_copy(w, w_raw.at[m], local_sem.at[6 + m])
        for m, w in enumerate((w0, w1, w2, w3))
    ]
    small = [
        pltpu.make_async_copy(src, dst, small_sem.at[i])
        for i, (src, dst) in enumerate(
            (
                (tokens_hbm, tokens),
                (gain_mixer_hbm, gain_mixer),
                (bias_in_hbm, bias_in),
                (bias_forget_hbm, bias_forget),
                (normalizer_hbm, normalizer),
                (stabilizer_hbm, stabilizer),
                (head_gain_hbm, head_gain),
                (gain_channel_hbm, gain_channel),
            )
        )
    ]
    for copy in raw_loads + small:
        copy.start()
    chunks = heads // 2
    direct_chunks = chunks // 2
    shared_chunks = range(direct_chunks, chunks)

    def flatten(m, which):
        for c in which:
            for i in range(2):
                w_own[m, c, :, i * 128 : (i + 1) * 128] = wide[
                    m, pl.ds(2 * c + i, 128, stride=heads), :
                ].astype(BF16)

    for m in range(4):
        raw_loads[m].wait()
        wide[m] = w_raw[m].astype(F32).reshape(128 * heads, 128)
        flatten(m, shared_chunks)
    small[0].wait()
    pl.semaphore_wait(barrier, 2 * (nz - 1) + (ny - 1) + (nx - 1) + 1)

    tok_copy = push(tokens, tok_in, pair_send.at[0], pair_recv.at[0], tp=other)
    own_block = pl.ds(pl.multiple_of(y * 128, 128), 128)

    def send_chunk(c):
        for d in near_y:
            to = (y + d) % ny
            push(
                w_own.at[to, c],
                w_flat.at[c, own_block],
                sent.at[WY],
                wy_recv.at[c],
                y=to,
            )

    some = 128 // nx

    def share_of(k):
        return pl.ds(pl.multiple_of(k * 128 + x_rank * some, some), some)

    for c in shared_chunks:
        for d in near_y:
            to = (y + d) % ny
            push(
                w_own.at[to, c, share_of(0)], w_flat.at[c, share_of(y)], sent.at[WQ], wq_recv.at[c], y=to
            )
    for copy in loads:
        copy.start()
    for m in range(4):
        flatten(m, range(direct_chunks))
    for copy in small[1:]:
        copy.wait()
    gains[0] = gain_mixer[...].astype(F32)
    gains[1] = gain_channel[...].astype(F32)
    tok_copy.wait_recv()
    mine, theirs = tokens[...].astype(F32), tok_in[...].astype(F32)
    first = jnp.where(tp == 0, mine, theirs)
    second = jnp.where(tp == 0, theirs, mine)
    chip = jnp.concatenate([first, second], axis=0).T.astype(BF16)
    tok_all[y] = chip
    for d in near_y:
        push(
            tok_all.at[y], tok_all.at[y], sent.at[TY], arrived.at[TY], y=(y + d) % ny
        )
    for c in range(direct_chunks):
        send_chunk(c)
    direct = depth // 2
    part = (depth - direct) // nx
    share = pl.ds(pl.multiple_of(direct + x_rank * part, part), part)
    for d in near_y:
        to = (y + d) % ny
        push(w_out.at[share], wo_all.at[tp, share, out_columns(y)], sent.at[OY], arrived.at[OY], y=to)
    head = pl.ds(0, direct)
    for d in near_y:
        to = (y + d) % ny
        push(w_out.at[head], wo_all.at[tp, head, out_columns(y)], sent.at[OD], arrived.at[OD], y=to)
    own_out = wo_all.at[tp, :, out_columns(y)]
    out_copy = push(w_out, own_out, pair_send.at[1], pair_recv.at[1], tp=other)
    for c in range(chunks):
        w_flat[c, own_block] = w_own[y, c]
    for c in shared_chunks:
        await_all(w_flat.at[c, : (ny - 1) * some], wq_recv.at[c])
        for d in near_y:
            there = w_flat.at[c, share_of((y + d) % ny)]
            for e in near_x:
                push(there, there, sent.at[WX], wy_recv.at[c], dp=(x_rank + e) % nx)
    await_all(tok_all.at[: ny - 1], arrived.at[TY])
    x = jnp.concatenate(
        [
            (tok_all[s].astype(F32) * gains[0, pl.ds(z * ny + s, 1), :]).astype(BF16)
            for s in range(ny)
        ],
        axis=1,
    )

    def project(c):
        product = jnp.dot(x, w_flat[c], preferred_element_type=F32)
        for k in range(nz):
            part_send[c, k] = jnp.concatenate(
                [
                    product[k * zrows : (k + 1) * zrows, :128],
                    product[k * zrows : (k + 1) * zrows, 128:],
                ],
                axis=0,
            ).astype(BF16)
        for d in far_z:
            to = (z + d) % nz
            push(
                part_send.at[c, to], part_recv.at[c, z], sent.at[PZ], pz_recv.at[c], z=to
            )

    squares = jnp.zeros((rows, 1), F32)
    for s in range(ny):
        wide_rows = tok_all[s].astype(F32)
        squares = squares + jnp.sum(wide_rows * wide_rows, axis=1, keepdims=True)
    loads[0].wait()
    loads[1].wait()
    gate = jnp.concatenate(
        [
            lax.dot_general(x, wig[...], contract, preferred_element_type=F32),
            lax.dot_general(x, wfg[...], contract, preferred_element_type=F32),
            jnp.broadcast_to(squares, (rows, 8)),
        ],
        axis=1,
    )
    for k in range(nz):
        groups = [gate[k * zrows + g * 8 : k * zrows + (g + 1) * 8] for g in range(zrows // 8)]
        gate_send[k] = jnp.concatenate(groups + [jnp.zeros((8, 128 - 5 * zrows), F32)], axis=1)
    for d in far_z:
        to = (z + d) % nz
        push(gate_send.at[to], gate_recv.at[z], sent.at[GZ], arrived.at[GZ], z=to)

    sequence = [direct_chunks, 0] + list(range(direct_chunks + 1, chunks)) + list(range(1, direct_chunks))
    for c in sequence:
        if c < direct_chunks:
            await_all(w_flat.at[c, : (ny - 1) * 128], wy_recv.at[c])
        elif nx > 1:
            await_all(w_flat.at[c, : (ny - 1) * (nx - 1) * some], wy_recv.at[c])
        project(c)

    await_all(wo_all.at[tp, share, : (ny - 1) * 128], arrived.at[OY])
    for d in near_y:
        there = wo_all.at[tp, share, out_columns((y + d) % ny)]
        for e in near_x:
            push(there, there, sent.at[OX], arrived.at[OX], dp=(x_rank + e) % nx)
    up_copy = push(w_up, up_all.at[tp], pair_send.at[2], pair_recv.at[2], tp=other)
    down_copy = push(w_down, down_all.at[tp], pair_send.at[3], pair_recv.at[3], tp=other)

    loads[2].wait()

    def split(i, carry):
        m_bh = mem[i]
        high = m_bh.astype(BF16)
        mem_split[i, :, :128] = high
        mem_split[i, :, 128:] = (m_bh - high.astype(F32)).astype(BF16)
        return carry

    lax.fori_loop(0, own * heads, split, 0)

    at = lax.broadcasted_iota(jnp.int32, (half_z * own, rows), 0)
    row = at + tp * half + y * own
    for k in range(1, half_z):
        row = row + jnp.where(at >= k * own, zrows - own, 0)
    chosen = jnp.where(
        lax.broadcasted_iota(jnp.int32, (half_z * own, rows), 1) == row, 1.0, 0.0
    ).astype(BF16)
    residual[...] = jnp.dot(
        chosen,
        jnp.concatenate([tok_all[k] for k in range(ny)], axis=1),
        preferred_element_type=F32,
    )

    await_all(gate_recv.at[: nz - 1], arrived.at[GZ])
    gate_sum = gate_send[z]
    for d in near_z:
        gate_sum = gate_sum + gate_recv[(z + d) % nz]
    gate_sum = jnp.concatenate(
        [gate_sum[:, g * 40 : (g + 1) * 40] for g in range(zrows // 8)], axis=0
    )
    inverse = lax.rsqrt(gate_sum[:, 32:33] / width_full + EPS)
    gate_pre = inverse * gate_sum
    gate_rows = jnp.zeros((own, 40), F32)
    for k in range(ny):
        gate_rows = gate_rows + jnp.where(y == k, gate_pre[k * own : (k + 1) * own], 0.0)
    in_all = gate_rows[:, 0:16] + bias_in[...]
    forget_all = gate_rows[:, 16:32] + bias_forget[...]
    ingate = jnp.where(tp == 0, in_all[:, :8], in_all[:, 8:])
    forget_pre = jnp.where(tp == 0, forget_all[:, :8], forget_all[:, 8:])
    forget = jnp.minimum(forget_pre, 0.0) - jnp.log(1.0 + jnp.exp(-jnp.abs(forget_pre)))
    carried = forget + stabilizer[...]
    new_stab = jnp.maximum(carried, ingate)
    packed[4 * own * heads : 4 * own * heads + own, :heads] = new_stab
    diagonal = lax.broadcasted_iota(jnp.int32, (heads, heads), 0) == lax.broadcasted_iota(
        jnp.int32, (heads, heads), 1
    )

    def column(value):
        return jnp.concatenate(
            [
                jnp.sum(
                    jnp.where(diagonal, jnp.broadcast_to(value[b : b + 1], (heads, heads)), 0.0),
                    axis=1,
                    keepdims=True,
                )
                for b in range(own)
            ],
            axis=0,
        )

    retain = column(jnp.exp(carried - new_stab))
    inflow = column(jnp.exp(ingate - new_stab))
    floor = column(jnp.exp(-new_stab))

    for c in sequence:
        await_all(part_recv.at[c, : nz - 1], pz_recv.at[c])
        total = part_send[c, z].astype(F32)
        for d in near_z:
            src = (z + d) % nz
            total = total + part_recv[c, src].astype(F32)
        for i in range(2):
            rows_wide[pl.ds(2 * c + i, zrows, stride=heads), :] = (
                inverse * total[i * zrows : (i + 1) * zrows]
            )
    piece = own * heads
    for k in range(ny):
        rows_send[k] = rows_wide[k * piece : (k + 1) * piece, :].astype(BF16)
    for d in near_y:
        to = (y + d) % ny
        push(rows_send.at[to], rows_recv.at[y], sent.at[RY], arrived.at[RY], y=to)
    rows_recv[y] = rows_send[y]
    await_all(rows_recv.at[: ny - 1], arrived.at[RY])

    query = rows_recv[0].astype(F32)
    key = rows_recv[1].astype(F32) * 128**-0.5
    value = rows_recv[2].astype(F32)
    gate_o = rows_recv[3].astype(F32)
    q_twice[...] = jnp.concatenate([query, query], axis=1)
    new_norm = retain * normalizer[...] + inflow * key
    packed[3 * piece : 4 * piece] = new_norm
    inflow_value = inflow * value
    packed[:piece] = inflow_value
    packed[piece : 2 * piece] = key
    packed[2 * piece : 3 * piece] = jnp.broadcast_to(retain, (piece, 128))
    sub = lax.broadcasted_iota(jnp.int32, (heads, 128), 0)

    for b in range(own):
        these = slice(b * heads, (b + 1) * heads)
        product = lax.dot_general(
            q_twice[these, :].astype(BF16),
            mem_split[these].reshape(heads * 128, 256),
            contract,
            preferred_element_type=F32,
        )
        found = product[:, :128]
        for h in range(1, heads):
            found = jnp.where(sub == h, product[:, h * 128 : (h + 1) * 128], found)
        mq[these, :] = found
    numerator = retain * mq[...] + inflow_value * jnp.sum(key * query, axis=1, keepdims=True)
    denominator = jnp.sum(new_norm * query, axis=1, keepdims=True)
    readout = numerator / jnp.maximum(jnp.abs(denominator), floor)
    centered = readout - jnp.mean(readout, axis=1, keepdims=True)
    normed = centered * lax.rsqrt(jnp.mean(centered * centered, axis=1, keepdims=True) + EPS)
    gain_all = head_gain[...].astype(F32)
    gain_own = jnp.where(tp == 0, gain_all[:heads], gain_all[heads:])
    heads_out = (
        normed * jnp.concatenate([gain_own] * own, axis=0) * (1.0 / (1.0 + jnp.exp(-gate_o)))
    ).astype(BF16)
    heads_own[...] = heads_out

    core = z // half_z
    zl = z % half_z

    @pl.when(tp == core)
    def _():
        heads_all[2 * zl + tp] = heads_out

    for d in far_z:
        push(
            heads_own,
            heads_all.at[2 * zl + tp],
            sent.at[HZ],
            arrived.at[HZ],
            z=(z + d) % nz,
            tp=core,
        )

    @pl.when(tp != core)
    def _():
        push(heads_own, heads_all.at[2 * zl + tp], sent.at[HZ], arrived.at[HZ], tp=other)

    loads[3].wait()
    if nx > 1:
        passed_on = wo_all.at[tp, : part * (nx - 1), : (ny - 1) * 128]
        await_all(passed_on, arrived.at[OX])
    await_all(wo_all.at[tp, head, : (ny - 1) * 128], arrived.at[OD])
    for d in near_y:
        whole = wo_all.at[tp, :, out_columns((y + d) % ny)]
        push(whole, whole, sent.at[OP], arrived.at[OP], tp=other)

    @pl.when(tp == core)
    def _():
        await_all(heads_all.at[: nz - 1], arrived.at[HZ])

    @pl.when(tp != core)
    def _():
        await_all(heads_all, arrived.at[HZ])

    for k in range(half_z):
        for t in range(2):
            start = (t * half_z + k) * piece
            heads_f32[start : start + piece, :] = heads_all[2 * k + t].astype(F32)
    mrows = half_z * own
    gathered = jnp.concatenate(
        [
            heads_f32[pl.ds(t * half_z * piece + h, mrows, stride=heads), :].astype(BF16)
            for t in range(2)
            for h in range(heads)
        ],
        axis=1,
    )
    out_copy.wait_recv()
    await_all(wo_all.at[other, :, : (ny - 1) * 128], arrived.at[OP])
    attended = jnp.dot(
        gathered, wo_all[...].reshape(2 * depth, block), preferred_element_type=F32
    )
    mixed = residual[...] + attended
    wcols = block // 2
    mixed_all[z, y] = jnp.concatenate([mixed[:, :wcols], mixed[:, wcols:]], axis=0).astype(BF16)

    mine_here = mixed_all.at[z, y]
    for e in near_y:
        push(mine_here, mine_here, sent.at[MY], my_recv.at[z], y=(y + e) % ny)
    for d in rest_z + next_z:
        push(mine_here, mine_here, sent.at[MZ], mz_recv.at[z], z=(z + d) % nz)
    await_all(mixed_all.at[z, : ny - 1], my_recv.at[z])
    for e in near_y:
        there = mixed_all.at[z, (y + e) % ny]
        for d in next_z:
            push(there, there, sent.at[MN], mz_recv.at[z], z=(z + d) % nz)
    for d in rest_z:
        s = (z + d) % nz
        here = mixed_all.at[s, y]
        await_all(here, mz_recv.at[s])
        for e in near_y:
            push(here, here, sent.at[MY], my_recv.at[s], y=(y + e) % ny)
    loads[4].wait()
    up_copy.wait_recv()
    hidden = up_all.shape[2]
    squares = [jnp.zeros((mrows, 1), F32)] * ny
    for d in [0] + near_z:
        s = (z + d) % nz
        if d in next_z:
            await_all(mixed_all.at[s], mz_recv.at[s])
        elif d:
            await_all(mixed_all.at[s, : ny - 1], my_recv.at[s])
        gain = jnp.concatenate([gains[1, pl.ds(s * ny + k, 1), :] for k in range(ny)], axis=1)
        scaled = []
        for k in range(ny):
            stacked = mixed_all[s, k].astype(F32)
            wide_rows = jnp.concatenate([stacked[:mrows], stacked[mrows:]], axis=1)
            squares[k] = squares[k] + jnp.sum(wide_rows * wide_rows, axis=1, keepdims=True)
            scaled.append(wide_rows * gain)
        lhs = jnp.concatenate(scaled, axis=0).astype(BF16)
        here = pl.ds(pl.multiple_of(s * block, block), block)
        for t in range(2):
            product = jnp.dot(lhs, up_all[t, here, :], preferred_element_type=F32)
            if d:
                product = product + acc[t]
            acc[t] = product
    inverse_mlp = lax.rsqrt(jnp.concatenate(squares, axis=0) / width_full + EPS)
    squared = []
    for t in range(2):
        activation = jnp.maximum(inverse_mlp * acc[t], 0.0)
        squared.append((activation * activation).astype(BF16))

    loads[5].wait()
    down_copy.wait_recv()
    rest = rest_z[::-1]
    for d in rest[:1] + next_z + rest[1:] + [0]:
        to = (z + d) % nz
        here = pl.ds(pl.multiple_of(to * block, block), block)
        product = jnp.dot(
            squared[0], down_all[0, :, here], preferred_element_type=F32
        ) + jnp.dot(squared[1], down_all[1, :, here], preferred_element_type=F32)
        for k in range(ny):
            piece_k = product[:, k * 128 : (k + 1) * 128]
            if d:
                down_send[to, k] = piece_k.astype(BF16)
            else:
                down_own[k] = piece_k
        if d in next_z:
            push(
                down_send.at[to],
                down_next.at[next_z.index(d)],
                sent.at[DN],
                arrived.at[DN],
                z=to,
            )
        elif d:
            for e in near_y:
                dst = (y + e) % ny
                push(
                    down_send.at[to, dst], down_y.at[y, to], sent.at[DY], dy_recv.at[to], y=dst
                )
    carried = []
    for k in range(ny):
        stacked = mixed_all[z, k].astype(F32)
        mine = jnp.zeros((mrows, 128), F32)
        for c in range(ny):
            down, across = c // (ny // 2) * mrows, c % (ny // 2) * 128
            mine = jnp.where(y == c, stacked[down : down + mrows, across : across + 128], mine)
        carried.append(mine)
    carried = jnp.concatenate(carried, axis=0)
    quarter = half // 2

    def columns_of(value, t):
        cols = value[:, 64 * t : 64 * (t + 1)]
        return jnp.concatenate([cols[:quarter], cols[quarter:]], axis=1)

    def add_next():
        await_all(down_next, arrived.at[DN])
        for k in range(ny):
            added = down_own[k]
            for i in range(len(next_z)):
                added = added + down_next[i, k].astype(F32)
            down_own[k] = added
            down_send[z, k] = added.astype(BF16)
        for e in near_y:
            dst = (y + e) % ny
            push(down_send.at[z, dst], down_y.at[y, z], sent.at[DY], dy_recv.at[z], y=dst)

    if not rest:
        add_next()
    for d in rest + [0]:
        to = (z + d) % nz
        await_all(down_y.at[: ny - 1, to], dy_recv.at[to])
        summed = down_send[to, y].astype(F32) if d else down_own[y]
        for e in near_y:
            summed = summed + down_y[(y + e) % ny, to].astype(F32)
        if d:
            for t in range(2):
                sum_send[t, to] = columns_of(summed, t).astype(BF16)
                push(sum_send.at[t, to], sum_recv.at[tp, z], sent.at[DZ], arrived.at[DZ], z=to, tp=t)
            if d == rest[0]:
                add_next()
        else:
            whole = summed + carried
            fin_send[0] = columns_of(whole, 0)
            fin_send[1] = columns_of(whole, 1)
            fin_copy = push(
                fin_send.at[other], fin_recv, pair_send.at[4], pair_recv.at[4], tp=other
            )
    if rest:
        await_all(sum_recv.at[:, : len(rest)], arrived.at[DZ])
    total = [fin_send[tp], jnp.zeros((quarter, 128), F32)]
    for d in rest:
        src = (z + d) % nz
        total[0] = total[0] + sum_recv[tp, src].astype(F32)
        total[1] = total[1] + sum_recv[other, src].astype(F32)
    fin_copy.wait_recv()
    total[1] = total[1] + fin_recv[...]
    top = 4 * piece + 8
    packed[top : top + quarter] = jnp.where(tp == 0, total[0], total[1])
    packed[top + quarter : top + half] = jnp.where(tp == 0, total[1], total[0])

    for copy in (tok_copy, out_copy, up_copy, down_copy, fin_copy):
        copy.wait_send()
    await_sent(w_own.at[: ny - 1, :direct_chunks], sent.at[WY])
    await_sent(w_flat.at[direct_chunks:, : (ny - 1) * some], sent.at[WQ])
    await_sent(wo_all.at[tp, head, : (ny - 1) * 128], sent.at[OD])
    await_sent(tok_all.at[: ny - 1], sent.at[TY])
    await_sent(part_send.at[:, : nz - 1], sent.at[PZ])
    await_sent(gate_send.at[: nz - 1], sent.at[GZ])
    await_sent(rows_send.at[: ny - 1], sent.at[RY])
    await_sent(wo_all.at[tp, share, : (ny - 1) * 128], sent.at[OY])
    if nx > 1:
        await_sent(w_flat.at[direct_chunks:, : (ny - 1) * (nx - 1) * some], sent.at[WX])
        await_sent(passed_on, sent.at[OX])
    await_sent(wo_all.at[tp, :, : (ny - 1) * 128], sent.at[OP])
    await_sent(mixed_all.at[: nz - 1, 0], sent.at[MZ])
    await_sent(mixed_all.at[: len(next_z), : ny - 1], sent.at[MN])
    await_sent(mixed_all.at[: nz - len(next_z), : ny - 1], sent.at[MY])
    await_sent(down_next, sent.at[DN])
    await_sent(down_send.at[: nz - len(next_z), : ny - 1], sent.at[DY])
    if rest:
        await_sent(sum_send.at[:, : len(rest)], sent.at[DZ])

    @pl.when(tp == core)
    def _():
        await_sent(heads_all.at[: nz - 1], sent.at[HZ])

    @pl.when(tp != core)
    def _():
        await_sent(heads_all, sent.at[HZ])


def update(ny, mem, packed, new_mem, out_hbm, norm_hbm, stab_hbm, made, out, stab, sems):
    piece = mem.shape[0]
    own = stab.shape[0]
    count = sems.shape[0] - 3
    each = piece // count
    copies = []

    def send(src, dst):
        copies.append(pltpu.make_async_copy(src, dst, sems.at[len(copies)]))
        copies[-1].start()

    inflow_v = packed[:piece].T
    for b in range(count):
        for i in range(b * each, (b + 1) * each):
            key, retain = packed[piece + i], packed[2 * piece + i]
            made[i] = retain[None] * mem[i] + inflow_v[:, i : i + 1] * key[None]
        here = pl.ds(b * each, each)
        send(made.at[here], new_mem.at[here])
        if b == 0:
            send(packed.at[pl.ds(3 * piece, piece)], norm_hbm)
            stab[...] = packed[4 * piece : 4 * piece + own, : stab.shape[1]]
            send(stab, stab_hbm)
            rows = out.shape[1]
            blocks = rows // own // 2
            per = blocks // ny
            quarter = rows // 4
            line = lax.broadcasted_iota(jnp.int32, (rows // 2, rows), 0).astype(F32)
            column = lax.broadcasted_iota(jnp.int32, (rows // 2, rows), 1).astype(F32)
            side = jnp.where(line >= quarter, 1.0, 0.0)
            orders = []
            for upper in range(2):
                at = line + side * quarter + upper * quarter
                group = jnp.floor((at + 0.5) / own)
                inner = group - side * blocks
                in_y = jnp.floor((inner + 0.5) / per)
                in_z = inner - in_y * per
                target = (side * blocks + in_z * ny + in_y) * own + (at - group * own)
                orders.append(jnp.where(column == target, 1.0, 0.0).astype(BF16))
            result = packed[4 * piece + 8 :].T.astype(BF16)
            turned = jnp.dot(result[:64], orders[0], preferred_element_type=F32) + jnp.dot(
                result[64:], orders[1], preferred_element_type=F32
            )
            out[...] = turned.astype(BF16)
            send(out, out_hbm)
    for copy in copies:
        copy.wait()


def body(
    tokens,
    gain_mixer,
    weight_query,
    weight_key,
    weight_value,
    weight_outgate,
    weight_ingate,
    weight_forget,
    bias_input,
    bias_forget,
    memory,
    normalizer,
    stabilizer,
    head_gain,
    weight_out,
    gain_channel,
    weight_up,
    weight_down,
):
    nx, nz, ny = lax.axis_size("dp"), lax.axis_size("z"), lax.axis_size("y")
    own, heads, hd = memory.shape[:3]
    width_full = gain_mixer.shape[0]
    tokens = tokens.T
    rows = tokens.shape[1]
    half = rows // 2
    piece = own * heads
    zrows = ny * own
    block = ny * 128
    chunks = heads // 2
    mrows = nz // 2 * own
    dma = pltpu.SemaphoreType.DMA
    vmem = pl.BlockSpec(memory_space=pltpu.VMEM)
    hbm = pl.BlockSpec(memory_space=pl.ANY)
    mem48 = memory.reshape(piece, hd, hd)
    small = (
        tokens,
        gain_mixer.reshape(-1, 128),
        bias_input.reshape(1, -1),
        bias_forget.reshape(1, -1),
        normalizer.reshape(piece, hd),
        stabilizer,
        head_gain,
        gain_channel.reshape(-1, 128),
    )
    packed = pl.pallas_call(
        functools.partial(kernel, nx, nz, ny, width_full),
        out_shape=jax.ShapeDtypeStruct((4 * piece + 8 + half, hd), F32),
        in_specs=[hbm] * 18,
        out_specs=vmem,
        scratch_shapes=[pltpu.VMEM(value.shape, value.dtype) for value in small]
        + [
            pltpu.VMEM(tokens.shape, BF16),
            pltpu.VMEM((ny, rows, 128), BF16),
            pltpu.VMEM((mrows, block), F32),
            pltpu.VMEM((2, width_full // 128, 128), F32),
            pltpu.VMEM((16, block), BF16),
            pltpu.VMEM((16, block), BF16),
            pltpu.VMEM((piece, hd, hd), F32),
            pltpu.VMEM((piece, hd, 2 * hd), BF16),
            pltpu.VMEM((ny, 128, heads, hd), BF16),
            pltpu.VMEM((4, 128 * heads, hd), F32),
            pltpu.VMEM((ny, chunks, 128, 2 * hd), BF16),
            pltpu.VMEM((chunks, block, 2 * hd), BF16),
            pltpu.VMEM((chunks, nz, 2 * zrows, hd), BF16),
            pltpu.VMEM((chunks, nz, 2 * zrows, hd), BF16),
            pltpu.VMEM((nz, 8, 128), F32),
            pltpu.VMEM((nz, 8, 128), F32),
            pltpu.VMEM((zrows * heads, hd), F32),
            pltpu.VMEM((ny, piece, hd), BF16),
            pltpu.VMEM((ny, piece, hd), BF16),
            pltpu.VMEM((piece, 2 * hd), F32),
            pltpu.VMEM((piece, hd), F32),
            pltpu.VMEM((piece, hd), BF16),
            pltpu.VMEM((nz, piece, hd), BF16),
            pltpu.VMEM((nz * piece, hd), F32),
            pltpu.VMEM((2, heads * hd, block), BF16),
            pltpu.VMEM((2, *weight_up.shape), BF16),
            pltpu.VMEM((2, *weight_down.shape), BF16),
            pltpu.VMEM((nz, ny, 2 * mrows, block // 2), BF16),
            pltpu.VMEM((2, half, weight_up.shape[1]), F32),
            pltpu.VMEM((nz, ny, half, 128), BF16),
            pltpu.VMEM((ny, half, 128), F32),
            pltpu.VMEM((min(2, nz - 1), ny, half, 128), BF16),
            pltpu.VMEM((ny, nz, half, 128), BF16),
            pltpu.VMEM((2, nz, half // 2, 128), BF16),
            pltpu.VMEM((2, nz, half // 2, 128), BF16),
            pltpu.VMEM((2, half // 2, 128), F32),
            pltpu.VMEM((half // 2, 128), F32),
            dma((8,)),
            dma((10,)),
            dma((5,)),
            dma((5,)),
            dma((len(PHASES),)),
            dma((len(PHASES),)),
            dma((chunks,)),
            dma((chunks,)),
            dma((chunks,)),
            dma((nz,)),
            dma((nz,)),
            dma((nz,)),
        ],
        compiler_params=pltpu.CompilerParams(
            collective_id=0, has_side_effects=True, vmem_limit_bytes=56 * 1024 * 1024
        ),
    )(
        *small,
        weight_query,
        weight_key,
        weight_value,
        weight_outgate,
        weight_ingate.T,
        weight_forget.T,
        mem48,
        weight_out,
        weight_up,
        weight_down,
    )
    new_memory, layer_out, new_norm, new_stab = pl.pallas_call(
        functools.partial(update, ny),
        out_shape=(
            jax.ShapeDtypeStruct(mem48.shape, F32),
            jax.ShapeDtypeStruct(tokens.shape, BF16),
            jax.ShapeDtypeStruct((piece, hd), F32),
            jax.ShapeDtypeStruct((own, heads), F32),
        ),
        in_specs=[vmem, vmem],
        out_specs=(hbm,) * 4,
        scratch_shapes=[
            pltpu.VMEM(mem48.shape, F32),
            pltpu.VMEM(tokens.shape, BF16),
            pltpu.VMEM((own, heads), F32),
            dma((piece // 4 + 3,)),
        ],
        compiler_params=pltpu.CompilerParams(vmem_limit_bytes=16 * 1024 * 1024),
    )(mem48, packed)
    new_memory = new_memory.reshape(memory.shape)
    return (layer_out.T, new_memory, new_norm.reshape(normalizer.shape), new_stab)


def solution(mesh):
    kv = mesh.shape["kv"]
    ny = 4
    torus = Mesh(
        mesh.devices.reshape(mesh.shape["dp"], kv // ny, ny, mesh.shape["tp"]),
        ("dp", "z", "y", "tp"),
    )
    placed = (
        P("dp", KV_TP),
        P(),
        P(KV, "tp", None),
        P(KV, "tp", None),
        P(KV, "tp", None),
        P(KV, "tp", None),
        P(),
        P(),
        P(),
        P(),
        P(DP_KV, "tp", None, None),
        P(DP_KV, "tp", None),
        P(DP_KV, "tp"),
        P(),
        P("tp", KV),
        P(),
        P(None, KV_TP),
        P(KV_TP, None),
    )
    return jax.shard_map(
        body,
        mesh=torus,
        in_specs=placed,
        out_specs=(
            P("dp", KV_TP),
            P(DP_KV, "tp", None, None),
            P(DP_KV, "tp", None),
            P(DP_KV, "tp"),
        ),
        check_vma=False,
    )
```
